512 devices in a mesh: sp: 32 (over z, core), tp: 16 (over y, x).
Axes of the slice: x: 4, y: 4, z: 16, core: 2. Of those that a mesh axis runs over, the one named last changes fastest.
Arguments:
- residual: bfloat16 [4096, 2048], P('sp', 'tp'), may hold values from -6 to 6
- out_cot: bfloat16 [4096, 2048], P('sp', 'tp'), may hold values from -6 to 6
- routes: int32 [4096, 2], P('sp'), may hold values from 0 to 31, all different within a row; in each aligned block of 128 rows (0 to 127, 128 to 255, ...) at most 10 rows name the same one
- route_weight: float32 [4096, 2], P('sp'), may hold values from 0.2 to 1
- w_gate: bfloat16 [32, 2048, 2048], P('sp', 'tp'), may hold values from -0.125 to 0.125
- w_up: bfloat16 [32, 2048, 2048], P('sp', 'tp'), may hold values from -0.125 to 0.125
- w_down: bfloat16 [32, 2048, 2048], P('sp', 'tp'), may hold values from -0.125 to 0.125
- w_out: bfloat16 [1024, 2048], P('tp'), may hold values from -0.1875 to 0.1875
- conv_out: bfloat16 [1024, 4096], P('tp', 'sp'), may hold values from -14 to 14
- gate_branch: bfloat16 [1024, 4096], P('tp', 'sp'), may hold values from -6 to 6
- w_recur: bfloat16 [16, 64, 64], P('tp'), may hold values from -0.75 to 0.75
- w_input: bfloat16 [16, 64, 64], P('tp'), may hold values from -0.75 to 0.75
- decay_param: float32 [1024], P('tp'), may hold values from 4.5 to 11
Outputs:
- grad_gate: bfloat16 [32, 2048, 2048], P('sp', 'tp')
- grad_up: bfloat16 [32, 2048, 2048], P('sp', 'tp')
- grad_down: bfloat16 [32, 2048, 2048], P('sp', 'tp')
- grad_proj: float32 [2048, 1024], P('sp', 'tp')
- grad_conv: float32 [1024, 4096], P('tp', 'sp')
- grad_branch: float32 [1024, 4096], P('tp', 'sp')
The draws below stay inside these ranges and needn't reach their ends.
Inputs may be any that keep to these rules, and one draw needn't show every extreme that they name: `routes`: in the rows of one index of sp no expert is named more than 10 times, a bound that some block reaches.
All inputs are finite; a program needn't handle non-finite values.
Results may differ from the reference program's by a relative error of at most 0.025.
Values may be sent and summed in bfloat16 or wider, within the bound.
No kernel may reach another device: no remote copies, remote signals or barrier semaphores. Data moves between devices by JAX's collectives and lax.ppermute only.
A program may use at most 64 MiB of HBM per device.

```python
import math
import jax
import jax.numpy as jnp
import numpy as np
from jax import lax

D = 2048
FF = 2048
MIX_W = 1024
LRU_BD = 64
TOPK = 2
TOK_SP = 128
TOKENS = 4096
EXPERTS = 32
CAP = 10
BLOCKS = 16
N_SP = 32
N_TP = 16


def draw_conv_out(key, part):
    key_base = jax.random.fold_in(key, 11)
    key_level = jax.random.fold_in(key, 12)
    levels = jnp.exp(jax.random.uniform(key_level, (1, TOKENS // 64), jnp.float32, math.log(0.35), math.log(2.8)))
    levels = jnp.repeat(levels, 64, axis=1)
    base = jnp.clip(jax.random.normal(key_base, (MIX_W, TOKENS), jnp.float32), -5.0, 5.0)
    return (base * levels).astype(jnp.bfloat16)


def draw_decay_param(key, part):
    key_pick = jax.random.fold_in(key, 21)
    key_slow = jax.random.fold_in(key, 22)
    key_fast = jax.random.fold_in(key, 23)
    share = 0.5
    slow = jax.random.uniform(key_pick, (MIX_W,), jnp.float32) < share
    slow_values = jax.random.uniform(key_slow, (MIX_W,), jnp.float32, 9.5, 11.0)
    fast_values = jax.random.uniform(key_fast, (MIX_W,), jnp.float32, 4.5, 6.0)
    return jnp.where(slow, slow_values, fast_values).astype(jnp.float32)


def with_spikes(array, rng, source, target, blocks, factor):
    def block_of(axis_at):
        return (jnp.arange(array.shape[axis_at]) // (array.shape[axis_at] // blocks)).reshape((-1,) + (1,) * (array.ndim - 1 - axis_at))

    one_side = jax.random.permutation(rng, blocks)[block_of(target)]
    other_side = (block_of(target) + blocks // 2) % blocks
    return jnp.where((block_of(source) == one_side) | (block_of(source) == other_side), factor * array, array)


def steps_of(stream_key, shape, pieces, low, largest):
    def one(dim, blocks):
        steps = jax.random.uniform(jax.random.fold_in(jax.random.fold_in(stream_key, 6), dim), (blocks,), jnp.float32, low / len(pieces), largest / len(pieces))
        return jnp.repeat(jnp.exp(steps), shape[dim] // blocks).reshape((-1,) + (1,) * (len(shape) - dim - 1))

    loudness = one(*pieces[0])
    for cut in pieces[1:]:
        loudness = loudness * one(*cut)
    return loudness


def shared_out(rng, own, number, rows, count, top, bound, slope):
    order = jax.random.permutation(rng, count)
    crowded, common = shares(count, rows * top, bound, slope, True), shares(count, rows * top, bound, slope, False)
    places = jnp.arange(count)

    def named(sizes, turn):
        used = int((sizes > 0).sum())
        fixed = max(1, used // 4)
        passed = fixed + (places - fixed + turn * (used - fixed)) % max(1, count - fixed)
        return jnp.zeros((count,), jnp.int32).at[order[jnp.where(places < fixed, places, passed)]].set(jnp.asarray(sizes, jnp.int32))

    sizes = jnp.where(number % 4 == 0, named(crowded, number // 4), named(common, number - number // 4 - 1))
    mixed = jax.random.permutation(jax.random.fold_in(own, 3), count)
    giver, receiver = mixed[0:count // 2 * 2:2], mixed[1:count // 2 * 2:2]
    slack = jnp.minimum(sizes[giver] - 1, bound - sizes[receiver]) // 2
    slack = jnp.where((giver == order[0]) | (receiver == order[0]) | (sizes[receiver] == 0), 0, jnp.maximum(slack, 0))
    passed = jax.random.randint(jax.random.fold_in(own, 4), (count // 2,), 0, 1 << 20) % (slack + 1)
    sizes = sizes.at[giver].add(-passed).at[receiver].add(passed)
    labels = jnp.searchsorted(jnp.cumsum(sizes), jnp.arange(rows * top), side="right").astype(jnp.int32)
    table = labels.reshape(top, rows).T
    table = table[jax.random.permutation(jax.random.fold_in(own, 1), rows)]
    turn = jax.random.randint(jax.random.fold_in(own, 2), (rows, 1), 0, top)
    return jnp.take_along_axis(table, (jnp.arange(top)[None, :] + turn) % top, axis=1)


def shares(count, total, most, skew, full):
    loads = [(1 << 20) // math.isqrt(grade ** skew) + 1 for grade in range(1, count + 1)]
    largest = most if full else min(most, max(-(-total // count), total * loads[0] // sum(loads)))
    least = 1 if total - largest >= count - 1 else 0
    holding, spare = [largest] + [least] * (count - 1), total - largest - least * (count - 1)
    while spare > 0:
        movable = [i for i in range(1, count) if holding[i] < largest] or [i for i in range(1, count) if holding[i] < most]
        mass, budget = sum([loads[i] for i in movable]), spare
        for i in movable:
            more = min(most - holding[i], max(1, budget * loads[i] // mass), spare)
            holding[i] = holding[i] + more
            spare = spare - more
    return np.array(holding)


def gaussian(stream_key, shape, deviation, most, shards=(), kind=jnp.bfloat16):
    gain = steps_of(stream_key, shape, shards, -0.22, 0.18) if shards else 1.0
    array = jax.random.normal(stream_key, shape, jnp.float32) * deviation * gain
    return jnp.minimum(jnp.maximum(array, -most), most).astype(kind)


def noise_with(stream_key, extent, width, most, cuts, heavy, kind=jnp.bfloat16):
    values = width * jax.random.normal(stream_key, extent, jnp.float32)
    if cuts:
        values = values * steps_of(stream_key, extent, cuts, -0.22, 0.18)
    return jnp.clip(with_spikes(values, jax.random.fold_in(stream_key, 3), *heavy), -most, most).astype(kind)


def setup_inputs(seed: int = 0) -> dict:
    splits = jax.random.split(jax.random.key(seed), 14)
    residual = gaussian(splits[0], (TOKENS, D), 1.0, 6.0, ((0, 32), (1, 16)))
    out_cot = noise_with(splits[1], (TOKENS, D), 1.0, 6.0, ((0, 32), (1, 16)), (0, 1, 32, 2.75))
    routes_keys = jax.random.split(jax.random.fold_in(splits[2], 1), TOKENS // TOK_SP)
    routes_turns = jax.random.permutation(jax.random.fold_in(splits[2], 3), TOKENS // TOK_SP)
    routes = jax.vmap(lambda own, number: shared_out(jax.random.fold_in(splits[2], 2), own, number, TOK_SP, EXPERTS, TOPK, CAP, 1))(routes_keys, routes_turns).reshape((TOKENS, TOPK))
    route_weight = jnp.clip(0.2 + 0.8 * jax.random.uniform(splits[3], (TOKENS, TOPK), jnp.float32) ** steps_of(splits[3], (TOKENS, TOPK), ((0, 32),), -0.2, 0.2), 0.2, 1.0)
    w_gate = gaussian(splits[4], (EXPERTS, FF, D), D ** -0.5, 0.125, ((0, 32), (1, 16)))
    w_up = gaussian(splits[5], (EXPERTS, FF, D), D ** -0.5, 0.125, ((0, 32), (1, 16)))
    w_down = gaussian(splits[6], (EXPERTS, FF, D), FF ** -0.5, 0.125, ((0, 32), (1, 16)))
    w_out = gaussian(splits[7], (MIX_W, D), MIX_W ** -0.5, 0.1875, ((0, 16),))
    conv_out = draw_conv_out(jax.random.fold_in(splits[13], 71), 0)
    gate_branch = gaussian(splits[9], (MIX_W, TOKENS), 1.0, 6.0, ((0, 16), (1, 32)))
    w_recur = gaussian(splits[10], (BLOCKS, LRU_BD, LRU_BD), LRU_BD ** -0.5, 0.75, ((0, 16),))
    w_input = gaussian(splits[11], (BLOCKS, LRU_BD, LRU_BD), LRU_BD ** -0.5, 0.75, ((0, 16),))
    decay_param = draw_decay_param(jax.random.fold_in(splits[13], 71), 0)
    return dict(residual=residual, out_cot=out_cot, routes=routes, route_weight=route_weight, w_gate=w_gate, w_up=w_up, w_down=w_down, w_out=w_out, conv_out=conv_out, gate_branch=gate_branch, w_recur=w_recur, w_input=w_input, decay_param=decay_param)


LEAK = 0.01
DECAY_SCALE = 8.0

def slot_table(route_ids, expert_count, capacity):
    flat_ids = route_ids.reshape(-1)
    hit_table = (flat_ids[:, None] == jnp.arange(expert_count, dtype=jnp.int32)[None, :]).astype(jnp.int32)
    before = jnp.cumsum(hit_table, axis=0) - hit_table
    slot_num = lax.optimization_barrier(jnp.sum(before * hit_table, axis=1))
    return (flat_ids * capacity + slot_num).astype(jnp.int32)

def fill_table(placed, total):
    match_table = placed[:, None] == jnp.arange(total, dtype=jnp.int32)[None, :]
    filled = jnp.any(match_table, axis=0)
    pair_idx = lax.optimization_barrier(jnp.sum(jnp.where(match_table, jnp.arange(placed.shape[0], dtype=jnp.int32)[:, None], 0), axis=0))
    return (filled, pair_idx.astype(jnp.int32))

def gate_pair(inputs, w_recur, w_input, softness):
    groups = w_recur.shape[0]
    block_width = w_recur.shape[1]
    shaped = inputs.reshape(groups, block_width, inputs.shape[1])
    recur_pre = jnp.einsum('nij,nit->njt', w_recur.astype(jnp.float32), shaped).reshape(inputs.shape)
    admit_pre = jnp.einsum('nij,nit->njt', w_input.astype(jnp.float32), shaped).reshape(inputs.shape)
    decay_rate = jnp.exp(-DECAY_SCALE * jax.nn.sigmoid(recur_pre) * softness[:, None])
    drive_in = jnp.sqrt(1.0 - decay_rate * decay_rate + LEAK) * jax.nn.sigmoid(admit_pre) * inputs
    return (decay_rate, drive_in)

def pair_link(earlier, later):
    return (earlier[0] * later[0], later[0] * earlier[1] + later[1])

def run_chain(decay_rate, drive_in):
    return lax.associative_scan(pair_link, (decay_rate, drive_in), axis=1)[1]

def reference(residual, out_cot, routes, route_weight, w_gate, w_up, w_down, w_out, conv_out, gate_branch, w_recur, w_input, decay_param):
    per_block = routes.reshape(N_SP, TOK_SP * TOPK)
    placed = jax.vmap(lambda route_ids: slot_table(route_ids, EXPERTS, CAP))(per_block)
    filled, pair_idx = jax.vmap(lambda spots: fill_table(spots, EXPERTS * CAP))(placed)
    offsets = (jnp.arange(N_SP, dtype=jnp.int32) * TOK_SP)[:, None]
    token_idx = (pair_idx // TOPK + offsets).astype(jnp.int32)
    factor = jnp.where(filled, jnp.take_along_axis(route_weight.reshape(N_SP, TOK_SP * TOPK), pair_idx, axis=1), 0.0)

    def by_expert(table):
        return jnp.swapaxes(table.reshape(N_SP, EXPERTS, CAP), 0, 1).reshape(EXPERTS, N_SP * CAP)
    token_e = by_expert(token_idx)
    filled_e = by_expert(filled)
    factor_e = by_expert(factor)

    def one_expert(bundle):
        gate_w, up_w, down_w, rows_idx, live, weight = bundle
        in_rows = jnp.where(live[:, None], residual[rows_idx], jnp.zeros((), jnp.bfloat16))
        cot_rows = (weight[:, None] * out_cot[rows_idx].astype(jnp.float32)).astype(jnp.bfloat16)
        pre_gate = jnp.dot(in_rows, gate_w.T, preferred_element_type=jnp.float32)
        pre_up = jnp.dot(in_rows, up_w.T, preferred_element_type=jnp.float32)
        silu_val, silu_back = jax.vjp(jax.nn.silu, pre_gate)
        activ = (silu_val * pre_up).astype(jnp.bfloat16)
        act_cot = jnp.dot(cot_rows, down_w.T, preferred_element_type=jnp.float32)
        gate_cot = silu_back(act_cot * pre_up)[0].astype(jnp.bfloat16)
        up_cot = (act_cot * silu_val).astype(jnp.bfloat16)
        grad_down = jnp.dot(activ.T, cot_rows, preferred_element_type=jnp.float32)
        grad_gate = jnp.dot(gate_cot.T, in_rows, preferred_element_type=jnp.float32)
        grad_up = jnp.dot(up_cot.T, in_rows, preferred_element_type=jnp.float32)
        span = FF // N_TP
        parts = jnp.einsum('snf,nfd->nsd', gate_cot.astype(jnp.float32).reshape(-1, N_TP, span), gate_w.astype(jnp.float32).reshape(N_TP, span, D))
        parts = parts + jnp.einsum('snf,nfd->nsd', up_cot.astype(jnp.float32).reshape(-1, N_TP, span), up_w.astype(jnp.float32).reshape(N_TP, span, D))
        rounded = lax.optimization_barrier(parts.astype(jnp.bfloat16)).astype(jnp.float32)
        slot_grad = lax.optimization_barrier(jnp.sum(rounded, axis=0)).astype(jnp.bfloat16)
        return (grad_gate.astype(jnp.bfloat16), grad_up.astype(jnp.bfloat16), grad_down.astype(jnp.bfloat16), slot_grad)
    results = lax.map(one_expert, (w_gate, w_up, w_down, token_e, filled_e, factor_e))
    slot_grads = results[3].reshape(EXPERTS, N_SP, CAP, D)
    expert_of = (placed // CAP).astype(jnp.int32)
    slot_of = (placed % CAP).astype(jnp.int32)
    picked = slot_grads[expert_of, jnp.arange(N_SP, dtype=jnp.int32)[:, None], slot_of]
    token_grad = lax.optimization_barrier(jnp.sum(picked.reshape(TOKENS, TOPK, D).astype(jnp.float32), axis=1))
    lifted = (out_cot.astype(jnp.float32) + token_grad).astype(jnp.bfloat16)
    mix_cot = lax.dot_general(w_out, lifted, (((1,), (1,)), ((), ())), preferred_element_type=jnp.float32)
    softness = jax.nn.softplus(-decay_param)

    def forward(inputs, branch):
        decay_rate, drive_in = gate_pair(inputs, w_recur, w_input, softness)
        ahead = run_chain(decay_rate, drive_in)
        behind = jnp.flip(run_chain(jnp.flip(decay_rate, 1), jnp.flip(drive_in, 1)), 1)
        return jax.nn.gelu(branch) * (ahead + behind)
    mixed_val, back = jax.vjp(forward, conv_out.astype(jnp.float32), gate_branch.astype(jnp.float32))
    grad_conv, grad_branch = back(mix_cot)
    mixed = mixed_val.astype(jnp.bfloat16)
    grad_proj = jnp.dot(lifted.T, mixed.T, preferred_element_type=jnp.float32)
    return (results[0], results[1], results[2], grad_proj, grad_conv, grad_branch)
```

```python
import jax
import jax.numpy as jnp
from jax import lax
from jax.experimental import pallas as pl
from jax.experimental.pallas import tpu as pltpu
from jax.sharding import PartitionSpec as P

LEAK = 0.01
DECAY_SCALE = 8.0
GELU_A = 0.7978845608028654
GELU_B = 0.044715

BF = jnp.bfloat16
F32 = jnp.float32
I32 = jnp.int32

SEND_ROWS = 24
HOME_ROWS = 16
LAST_ROWS = 40


def iota(shape, dim):
    return lax.broadcasted_iota(I32, shape, dim)


def dot(a, b, ca=1, cb=0, precision=None):
    return lax.dot_general(
        a, b, (((ca,), (cb,)), ((), ())), precision=precision, preferred_element_type=F32
    )


def call(body, outs, args, flops=1, bytes_moved=1, scalars=0, scratch=()):
    specs = [pl.BlockSpec(memory_space=pltpu.SMEM)] * scalars
    specs += [pl.BlockSpec(memory_space=pltpu.VMEM)] * (len(args) - scalars)
    return pl.pallas_call(
        body,
        out_shape=[jax.ShapeDtypeStruct(s, d) for s, d in outs],
        in_specs=specs,
        out_specs=[pl.BlockSpec(memory_space=pltpu.VMEM)] * len(outs),
        scratch_shapes=list(scratch),
        compiler_params=pltpu.CompilerParams(vmem_limit_bytes=24 * 1024 * 1024),
        cost_estimate=pl.CostEstimate(
            flops=flops, bytes_accessed=bytes_moved, transcendentals=0
        ),
    )(*args)


def dispatch_body(experts, routes, weight, residual, cot, sent, comb):
    tokens = residual.shape[0]
    first, second = routes[0:1, :], routes[1:2, :]
    expert = iota((experts, tokens), 0)
    hit0 = (expert == first).astype(F32)
    hit1 = (expert == second).astype(F32)
    earlier = (iota((tokens, tokens), 0) < iota((tokens, tokens), 1)).astype(BF)
    before = dot((hit0 + hit1).astype(BF), earlier)
    slot0 = jnp.sum(before * hit0, axis=0, keepdims=True).astype(I32)
    slot1 = jnp.sum((before + hit0) * hit1, axis=0, keepdims=True).astype(I32)
    back = iota((experts * HOME_ROWS, tokens), 0)
    at_home = (back == first * HOME_ROWS + slot0) | (back == second * HOME_ROWS + slot1)
    comb[...] = at_home.astype(F32).astype(BF)
    row = iota((experts * SEND_ROWS, tokens), 0)
    place0 = first * SEND_ROWS + slot0
    place1 = second * SEND_ROWS + slot1
    in_rows = ((row == place0) | (row == place1)).astype(F32).astype(BF)
    capacity = SEND_ROWS // 2 - 2
    cot0 = row == place0 + capacity
    cot1 = row == place1 + capacity
    factor = jnp.sum(
        jnp.where(cot0, weight[0:1, :], 0.0) + jnp.where(cot1, weight[1:2, :], 0.0),
        axis=1,
        keepdims=True,
    )
    cot_rows = (cot0 | cot1).astype(F32).astype(BF)
    rows = dot(in_rows, residual[...]) + factor * dot(cot_rows, cot[...])
    sent[...] = rows.astype(BF)


def compact_body(experts, capacity, got, out):
    slots = experts * capacity
    total = got.shape[0]
    row = iota((2 * slots, 1), 0)
    half = (row >= slots).astype(I32)
    rest = row - half * slots
    source = jnp.floor((rest.astype(F32) + 0.5) * (1.0 / capacity)).astype(I32)
    target = source * SEND_ROWS + half * capacity + (rest - source * capacity)
    pick = (iota((2 * slots, total), 1) == target).astype(F32).astype(BF)
    rows = dot(pick, got[...]).astype(BF)
    for j in range(out.shape[0]):
        out[j] = rows


def pair(ref, k, lo, hi):
    return jnp.concatenate([ref[2 * k, lo:hi, :], ref[2 * k + 1, lo:hi, :]], axis=1)


def expert_body(whole, w_gate, w_up, w_down, dxp, acts):
    slots = whole.shape[1] // 2
    blocks = whole.shape[0]
    hidden = w_gate.shape[0]
    pre = jnp.zeros((slots, 2 * hidden), F32)
    act_cot = jnp.zeros((slots, hidden), F32)
    for k in range(blocks // 2):
        cols = slice(256 * k, 256 * (k + 1))
        both = jnp.concatenate([w_gate[:, cols], w_up[:, cols]], axis=0)
        pre = pre + dot(pair(whole, k, 0, slots), both, 1, 1)
        act_cot = act_cot + dot(pair(whole, k, slots, 2 * slots), w_down[:, cols], 1, 1)
    pre_gate, pre_up = pre[:, :hidden], pre[:, hidden:]
    sig = jax.nn.sigmoid(pre_gate)
    silu = pre_gate * sig
    slope = sig * (1.0 + pre_gate * (1.0 - sig))
    act = (silu * pre_up).astype(BF)
    gate_cot = (act_cot * pre_up * slope).astype(BF)
    up_cot = (act_cot * silu).astype(BF)
    cots = jnp.concatenate([gate_cot, up_cot], axis=1)
    acts[:, : 2 * hidden] = cots
    acts[:, 2 * hidden :] = act
    for k in range(blocks // 2):
        cols = slice(256 * k, 256 * (k + 1))
        both = jnp.concatenate([w_gate[:, cols], w_up[:, cols]], axis=0)
        part = dot(cots, both).astype(BF)
        dxp[2 * k] = part[:, :128]
        dxp[2 * k + 1] = part[:, 128:]


def grads_body(whole, acts, g_gate, g_up, g_down):
    slots = whole.shape[1] // 2
    hidden = acts.shape[1] // 3
    both = dot(acts[:, : 2 * hidden], pair(whole, 0, 0, slots), 0, 0).astype(BF)
    g_gate[0] = both[:hidden]
    g_up[0] = both[hidden:]
    g_down[0] = dot(acts[:, 2 * hidden :], pair(whole, 0, slots, 2 * slots), 0, 0).astype(BF)


def expert_grads(whole, acts, width):
    blocks, rows, lanes = whole.shape
    hidden = acts.shape[1] // 3
    out = jax.ShapeDtypeStruct((1, hidden, width), BF)
    spec = pl.BlockSpec((1, hidden, 2 * lanes), lambda i: (0, 0, i))
    return pl.pallas_call(
        grads_body,
        grid=(blocks // 2,),
        out_shape=[out] * 3,
        in_specs=[
            pl.BlockSpec((2, rows, lanes), lambda i: (i, 0, 0)),
            pl.BlockSpec(acts.shape, lambda i: (0, 0)),
        ],
        out_specs=[spec] * 3,
        compiler_params=pltpu.CompilerParams(vmem_limit_bytes=16 * 1024 * 1024),
        cost_estimate=pl.CostEstimate(
            flops=3 * rows * hidden * width, bytes_accessed=6 * hidden * width, transcendentals=0
        ),
    )(whole, acts)


def owner_sum_body(experts, capacity, parts, carry, out):
    total = parts[0].astype(F32)
    for j in range(1, parts.shape[0]):
        total = total + parts[j].astype(F32)
    total = total.astype(BF)
    rows = experts * HOME_ROWS
    place = iota((rows, 1), 0)
    inner = place & (HOME_ROWS - 1)
    source = jnp.where(inner < capacity, (place >> 4) * capacity + inner, -1)
    pick = (iota((rows, experts * capacity), 1) == source).astype(F32).astype(BF)
    extra = (iota((rows, carry.shape[0]), 1) == inner - capacity).astype(F32).astype(BF)
    out[...] = (dot(pick, total) + dot(extra, carry[...])).astype(BF)


def lift_body(home, comb, cot, out):
    grad = dot(comb[...], home[...], 0, 0)
    lifted = (cot[...].astype(F32) + grad).astype(BF)
    for j in range(out.shape[0]):
        out[j] = lifted


def shift_in(x, d, fill, lane):
    return jnp.where(lane >= d, pltpu.roll(x, d, 1), fill)


def shift_out(x, d, fill, lane):
    width = x.shape[1]
    return jnp.where(lane < width - d, pltpu.roll(x, width - d, 1), fill)


def scan(decay, drive, lane, moved):
    d = 1
    while d < decay.shape[1]:
        drive = decay * moved(drive, d, 0.0, lane) + drive
        decay = decay * moved(decay, d, 1.0, lane)
        d *= 2
    return decay, drive


def in_three(x):
    high = x.astype(BF)
    rest = x - high.astype(F32)
    mid = rest.astype(BF)
    low = (rest - mid.astype(F32)).astype(BF)
    return high, mid, low


def ends_row(up, down, lane):
    width = up.shape[1]
    ends = jnp.concatenate(
        [jnp.where(lane == width - 1, up, 0.0), jnp.where(lane == 0, down, 0.0)], axis=0
    )
    return dot(jnp.ones((8, width), F32), ends, 1, 1, lax.Precision.HIGHEST)


def to_columns(row, lane):
    channel = iota(lane.shape, 0)
    channels = lane.shape[0]
    up = jnp.sum(jnp.where(lane == channel, row, 0.0), axis=1, keepdims=True)
    down = jnp.sum(jnp.where(lane == channel + channels, row, 0.0), axis=1, keepdims=True)
    return up, down


def fold(me, prods, adds, channels):
    devices, width = prods.shape
    lane = iota((1, width), 1)
    ahead = lane < channels
    total = jnp.zeros((1, width), F32)
    for n in range(devices):
        m = devices - 1 - n
        prod = jnp.where(ahead, prods[n : n + 1, :], prods[m : m + 1, :])
        add = jnp.where(ahead, adds[n : n + 1, :], adds[m : m + 1, :])
        live = jnp.where(ahead, (me > n).astype(I32), (me < m).astype(I32)) > 0
        total = jnp.where(live, prod * total + add, total)
    return total


SAVED = 11


def state_body(conv, branch, w_recur, w_input, soft, saved, carry):
    channels, tokens = conv.shape
    lane = iota((channels, tokens), 1)
    eye = iota((channels, channels), 0) == iota((channels, channels), 1)
    softness = jnp.sum(jnp.where(eye, soft[...], 0.0), axis=1, keepdims=True)
    values = conv[...].astype(F32)
    sig_r = jax.nn.sigmoid(dot(w_recur[0], conv[...], 0, 0))
    sig_a = jax.nn.sigmoid(dot(w_input[0], conv[...], 0, 0))
    decay = jnp.exp(-DECAY_SCALE * sig_r * softness)
    root = jnp.sqrt(1.0 - decay * decay + LEAK)
    direct = root * sig_a
    drive = direct * values
    up_prod, up_state = scan(decay, drive, lane, shift_in)
    down_prod, down_state = scan(decay, drive, lane, shift_out)
    x = branch[...].astype(F32)
    th = jnp.tanh(GELU_A * (x + GELU_B * x * x * x))
    saved[0] = decay
    saved[1] = up_prod
    saved[2] = up_state
    saved[3] = down_prod
    saved[4] = down_state
    saved[5] = 0.5 * x * (1.0 + th)
    saved[6] = 0.5 * (1.0 + th) + 0.5 * x * (1.0 - th * th) * GELU_A * (
        1.0 + 3.0 * GELU_B * x * x
    )
    saved[7] = decay * (-DECAY_SCALE * softness) * sig_r * (1.0 - sig_r)
    saved[8] = -(decay / root) * sig_a * values
    saved[9] = root * values * sig_a * (1.0 - sig_a)
    saved[10] = direct
    rows = in_three(ends_row(up_prod, down_prod, lane)) + in_three(
        ends_row(up_state, down_state, lane)
    )
    place = iota((8, tokens), 0)
    total = jnp.zeros((8, tokens), F32)
    for k, row in enumerate(rows):
        total = jnp.where(place == k, row.astype(F32), total)
    carry[...] = total.astype(BF)


def join_body(me, home, saved, mix, joined, prods, adds):
    devices = prods.shape[0]
    channels, tokens = mix.shape
    rows = home.shape[0]
    lane = iota((channels, tokens), 1)
    offset = iota((devices, rows), 1) - HOME_ROWS * iota((devices, rows), 0)
    base = HOME_ROWS - 6
    prod_rows = ((offset >= base) & (offset < base + 3)).astype(F32).astype(BF)
    add_rows = ((offset >= base + 3) & (offset < base + 6)).astype(F32).astype(BF)
    prods[...] = dot(prod_rows, home[...])
    adds[...] = dot(add_rows, home[...])
    state_in, state_back = to_columns(fold(me[0], prods, adds, channels), lane)
    fwd = saved[2] + saved[1] * state_in
    bwd = saved[4] + saved[3] * state_back
    total = fwd + bwd
    mix[...] = (saved[5] * total).astype(BF)
    joined[0] = jnp.where(lane == 0, state_in, pltpu.roll(fwd, 1, 1))
    joined[1] = jnp.where(lane == tokens - 1, state_back, pltpu.roll(bwd, tokens - 1, 1))
    joined[2] = total * saved[6]


def last_body(lifted, w_out, mix, saved, out, kept):
    blocks, tokens, _ = lifted.shape
    channels = mix.shape[0]
    half = channels // 2
    lane = iota((channels, tokens), 1)
    left = iota((half, 128), 1) < 64
    mixed = mix[...]
    mix_cot = jnp.zeros((channels, tokens), F32)
    for k in range(blocks // 2):
        both = pair(lifted, k, 0, tokens)
        mix_cot = mix_cot + dot(w_out[:, 256 * k : 256 * (k + 1)], both, 1, 1)
        proj = dot(mixed, both)
        for q in range(2):
            part = proj[:, 128 * q : 128 * (q + 1)]
            top, bottom = part[:half], part[half:]
            spot = 4 * k + 2 * q
            out[spot, :half, :] = jnp.where(left, top, pltpu.roll(bottom, 64, 1)).astype(BF)
            out[spot + 1, :half, :] = jnp.where(left, pltpu.roll(top, 64, 1), bottom).astype(BF)
    decay = saved[0]
    cot = mix_cot * saved[5]
    weighted = decay * cot
    _, up = scan(decay, weighted, lane, shift_in)
    _, down = scan(decay, weighted, lane, shift_out)
    kept[0] = mix_cot
    kept[1] = cot
    kept[2] = up
    kept[3] = down
    rows = in_three(ends_row(up, down, lane))
    place = iota((8, tokens), 0)
    total = jnp.zeros((8, tokens), F32)
    for k, row in enumerate(rows):
        total = jnp.where(place == k, row.astype(F32), total)
    total = total.astype(BF)
    for s in range(out.shape[0]):
        out[s, half:, :] = total


def finish_body(me, last, prods, saved, joined, kept, w_recur, w_input, g_proj, g_conv, g_branch, adds):
    devices = prods.shape[0]
    channels, tokens = g_conv.shape
    half = channels // 2
    lane = iota((channels, tokens), 1)
    total = last[0, :half, :].astype(F32)
    carry = jnp.zeros((8, tokens), F32)
    for s in range(devices):
        if s:
            total = total + last[s, :half, :].astype(F32)
        adds[s : s + 1, :] = jnp.sum(last[s, half:, :].astype(F32), axis=0, keepdims=True)
    turned = total.T
    g_proj[...] = jnp.concatenate([turned[:64], turned[64:]], axis=1)
    adj_in, adj_back = to_columns(fold(me[0], prods, adds, channels), lane)
    cot = kept[1]
    up = kept[2] + saved[1] * adj_in
    down = kept[3] + saved[3] * adj_back
    past = cot + jnp.where(lane == 0, adj_in, pltpu.roll(up, 1, 1))
    future = cot + jnp.where(lane == tokens - 1, adj_back, pltpu.roll(down, tokens - 1, 1))
    drive_cot = past + future
    decay_cot = future * joined[0] + past * joined[1] + drive_cot * saved[8]
    recur_cot = decay_cot * saved[7]
    admit_cot = drive_cot * saved[9]
    exact = lax.Precision.HIGHEST
    g_conv[...] = (
        drive_cot * saved[10]
        + dot(w_recur[0].astype(F32), recur_cot, 1, 0, exact)
        + dot(w_input[0].astype(F32), admit_cot, 1, 0, exact)
    )
    g_branch[...] = kept[0] * joined[2]


def local(
    residual,
    out_cot,
    routes,
    route_weight,
    w_gate,
    w_up,
    w_down,
    w_out,
    conv_out,
    gate_branch,
    w_recur,
    w_input,
    decay_param,
):
    experts = lax.axis_size("sp")
    blocks = lax.axis_size("tp")
    me = lax.axis_index("sp").reshape(1).astype(I32)
    tokens, lanes = residual.shape
    capacity = 2 * tokens // experts + 2
    slots = experts * capacity
    hidden, width = w_gate.shape[1:]
    channels = conv_out.shape[0]

    def kernel(body, *static):
        def run(*refs):
            body(*static, *refs)

        return run

    sent, comb = call(
        kernel(dispatch_body, experts),
        [((experts * SEND_ROWS, lanes), BF), ((experts * HOME_ROWS, tokens), BF)],
        (routes.T, route_weight.T, residual, out_cot),
    )
    got = lax.all_to_all(
        sent.reshape(experts, SEND_ROWS, lanes), "sp", split_axis=0, concat_axis=0, tiled=True
    )
    (spread,) = call(
        kernel(compact_body, experts, capacity),
        [((blocks, 2 * slots, lanes), BF)],
        (got.reshape(experts * SEND_ROWS, lanes),),
    )
    whole = lax.all_to_all(spread, "tp", 0, 0, tiled=True)
    soft = jax.nn.softplus(-decay_param).reshape(1, channels)
    saved, carry = call(
        state_body,
        [((SAVED, channels, tokens), F32), ((8, tokens), BF)],
        (conv_out, gate_branch, w_recur, w_input, soft),
        flops=20_000_000,
    )
    dxp, acts = call(
        expert_body,
        [((blocks, slots, lanes), BF), ((slots, 3 * hidden), BF)],
        (whole, w_gate[0], w_up[0], w_down[0]),
        flops=10 * slots * hidden * width,
    )
    parts = lax.all_to_all(dxp, "tp", 0, 0, tiled=True)
    grads = expert_grads(whole, acts, width)
    (returned,) = call(
        kernel(owner_sum_body, experts, capacity),
        [((experts * HOME_ROWS, lanes), BF)],
        (parts, carry),
    )
    home = lax.all_to_all(
        returned.reshape(experts, HOME_ROWS, lanes), "sp", split_axis=0, concat_axis=0, tiled=True
    ).reshape(experts * HOME_ROWS, lanes)
    (own,) = call(lift_body, [((blocks, tokens, lanes), BF)], (home, comb, out_cot))
    lifted = lax.all_to_all(own, "tp", 0, 0, tiled=True)
    mix, joined, prods = call(
        join_body,
        [((channels, tokens), BF), ((3, channels, tokens), F32), ((experts, tokens), F32)],
        (me, home, saved),
        flops=20_000_000,
        scalars=1,
        scratch=(pltpu.VMEM((experts, tokens), F32),),
    )
    piece, kept = call(
        last_body,
        [((experts, LAST_ROWS, lanes), BF), ((4, channels, tokens), F32)],
        (lifted, w_out, mix, saved),
    )
    last = lax.all_to_all(piece, "sp", split_axis=0, concat_axis=0, tiled=True)
    g_proj, g_conv, g_branch = call(
        finish_body,
        [((width // experts, channels), F32), ((channels, tokens), F32), ((channels, tokens), F32)],
        (me, last, prods, saved, joined, kept, w_recur, w_input),
        scalars=1,
        scratch=(pltpu.VMEM((experts, tokens), F32),),
    )
    return (grads[0], grads[1], grads[2], g_proj, g_conv, g_branch)


def solution(mesh):
    return jax.shard_map(
        local,
        mesh=mesh,
        in_specs=(
            P("sp", "tp"),
            P("sp", "tp"),
            P("sp", None),
            P("sp", None),
            P("sp", "tp", None),
            P("sp", "tp", None),
            P("sp", "tp", None),
            P("tp", None),
            P("tp", "sp"),
            P("tp", "sp"),
            P("tp", None, None),
            P("tp", None, None),
            P("tp"),
        ),
        out_specs=(
            P("sp", "tp", None),
            P("sp", "tp", None),
            P("sp", "tp", None),
            P("sp", "tp"),
            P("tp", "sp"),
            P("tp", "sp"),
        ),
        check_vma=False,
    )
```

```python
import jax
import jax.numpy as jnp
from jax import lax
from jax.experimental import pallas as pl
from jax.experimental.pallas import tpu as pltpu
from jax.sharding import PartitionSpec as P

LEAK = 0.01
DECAY_SCALE = 8.0
GELU_A = 0.7978845608028654
GELU_B = 0.044715

BF = jnp.bfloat16
F32 = jnp.float32
I32 = jnp.int32

SEND_ROWS = 24
HOME_ROWS = 16
LAST_ROWS = 40


def iota(shape, dim):
    return lax.broadcasted_iota(I32, shape, dim)


def dot(a, b, ca=1, cb=0, precision=None):
    return lax.dot_general(
        a, b, (((ca,), (cb,)), ((), ())), precision=precision, preferred_element_type=F32
    )


def call(body, outs, args, flops=1, bytes_moved=1, fetched=0, scratch=(), far=()):
    specs = [pl.BlockSpec(memory_space=pltpu.HBM)] * fetched
    specs += [pl.BlockSpec(memory_space=pltpu.VMEM)] * (len(args) - fetched)
    scratch = [pltpu.VMEM(a.shape, a.dtype) for a in args[:fetched]] + list(scratch)
    kept = [pltpu.with_memory_space_constraint(a, pltpu.HBM) for a in args[:fetched]]
    args = kept + list(args[fetched:])
    if fetched:
        scratch.append(pltpu.SemaphoreType.DMA((fetched,)))
    return pl.pallas_call(
        body,
        out_shape=[
            pltpu.HBM(*out) if k in far else jax.ShapeDtypeStruct(*out)
            for k, out in enumerate(outs)
        ],
        in_specs=specs,
        out_specs=[
            pl.BlockSpec(memory_space=pltpu.HBM if k in far else pltpu.VMEM)
            for k in range(len(outs))
        ],
        scratch_shapes=scratch,
        compiler_params=pltpu.CompilerParams(vmem_limit_bytes=24 * 1024 * 1024),
        cost_estimate=pl.CostEstimate(
            flops=flops, bytes_accessed=bytes_moved, transcendentals=0
        ),
    )(*args)


def fetch(sources, targets, sems):
    copies = [
        pltpu.make_async_copy(source, target, sems.at[k])
        for k, (source, target) in enumerate(zip(sources, targets))
    ]
    for copy in copies:
        copy.start()
    return copies


def dispatch_body(experts, *refs):
    sources, (sent, comb), targets, sems = refs[:4], refs[4:6], refs[6:10], refs[10]
    for copy in fetch(sources, targets, sems):
        copy.wait()
    routes, weight, residual, cot = targets
    tokens = residual.shape[0]
    first, second = routes[0:1, :], routes[1:2, :]
    expert = iota((experts, tokens), 0)
    hit0 = (expert == first).astype(F32)
    hit1 = (expert == second).astype(F32)
    earlier = (iota((tokens, tokens), 0) < iota((tokens, tokens), 1)).astype(BF)
    before = dot((hit0 + hit1).astype(BF), earlier)
    slot0 = jnp.sum(before * hit0, axis=0, keepdims=True).astype(I32)
    slot1 = jnp.sum((before + hit0) * hit1, axis=0, keepdims=True).astype(I32)
    back = iota((experts * HOME_ROWS, tokens), 0)
    at_home = (back == first * HOME_ROWS + slot0) | (back == second * HOME_ROWS + slot1)
    comb[...] = at_home.astype(F32).astype(BF)
    row = iota((experts * SEND_ROWS, tokens), 0)
    place0 = first * SEND_ROWS + slot0
    place1 = second * SEND_ROWS + slot1
    in_rows = ((row == place0) | (row == place1)).astype(F32).astype(BF)
    capacity = SEND_ROWS // 2 - 2
    cot0 = row == place0 + capacity
    cot1 = row == place1 + capacity
    factor = jnp.sum(
        jnp.where(cot0, weight[0:1, :], 0.0) + jnp.where(cot1, weight[1:2, :], 0.0),
        axis=1,
        keepdims=True,
    )
    cot_rows = (cot0 | cot1).astype(F32).astype(BF)
    rows = dot(in_rows, residual[...]) + factor * dot(cot_rows, cot[...])
    sent[...] = rows.astype(BF)


def compact_body(experts, capacity, got, out):
    slots = experts * capacity
    total = got.shape[0]
    row = iota((2 * slots, 1), 0)
    half = (row >= slots).astype(I32)
    rest = row - half * slots
    source = jnp.floor((rest.astype(F32) + 0.5) * (1.0 / capacity)).astype(I32)
    target = source * SEND_ROWS + half * capacity + (rest - source * capacity)
    pick = (iota((2 * slots, total), 1) == target).astype(F32).astype(BF)
    rows = dot(pick, got[...]).astype(BF)
    for j in range(out.shape[0]):
        out[j] = rows


def pair(ref, k, lo, hi):
    return jnp.concatenate([ref[2 * k, lo:hi, :], ref[2 * k + 1, lo:hi, :]], axis=1)


def expert_body(*refs):
    sources, (whole, w_gate, w_up, w_down) = refs[:5], refs[5:9]
    dxp, far_acts, saved, carry = refs[9:13]
    targets, acts, acts_sem, sems = refs[13:18], refs[18], refs[19], refs[20]
    copies = fetch(sources, targets, sems)
    slots = whole.shape[1] // 2
    blocks = whole.shape[0]
    hidden = w_gate.shape[0]
    pre = jnp.zeros((slots, 2 * hidden), F32)
    act_cot = jnp.zeros((slots, hidden), F32)
    for k in range(blocks // 2):
        cols = slice(256 * k, 256 * (k + 1))
        both = jnp.concatenate([w_gate[:, cols], w_up[:, cols]], axis=0)
        pre = pre + dot(pair(whole, k, 0, slots), both, 1, 1)
        act_cot = act_cot + dot(pair(whole, k, slots, 2 * slots), w_down[:, cols], 1, 1)
    pre_gate, pre_up = pre[:, :hidden], pre[:, hidden:]
    sig = jax.nn.sigmoid(pre_gate)
    silu = pre_gate * sig
    slope = sig * (1.0 + pre_gate * (1.0 - sig))
    act = (silu * pre_up).astype(BF)
    gate_cot = (act_cot * pre_up * slope).astype(BF)
    up_cot = (act_cot * silu).astype(BF)
    cots = jnp.concatenate([gate_cot, up_cot], axis=1)
    acts[:, : 2 * hidden] = cots
    acts[:, 2 * hidden :] = act
    write = pltpu.make_async_copy(acts, far_acts, acts_sem)
    write.start()
    for k in range(blocks // 2):
        cols = slice(256 * k, 256 * (k + 1))
        both = jnp.concatenate([w_gate[:, cols], w_up[:, cols]], axis=0)
        part = dot(cots, both).astype(BF)
        dxp[2 * k] = part[:, :128]
        dxp[2 * k + 1] = part[:, 128:]
    for copy in copies:
        copy.wait()
    state_body(*targets, saved, carry)
    write.wait()


def grads_body(whole, acts, g_gate, g_up, g_down):
    slots = whole.shape[1] // 2
    hidden = acts.shape[1] // 3
    both = dot(acts[:, : 2 * hidden], pair(whole, 0, 0, slots), 0, 0).astype(BF)
    g_gate[0] = both[:hidden]
    g_up[0] = both[hidden:]
    g_down[0] = dot(acts[:, 2 * hidden :], pair(whole, 0, slots, 2 * slots), 0, 0).astype(BF)


def expert_grads(whole, acts, width):
    blocks, rows, lanes = whole.shape
    hidden = acts.shape[1] // 3
    out = jax.ShapeDtypeStruct((1, hidden, width), BF)
    spec = pl.BlockSpec((1, hidden, 2 * lanes), lambda i: (0, 0, i))
    return pl.pallas_call(
        grads_body,
        grid=(blocks // 2,),
        out_shape=[out] * 3,
        in_specs=[
            pl.BlockSpec((2, rows, lanes), lambda i: (i, 0, 0)),
            pl.BlockSpec(acts.shape, lambda i: (0, 0)),
        ],
        out_specs=[spec] * 3,
        compiler_params=pltpu.CompilerParams(vmem_limit_bytes=16 * 1024 * 1024),
        cost_estimate=pl.CostEstimate(
            flops=3 * rows * hidden * width, bytes_accessed=6 * hidden * width, transcendentals=0
        ),
    )(whole, acts)


def owner_sum_body(experts, capacity, parts, carry, out):
    total = parts[0].astype(F32)
    for j in range(1, parts.shape[0]):
        total = total + parts[j].astype(F32)
    total = total.astype(BF)
    rows = experts * HOME_ROWS
    place = iota((rows, 1), 0)
    inner = place & (HOME_ROWS - 1)
    source = jnp.where(inner < capacity, (place >> 4) * capacity + inner, -1)
    pick = (iota((rows, experts * capacity), 1) == source).astype(F32).astype(BF)
    extra = (iota((rows, carry.shape[0]), 1) == inner - capacity).astype(F32).astype(BF)
    out[...] = (dot(pick, total) + dot(extra, carry[...])).astype(BF)


def lift_body(home, comb, cot, saved, out, mix, ends, adds):
    grad = dot(comb[...], home[...], 0, 0)
    lifted = (cot[...].astype(F32) + grad).astype(BF)
    for j in range(out.shape[0]):
        out[j] = lifted
    join_body(home, saved, mix, ends, adds)


def shift_in(x, d, fill, lane):
    return jnp.where(lane >= d, pltpu.roll(x, d, 1), fill)


def shift_out(x, d, fill, lane):
    width = x.shape[1]
    return jnp.where(lane < width - d, pltpu.roll(x, width - d, 1), fill)


def scan(decay, drive, lane, moved):
    d = 1
    while d < decay.shape[1]:
        drive = decay * moved(drive, d, 0.0, lane) + drive
        decay = decay * moved(decay, d, 1.0, lane)
        d *= 2
    return decay, drive


def in_three(x):
    high = x.astype(BF)
    rest = x - high.astype(F32)
    mid = rest.astype(BF)
    low = (rest - mid.astype(F32)).astype(BF)
    return high, mid, low


def ends_row(up, down, lane):
    width = up.shape[1]
    ends = jnp.concatenate(
        [jnp.where(lane == width - 1, up, 0.0), jnp.where(lane == 0, down, 0.0)], axis=0
    )
    return dot(jnp.ones((8, width), F32), ends, 1, 1, lax.Precision.HIGHEST)


def to_columns(row, lane):
    channel = iota(lane.shape, 0)
    channels = lane.shape[0]
    up = jnp.sum(jnp.where(lane == channel, row, 0.0), axis=1, keepdims=True)
    down = jnp.sum(jnp.where(lane == channel + channels, row, 0.0), axis=1, keepdims=True)
    return up, down


def fold(me, prods, adds, channels):
    devices, width = prods.shape
    lane = iota((1, width), 1)
    ahead = lane < channels
    total = jnp.zeros((1, width), F32)
    for n in range(devices):
        m = devices - 1 - n
        prod = jnp.where(ahead, prods[n : n + 1, :], prods[m : m + 1, :])
        add = jnp.where(ahead, adds[n : n + 1, :], adds[m : m + 1, :])
        live = jnp.where(ahead, (me > n).astype(I32), (me < m).astype(I32)) > 0
        total = jnp.where(live, prod * total + add, total)
    return total


SAVED = 12


def soft_plus(x):
    small = jnp.exp(-jnp.abs(x))
    z = small / (2.0 + small)
    square = z * z
    series = jnp.full_like(z, 1.0 / 19.0)
    for odd in (17, 15, 13, 11, 9, 7, 5, 3, 1):
        series = series * square + 1.0 / odd
    return jnp.maximum(x, 0.0) + 2.0 * z * series


def state_body(conv, branch, w_recur, w_input, decay_param, saved, carry):
    channels, tokens = conv.shape
    lane = iota((channels, tokens), 1)
    eye = iota((channels, channels), 0) == iota((channels, channels), 1)
    softness = jnp.sum(jnp.where(eye, soft_plus(-decay_param[...]), 0.0), axis=1, keepdims=True)
    values = conv[...].astype(F32)
    sig_r = jax.nn.sigmoid(dot(w_recur[0], conv[...], 0, 0))
    sig_a = jax.nn.sigmoid(dot(w_input[0], conv[...], 0, 0))
    decay = jnp.exp(-DECAY_SCALE * sig_r * softness)
    root = jnp.sqrt(1.0 - decay * decay + LEAK)
    direct = root * sig_a
    drive = direct * values
    up_prod, up_state = scan(decay, drive, lane, shift_in)
    down_prod, down_state = scan(decay, drive, lane, shift_out)
    x = branch[...].astype(F32)
    th = jnp.tanh(GELU_A * (x + GELU_B * x * x * x))
    saved[0] = decay
    saved[1] = up_prod
    saved[2] = up_state
    saved[3] = down_prod
    saved[4] = down_state
    saved[5] = 0.5 * x * (1.0 + th)
    saved[6] = 0.5 * (1.0 + th) + 0.5 * x * (1.0 - th * th) * GELU_A * (
        1.0 + 3.0 * GELU_B * x * x
    )
    saved[7] = decay * (-DECAY_SCALE * softness) * sig_r * (1.0 - sig_r)
    saved[8] = -(decay / root) * sig_a * values
    saved[9] = root * values * sig_a * (1.0 - sig_a)
    saved[10] = direct
    saved[11] = jnp.concatenate([w_recur[0], w_input[0]], axis=1).astype(F32)
    rows = in_three(ends_row(up_prod, down_prod, lane)) + in_three(
        ends_row(up_state, down_state, lane)
    )
    place = iota((8, tokens), 0)
    total = jnp.zeros((8, tokens), F32)
    for k, row in enumerate(rows):
        total = jnp.where(place == k, row.astype(F32), total)
    carry[...] = total.astype(BF)


def joined_states(saved, state_in, state_back):
    return saved[2] + saved[1] * state_in, saved[4] + saved[3] * state_back


def join_body(home, saved, mix, ends, adds):
    channels, tokens = mix.shape
    devices = adds.shape[0]
    rows = home.shape[0]
    lane = iota((channels, tokens), 1)
    offset = iota((devices, rows), 1) - HOME_ROWS * iota((devices, rows), 0)
    base = HOME_ROWS - 6
    prod_rows = ((offset >= base) & (offset < base + 3)).astype(F32).astype(BF)
    add_rows = ((offset >= base + 3) & (offset < base + 6)).astype(F32).astype(BF)
    prods = ends.at[channels:, :]
    prods[...] = dot(prod_rows, home[...])
    adds[...] = dot(add_rows, home[...])
    state_in, state_back = to_columns(fold(lax.axis_index("sp"), prods, adds, channels), lane)
    ends[:channels, :] = jnp.where(lane < channels, state_in, state_back)
    fwd, bwd = joined_states(saved, state_in, state_back)
    mix[...] = (saved[5] * (fwd + bwd)).astype(BF)


def last_body(lifted, w_out, mix, saved, far_out, kept, out, sems):
    blocks, tokens, _ = lifted.shape
    channels = mix.shape[0]
    half = channels // 2
    lane = iota((channels, tokens), 1)
    left = iota((half, 128), 1) < 64
    mixed = mix[...]
    mix_cot = jnp.zeros((channels, tokens), F32)
    for k in range(blocks // 2):
        both = pair(lifted, k, 0, tokens)
        mix_cot = mix_cot + dot(w_out[:, 256 * k : 256 * (k + 1)], both, 1, 1)
        proj = dot(mixed, both)
        for q in range(2):
            part = proj[:, 128 * q : 128 * (q + 1)]
            top, bottom = part[:half], part[half:]
            spot = 4 * k + 2 * q
            out[spot, :half, :] = jnp.where(left, top, pltpu.roll(bottom, 64, 1)).astype(BF)
            out[spot + 1, :half, :] = jnp.where(left, pltpu.roll(top, 64, 1), bottom).astype(BF)
    first = pltpu.make_async_copy(out.at[:, :half, :], far_out.at[:, :half, :], sems.at[0])
    first.start()
    decay = saved[0]
    cot = mix_cot * saved[5]
    weighted = decay * cot
    _, up = scan(decay, weighted, lane, shift_in)
    _, down = scan(decay, weighted, lane, shift_out)
    kept[0] = mix_cot
    kept[1] = cot
    kept[2] = up
    kept[3] = down
    rows = in_three(ends_row(up, down, lane))
    place = iota((8, tokens), 0)
    total = jnp.zeros((8, tokens), F32)
    for k, row in enumerate(rows):
        total = jnp.where(place == k, row.astype(F32), total)
    total = total.astype(BF)
    for s in range(out.shape[0]):
        out[s, half:, :] = total
    second = pltpu.make_async_copy(out.at[:, half:, :], far_out.at[:, half:, :], sems.at[1])
    second.start()
    first.wait()
    second.wait()


def finish_body(last, ends, saved, kept, g_proj, g_conv, g_branch, adds):
    devices = adds.shape[0]
    channels, tokens = g_conv.shape
    prods = ends.at[channels:, :]
    half = channels // 2
    lane = iota((channels, tokens), 1)
    total = last[0, :half, :].astype(F32)
    for s in range(devices):
        if s:
            total = total + last[s, :half, :].astype(F32)
        adds[s : s + 1, :] = jnp.sum(last[s, half:, :].astype(F32), axis=0, keepdims=True)
    turned = total.T
    g_proj[...] = jnp.concatenate([turned[:64], turned[64:]], axis=1)
    adj_in, adj_back = to_columns(fold(lax.axis_index("sp"), prods, adds, channels), lane)
    state_in, state_back = ends[:channels, :1], ends[:channels, tokens - 1 :]
    fwd, bwd = joined_states(saved, state_in, state_back)
    before = jnp.where(lane == 0, state_in, pltpu.roll(fwd, 1, 1))
    after = jnp.where(lane == tokens - 1, state_back, pltpu.roll(bwd, tokens - 1, 1))
    cot = kept[1]
    up = kept[2] + saved[1] * adj_in
    down = kept[3] + saved[3] * adj_back
    past = cot + jnp.where(lane == 0, adj_in, pltpu.roll(up, 1, 1))
    future = cot + jnp.where(lane == tokens - 1, adj_back, pltpu.roll(down, tokens - 1, 1))
    drive_cot = past + future
    decay_cot = future * before + past * after + drive_cot * saved[8]
    recur_cot = decay_cot * saved[7]
    admit_cot = drive_cot * saved[9]
    exact = lax.Precision.HIGHEST
    g_conv[...] = (
        drive_cot * saved[10]
        + dot(saved[11], jnp.concatenate([recur_cot, admit_cot], axis=0), 1, 0, exact)
    )
    g_branch[...] = kept[0] * (fwd + bwd) * saved[6]


def local(
    residual,
    out_cot,
    routes,
    route_weight,
    w_gate,
    w_up,
    w_down,
    w_out,
    conv_out,
    gate_branch,
    w_recur,
    w_input,
    decay_param,
):
    experts = lax.axis_size("sp")
    blocks = lax.axis_size("tp")
    tokens, lanes = residual.shape
    capacity = 2 * tokens // experts + 2
    slots = experts * capacity
    hidden, width = w_gate.shape[1:]
    channels = conv_out.shape[0]

    def kernel(body, *static):
        def run(*refs):
            body(*static, *refs)

        return run

    sent, comb = call(
        kernel(dispatch_body, experts),
        [((experts * SEND_ROWS, lanes), BF), ((experts * HOME_ROWS, tokens), BF)],
        (routes.T, route_weight.T, residual, out_cot),
        fetched=4,
    )
    got = lax.all_to_all(
        sent.reshape(experts, SEND_ROWS, lanes), "sp", split_axis=0, concat_axis=0, tiled=True
    )
    (spread,) = call(
        kernel(compact_body, experts, capacity),
        [((blocks, 2 * slots, lanes), BF)],
        (got.reshape(experts * SEND_ROWS, lanes),),
    )
    whole = lax.all_to_all(spread, "tp", 0, 0, tiled=True)
    dxp, acts, saved, carry = call(
        expert_body,
        [
            ((blocks, slots, lanes), BF),
            ((slots, 3 * hidden), BF),
            ((SAVED, channels, tokens), F32),
            ((8, tokens), BF),
        ],
        (
            conv_out,
            gate_branch,
            w_recur,
            w_input,
            decay_param.reshape(1, channels),
            whole,
            w_gate[0],
            w_up[0],
            w_down[0],
        ),
        fetched=5,
        scratch=(pltpu.VMEM((slots, 3 * hidden), BF), pltpu.SemaphoreType.DMA),
        far=(1,),
        flops=10 * slots * hidden * width,
    )
    parts = lax.all_to_all(dxp, "tp", 0, 0, tiled=True)
    (returned,) = call(
        kernel(owner_sum_body, experts, capacity),
        [((experts * HOME_ROWS, lanes), BF)],
        (parts, carry),
    )
    home = lax.all_to_all(
        returned.reshape(experts, HOME_ROWS, lanes), "sp", split_axis=0, concat_axis=0, tiled=True
    ).reshape(experts * HOME_ROWS, lanes)
    own, mix, ends = call(
        lift_body,
        [
            ((blocks, tokens, lanes), BF),
            ((channels, tokens), BF),
            ((channels + experts, tokens), F32),
        ],
        (home, comb, out_cot, saved),
        scratch=(pltpu.VMEM((experts, tokens), F32),),
    )
    lifted = lax.all_to_all(own, "tp", 0, 0, tiled=True)
    piece, kept = call(
        last_body,
        [((experts, LAST_ROWS, lanes), BF), ((4, channels, tokens), F32)],
        (lifted, w_out, mix, saved),
        scratch=(pltpu.VMEM((experts, LAST_ROWS, lanes), BF), pltpu.SemaphoreType.DMA((2,))),
        far=(0,),
    )
    piece, acts = lax.optimization_barrier((piece, acts))
    grads = expert_grads(whole, acts, width)
    last = lax.all_to_all(piece, "sp", split_axis=0, concat_axis=0, tiled=True)
    g_proj, g_conv, g_branch = call(
        finish_body,
        [((width // experts, channels), F32), ((channels, tokens), F32), ((channels, tokens), F32)],
        (last, ends, saved, kept),
        scratch=(pltpu.VMEM((experts, tokens), F32),),
    )
    return (grads[0], grads[1], grads[2], g_proj, g_conv, g_branch)


def solution(mesh):
    return jax.shard_map(
        local,
        mesh=mesh,
        in_specs=(
            P("sp", "tp"),
            P("sp", "tp"),
            P("sp", None),
            P("sp", None),
            P("sp", "tp", None),
            P("sp", "tp", None),
            P("sp", "tp", None),
            P("tp", None),
            P("tp", "sp"),
            P("tp", "sp"),
            P("tp", None, None),
            P("tp", None, None),
            P("tp"),
        ),
        out_specs=(
            P("sp", "tp", None),
            P("sp", "tp", None),
            P("sp", "tp", None),
            P("sp", "tp"),
            P("tp", "sp"),
            P("tp", "sp"),
        ),
        check_vma=False,
    )
```

```python
import jax
import jax.numpy as jnp
from jax import lax
from jax.experimental import pallas as pl
from jax.experimental.pallas import tpu as pltpu
from jax.sharding import PartitionSpec as P

LEAK = 0.01
DECAY_SCALE = 8.0
GELU_A = 0.7978845608028654
GELU_B = 0.044715

BF = jnp.bfloat16
F32 = jnp.float32
I32 = jnp.int32

HOME_ROWS = 16
GROUP = 4


def iota(shape, dim):
    return lax.broadcasted_iota(I32, shape, dim)


def dot(a, b, ca=1, cb=0, precision=None):
    return lax.dot_general(
        a, b, (((ca,), (cb,)), ((), ())), precision=precision, preferred_element_type=F32
    )


def call(body, outs, args, flops=1, bytes_moved=1, fetched=0, scratch=(), far=()):
    specs = [pl.BlockSpec(memory_space=pltpu.HBM)] * fetched
    specs += [pl.BlockSpec(memory_space=pltpu.VMEM)] * (len(args) - fetched)
    scratch = [pltpu.VMEM(a.shape, a.dtype) for a in args[:fetched]] + list(scratch)
    kept = [pltpu.with_memory_space_constraint(a, pltpu.HBM) for a in args[:fetched]]
    args = kept + list(args[fetched:])
    if fetched:
        scratch.append(pltpu.SemaphoreType.DMA((fetched,)))
    return pl.pallas_call(
        body,
        out_shape=[
            pltpu.HBM(*out) if k in far else jax.ShapeDtypeStruct(*out)
            for k, out in enumerate(outs)
        ],
        in_specs=specs,
        out_specs=[
            pl.BlockSpec(memory_space=pltpu.HBM if k in far else pltpu.VMEM)
            for k in range(len(outs))
        ],
        scratch_shapes=scratch,
        compiler_params=pltpu.CompilerParams(vmem_limit_bytes=24 * 1024 * 1024),
        cost_estimate=pl.CostEstimate(
            flops=flops, bytes_accessed=bytes_moved, transcendentals=0
        ),
    )(*args)


def fetch(sources, targets, sems):
    copies = [
        pltpu.make_async_copy(source, target, sems.at[k])
        for k, (source, target) in enumerate(zip(sources, targets))
    ]
    for copy in copies:
        copy.start()
    return copies


def dispatch_body(experts, *refs):
    sources, (sent, comb), targets, sems = refs[:4], refs[4:6], refs[6:10], refs[10]
    for copy in fetch(sources, targets, sems):
        copy.wait()
    routes, weight, residual, cot = targets
    tokens = residual.shape[0]
    first, second = routes[0:1, :], routes[1:2, :]
    expert = iota((experts, tokens), 0)
    hit0 = (expert == first).astype(F32)
    hit1 = (expert == second).astype(F32)
    earlier = (iota((tokens, tokens), 0) < iota((tokens, tokens), 1)).astype(BF)
    before = dot((hit0 + hit1).astype(BF), earlier)
    slot0 = jnp.sum(before * hit0, axis=0, keepdims=True).astype(I32)
    slot1 = jnp.sum((before + hit0) * hit1, axis=0, keepdims=True).astype(I32)
    back = iota((experts * HOME_ROWS, tokens), 0)
    at_home = (back == first * HOME_ROWS + slot0) | (back == second * HOME_ROWS + slot1)
    comb[...] = at_home.astype(F32).astype(BF)
    count = sent.shape[2] // tokens
    capacity = GROUP * count // 2
    row = iota((experts * GROUP, tokens), 0)
    place0 = first * 2 * capacity + slot0
    place1 = second * 2 * capacity + slot1
    spot = (row & (GROUP - 1)) + (row >> 2) * 2 * capacity
    for k in range(count):
        here = spot + GROUP * k
        in_rows = ((here == place0) | (here == place1)).astype(F32).astype(BF)
        cot0 = here == place0 + capacity
        cot1 = here == place1 + capacity
        factor = jnp.sum(
            jnp.where(cot0, weight[0:1, :], 0.0) + jnp.where(cot1, weight[1:2, :], 0.0),
            axis=1,
            keepdims=True,
        )
        cot_rows = (cot0 | cot1).astype(F32).astype(BF)
        rows = dot(in_rows, residual[...]) + factor * dot(cot_rows, cot[...])
        for e in range(experts):
            sent[e, :, tokens * k : tokens * (k + 1)] = rows[GROUP * e : GROUP * (e + 1)].astype(BF)


def compact_body(experts, capacity, got, out):
    slots = experts * capacity
    lanes = out.shape[2]
    count = got.shape[2] // lanes
    blocks = [
        jnp.concatenate(
            [got[e, :, lanes * k : lanes * (k + 1)].astype(F32) for e in range(experts)], axis=0
        )
        for k in range(count)
    ]
    row = iota((2 * slots, 1), 0)
    half = (row >= slots).astype(I32)
    rest = row - half * slots
    source = jnp.floor((rest.astype(F32) + 0.5) * (1.0 / capacity)).astype(I32)
    inner = half * capacity + (rest - source * capacity)
    target = (inner >> 2) * experts * GROUP + source * GROUP + (inner & (GROUP - 1))
    total = count * experts * GROUP
    pick = (iota((2 * slots, total), 1) == target).astype(F32).astype(BF)
    rows = dot(pick, jnp.concatenate(blocks, axis=0).astype(BF)).astype(BF)
    for j in range(out.shape[0]):
        out[j] = rows


def pair(ref, k, lo, hi):
    return jnp.concatenate([ref[2 * k, lo:hi, :], ref[2 * k + 1, lo:hi, :]], axis=1)


def expert_body(*refs):
    sources, (whole, w_gate, w_up, w_down) = refs[:5], refs[5:9]
    dxp, far_acts, saved, carry = refs[9:13]
    targets, acts, acts_sem, sems = refs[13:18], refs[18], refs[19], refs[20]
    copies = fetch(sources, targets, sems)
    slots = whole.shape[1] // 2
    blocks = whole.shape[0]
    hidden = w_gate.shape[0]
    pre = jnp.zeros((slots, 2 * hidden), F32)
    act_cot = jnp.zeros((slots, hidden), F32)
    for k in range(blocks // 2):
        cols = slice(256 * k, 256 * (k + 1))
        both = jnp.concatenate([w_gate[:, cols], w_up[:, cols]], axis=0)
        pre = pre + dot(pair(whole, k, 0, slots), both, 1, 1)
        act_cot = act_cot + dot(pair(whole, k, slots, 2 * slots), w_down[:, cols], 1, 1)
    pre_gate, pre_up = pre[:, :hidden], pre[:, hidden:]
    sig = jax.nn.sigmoid(pre_gate)
    silu = pre_gate * sig
    slope = sig * (1.0 + pre_gate * (1.0 - sig))
    act = (silu * pre_up).astype(BF)
    gate_cot = (act_cot * pre_up * slope).astype(BF)
    up_cot = (act_cot * silu).astype(BF)
    cots = jnp.concatenate([gate_cot, up_cot], axis=1)
    acts[:, : 2 * hidden] = cots
    acts[:, 2 * hidden :] = act
    write = pltpu.make_async_copy(acts, far_acts, acts_sem)
    write.start()
    for k in range(blocks // 2):
        cols = slice(256 * k, 256 * (k + 1))
        both = jnp.concatenate([w_gate[:, cols], w_up[:, cols]], axis=0)
        part = dot(cots, both).astype(BF)
        dxp[2 * k] = part[:, :128]
        dxp[2 * k + 1] = part[:, 128:]
    for copy in copies:
        copy.wait()
    state_body(*targets, saved, carry)
    write.wait()


def grads_body(whole, acts, g_gate, g_up, g_down):
    slots = whole.shape[1] // 2
    hidden = acts.shape[1] // 3
    both = dot(acts[:, : 2 * hidden], pair(whole, 0, 0, slots), 0, 0).astype(BF)
    g_gate[0] = both[:hidden]
    g_up[0] = both[hidden:]
    g_down[0] = dot(acts[:, 2 * hidden :], pair(whole, 0, slots, 2 * slots), 0, 0).astype(BF)


def expert_grads(whole, acts, width):
    blocks, rows, lanes = whole.shape
    hidden = acts.shape[1] // 3
    out = jax.ShapeDtypeStruct((1, hidden, width), BF)
    spec = pl.BlockSpec((1, hidden, 2 * lanes), lambda i: (0, 0, i))
    return pl.pallas_call(
        grads_body,
        grid=(blocks // 2,),
        out_shape=[out] * 3,
        in_specs=[
            pl.BlockSpec((2, rows, lanes), lambda i: (i, 0, 0)),
            pl.BlockSpec(acts.shape, lambda i: (0, 0)),
        ],
        out_specs=[spec] * 3,
        compiler_params=pltpu.CompilerParams(vmem_limit_bytes=16 * 1024 * 1024),
        cost_estimate=pl.CostEstimate(
            flops=3 * rows * hidden * width, bytes_accessed=6 * hidden * width, transcendentals=0
        ),
    )(whole, acts)


def owner_sum_body(experts, capacity, parts, carry, out):
    total = parts[0].astype(F32)
    for j in range(1, parts.shape[0]):
        total = total + parts[j].astype(F32)
    total = total.astype(BF)
    rows = experts * HOME_ROWS
    place = iota((rows, 1), 0)
    inner = place & (HOME_ROWS - 1)
    source = jnp.where(inner < capacity, (place >> 4) * capacity + inner, -1)
    pick = (iota((rows, experts * capacity), 1) == source).astype(F32).astype(BF)
    extra = (iota((rows, carry.shape[0]), 1) == inner - capacity).astype(F32).astype(BF)
    out[...] = (dot(pick, total) + dot(extra, carry[...])).astype(BF)


def lift_body(home, comb, cot, saved, out, mix, ends, adds):
    grad = dot(comb[...], home[...], 0, 0)
    lifted = (cot[...].astype(F32) + grad).astype(BF)
    for j in range(out.shape[0]):
        out[j] = lifted
    join_body(home, saved, mix, ends, adds)


def shift_in(x, d, fill, lane):
    return jnp.where(lane >= d, pltpu.roll(x, d, 1), fill)


def shift_out(x, d, fill, lane):
    width = x.shape[1]
    return jnp.where(lane < width - d, pltpu.roll(x, width - d, 1), fill)


def scan(decay, drive, lane, moved):
    d = 1
    while d < decay.shape[1]:
        drive = decay * moved(drive, d, 0.0, lane) + drive
        decay = decay * moved(decay, d, 1.0, lane)
        d *= 2
    return decay, drive


def in_three(x):
    high = x.astype(BF)
    rest = x - high.astype(F32)
    mid = rest.astype(BF)
    low = (rest - mid.astype(F32)).astype(BF)
    return high, mid, low


def ends_row(up, down, lane):
    width = up.shape[1]
    ends = jnp.concatenate(
        [jnp.where(lane == width - 1, up, 0.0), jnp.where(lane == 0, down, 0.0)], axis=0
    )
    return dot(jnp.ones((8, width), F32), ends, 1, 1, lax.Precision.HIGHEST)


def to_columns(row, lane):
    channel = iota(lane.shape, 0)
    channels = lane.shape[0]
    up = jnp.sum(jnp.where(lane == channel, row, 0.0), axis=1, keepdims=True)
    down = jnp.sum(jnp.where(lane == channel + channels, row, 0.0), axis=1, keepdims=True)
    return up, down


def fold(me, prods, adds, channels):
    devices, width = prods.shape
    lane = iota((1, width), 1)
    ahead = lane < channels
    total = jnp.zeros((1, width), F32)
    for n in range(devices):
        m = devices - 1 - n
        prod = jnp.where(ahead, prods[n : n + 1, :], prods[m : m + 1, :])
        add = jnp.where(ahead, adds[n : n + 1, :], adds[m : m + 1, :])
        live = jnp.where(ahead, (me > n).astype(I32), (me < m).astype(I32)) > 0
        total = jnp.where(live, prod * total + add, total)
    return total


SAVED = 12


def soft_plus(x):
    small = jnp.exp(-jnp.abs(x))
    z = small / (2.0 + small)
    square = z * z
    series = jnp.full_like(z, 1.0 / 19.0)
    for odd in (17, 15, 13, 11, 9, 7, 5, 3, 1):
        series = series * square + 1.0 / odd
    return jnp.maximum(x, 0.0) + 2.0 * z * series


def state_body(conv, branch, w_recur, w_input, decay_param, saved, carry):
    channels, tokens = conv.shape
    lane = iota((channels, tokens), 1)
    eye = iota((channels, channels), 0) == iota((channels, channels), 1)
    softness = jnp.sum(jnp.where(eye, soft_plus(-decay_param[...]), 0.0), axis=1, keepdims=True)
    values = conv[...].astype(F32)
    sig_r = jax.nn.sigmoid(dot(w_recur[0], conv[...], 0, 0))
    sig_a = jax.nn.sigmoid(dot(w_input[0], conv[...], 0, 0))
    decay = jnp.exp(-DECAY_SCALE * sig_r * softness)
    root = jnp.sqrt(1.0 - decay * decay + LEAK)
    direct = root * sig_a
    drive = direct * values
    up_prod, up_state = scan(decay, drive, lane, shift_in)
    down_prod, down_state = scan(decay, drive, lane, shift_out)
    x = branch[...].astype(F32)
    th = jnp.tanh(GELU_A * (x + GELU_B * x * x * x))
    saved[0] = decay
    saved[1] = up_prod
    saved[2] = up_state
    saved[3] = down_prod
    saved[4] = down_state
    saved[5] = 0.5 * x * (1.0 + th)
    saved[6] = 0.5 * (1.0 + th) + 0.5 * x * (1.0 - th * th) * GELU_A * (
        1.0 + 3.0 * GELU_B * x * x
    )
    saved[7] = decay * (-DECAY_SCALE * softness) * sig_r * (1.0 - sig_r)
    saved[8] = -(decay / root) * sig_a * values
    saved[9] = root * values * sig_a * (1.0 - sig_a)
    saved[10] = direct
    saved[11] = jnp.concatenate([w_recur[0], w_input[0]], axis=1).astype(F32)
    rows = in_three(ends_row(up_prod, down_prod, lane)) + in_three(
        ends_row(up_state, down_state, lane)
    )
    place = iota((8, tokens), 0)
    total = jnp.zeros((8, tokens), F32)
    for k, row in enumerate(rows):
        total = jnp.where(place == k, row.astype(F32), total)
    carry[...] = total.astype(BF)


def joined_states(saved, state_in, state_back):
    return saved[2] + saved[1] * state_in, saved[4] + saved[3] * state_back


def join_body(home, saved, mix, ends, adds):
    channels, tokens = mix.shape
    devices = adds.shape[0]
    rows = home.shape[0]
    lane = iota((channels, tokens), 1)
    offset = iota((devices, rows), 1) - HOME_ROWS * iota((devices, rows), 0)
    base = HOME_ROWS - 6
    prod_rows = ((offset >= base) & (offset < base + 3)).astype(F32).astype(BF)
    add_rows = ((offset >= base + 3) & (offset < base + 6)).astype(F32).astype(BF)
    prods = ends.at[channels:, :]
    prods[...] = dot(prod_rows, home[...])
    adds[...] = dot(add_rows, home[...])
    state_in, state_back = to_columns(fold(lax.axis_index("sp"), prods, adds, channels), lane)
    ends[:channels, :] = jnp.where(lane < channels, state_in, state_back)
    fwd, bwd = joined_states(saved, state_in, state_back)
    mix[...] = (saved[5] * (fwd + bwd)).astype(BF)


def in_groups(out, spot, rows):
    width = rows.shape[1]
    for k in range(rows.shape[0] // GROUP):
        out[spot, :, width * k : width * (k + 1)] = rows[GROUP * k : GROUP * (k + 1)].astype(BF)


def last_body(lifted, w_out, mix, saved, ends, far_out, far_kept, out, kept, sems):
    blocks, tokens, _ = lifted.shape
    channels = mix.shape[0]
    half = channels // 2
    lane = iota((channels, tokens), 1)
    left = iota((half, 128), 1) < 64
    mixed = mix[...]
    mix_cot = jnp.zeros((channels, tokens), F32)
    for k in range(blocks // 2):
        both = pair(lifted, k, 0, tokens)
        mix_cot = mix_cot + dot(w_out[:, 256 * k : 256 * (k + 1)], both, 1, 1)
        proj = dot(mixed, both)
        for q in range(2):
            part = proj[:, 128 * q : 128 * (q + 1)]
            top, bottom = part[:half], part[half:]
            spot = 4 * k + 2 * q
            in_groups(out, spot, jnp.where(left, top, pltpu.roll(bottom, 64, 1)))
            in_groups(out, spot + 1, jnp.where(left, pltpu.roll(top, 64, 1), bottom))
    cut = half // GROUP * 128
    first = pltpu.make_async_copy(out.at[:, :, :cut], far_out.at[:, :, :cut], sems.at[0])
    first.start()
    decay = saved[0]
    cot = mix_cot * saved[5]
    weighted = decay * cot
    _, up = scan(decay, weighted, lane, shift_in)
    _, down = scan(decay, weighted, lane, shift_out)
    kept[:channels] = mix_cot
    kept[channels : 2 * channels] = cot
    kept[2 * channels : 3 * channels] = up
    kept[3 * channels : 4 * channels] = down
    kept[4 * channels :] = ends[...]
    third = pltpu.make_async_copy(kept, far_kept, sems.at[2])
    third.start()
    rows = in_three(ends_row(up, down, lane))
    place = iota((8, tokens), 0)
    total = jnp.zeros((8, tokens), F32)
    for k, row in enumerate(rows):
        total = jnp.where(place == k, row.astype(F32), total)
    total = total[:GROUP].astype(BF)
    for s in range(out.shape[0]):
        out[s, :, cut:] = total
    second = pltpu.make_async_copy(out.at[:, :, cut:], far_out.at[:, :, cut:], sems.at[1])
    second.start()
    first.wait()
    third.wait()
    second.wait()


def finish_body(far_kept, last, saved, g_proj, g_conv, g_branch, kept, adds, sems):
    (copy,) = fetch((far_kept,), (kept,), sems)
    devices = adds.shape[0]
    channels, tokens = g_conv.shape
    ends = kept.at[4 * channels :, :]
    prods = kept.at[5 * channels :, :]
    half = channels // 2
    lane = iota((channels, tokens), 1)
    cut = half // GROUP * 128
    total = last[0, :, :cut].astype(F32)
    for s in range(devices):
        if s:
            total = total + last[s, :, :cut].astype(F32)
        adds[s : s + 1, :] = jnp.sum(last[s, :, cut:].astype(F32), axis=0, keepdims=True)
    turned = jnp.concatenate([total[:, k : k + 128] for k in range(0, cut, 128)], axis=0).T
    g_proj[...] = jnp.concatenate([turned[:64], turned[64:]], axis=1)
    copy.wait()
    adj_in, adj_back = to_columns(fold(lax.axis_index("sp"), prods, adds, channels), lane)
    state_in, state_back = ends[:channels, :1], ends[:channels, tokens - 1 :]
    fwd, bwd = joined_states(saved, state_in, state_back)
    before = jnp.where(lane == 0, state_in, pltpu.roll(fwd, 1, 1))
    after = jnp.where(lane == tokens - 1, state_back, pltpu.roll(bwd, tokens - 1, 1))
    cot = kept[channels : 2 * channels]
    up = kept[2 * channels : 3 * channels] + saved[1] * adj_in
    down = kept[3 * channels : 4 * channels] + saved[3] * adj_back
    past = cot + jnp.where(lane == 0, adj_in, pltpu.roll(up, 1, 1))
    future = cot + jnp.where(lane == tokens - 1, adj_back, pltpu.roll(down, tokens - 1, 1))
    drive_cot = past + future
    decay_cot = future * before + past * after + drive_cot * saved[8]
    recur_cot = decay_cot * saved[7]
    admit_cot = drive_cot * saved[9]
    exact = lax.Precision.HIGHEST
    g_conv[...] = (
        drive_cot * saved[10]
        + dot(saved[11], jnp.concatenate([recur_cot, admit_cot], axis=0), 1, 0, exact)
    )
    g_branch[...] = kept[:channels] * (fwd + bwd) * saved[6]


def local(
    residual,
    out_cot,
    routes,
    route_weight,
    w_gate,
    w_up,
    w_down,
    w_out,
    conv_out,
    gate_branch,
    w_recur,
    w_input,
    decay_param,
):
    experts = lax.axis_size("sp")
    blocks = lax.axis_size("tp")
    tokens, lanes = residual.shape
    capacity = 2 * tokens // experts + 2
    slots = experts * capacity
    hidden, width = w_gate.shape[1:]
    channels = conv_out.shape[0]

    def kernel(body, *static):
        def run(*refs):
            body(*static, *refs)

        return run

    sent, comb = call(
        kernel(dispatch_body, experts),
        [
            ((experts, GROUP, 2 * capacity // GROUP * lanes), BF),
            ((experts * HOME_ROWS, tokens), BF),
        ],
        (routes.T, route_weight.T, residual, out_cot),
        fetched=4,
    )
    got = lax.all_to_all(sent, "sp", split_axis=0, concat_axis=0, tiled=True)
    (spread,) = call(
        kernel(compact_body, experts, capacity),
        [((blocks, 2 * slots, lanes), BF)],
        (got,),
    )
    whole = lax.all_to_all(spread, "tp", 0, 0, tiled=True)
    dxp, acts, saved, carry = call(
        expert_body,
        [
            ((blocks, slots, lanes), BF),
            ((slots, 3 * hidden), BF),
            ((SAVED, channels, tokens), F32),
            ((8, tokens), BF),
        ],
        (
            conv_out,
            gate_branch,
            w_recur,
            w_input,
            decay_param.reshape(1, channels),
            whole,
            w_gate[0],
            w_up[0],
            w_down[0],
        ),
        fetched=5,
        scratch=(pltpu.VMEM((slots, 3 * hidden), BF), pltpu.SemaphoreType.DMA),
        far=(1,),
        flops=10 * slots * hidden * width,
    )
    parts = lax.all_to_all(dxp, "tp", 0, 0, tiled=True)
    (returned,) = call(
        kernel(owner_sum_body, experts, capacity),
        [((experts * HOME_ROWS, lanes), BF)],
        (parts, carry),
    )
    home = lax.all_to_all(
        returned.reshape(experts, HOME_ROWS, lanes), "sp", split_axis=0, concat_axis=0, tiled=True
    ).reshape(experts * HOME_ROWS, lanes)
    own, mix, ends = call(
        lift_body,
        [
            ((blocks, tokens, lanes), BF),
            ((channels, tokens), BF),
            ((channels + experts, tokens), F32),
        ],
        (home, comb, out_cot, saved),
        scratch=(pltpu.VMEM((experts, tokens), F32),),
    )
    lifted = lax.all_to_all(own, "tp", 0, 0, tiled=True)
    last_width = (channels // 2 // GROUP + 1) * lanes
    piece, kept = call(
        last_body,
        [((experts, GROUP, last_width), BF), ((5 * channels + experts, tokens), F32)],
        (lifted, w_out, mix, saved, ends),
        scratch=(
            pltpu.VMEM((experts, GROUP, last_width), BF),
            pltpu.VMEM((5 * channels + experts, tokens), F32),
            pltpu.SemaphoreType.DMA((3,)),
        ),
        far=(0, 1),
    )
    piece, acts = lax.optimization_barrier((piece, acts))
    grads = expert_grads(whole, acts, width)
    last = lax.all_to_all(piece, "sp", split_axis=0, concat_axis=0, tiled=True)
    g_proj, g_conv, g_branch = call(
        finish_body,
        [((width // experts, channels), F32), ((channels, tokens), F32), ((channels, tokens), F32)],
        (kept, last, saved),
        fetched=1,
        scratch=(pltpu.VMEM((experts, tokens), F32),),
    )
    return (grads[0], grads[1], grads[2], g_proj, g_conv, g_branch)


def solution(mesh):
    return jax.shard_map(
        local,
        mesh=mesh,
        in_specs=(
            P("sp", "tp"),
            P("sp", "tp"),
            P("sp", None),
            P("sp", None),
            P("sp", "tp", None),
            P("sp", "tp", None),
            P("sp", "tp", None),
            P("tp", None),
            P("tp", "sp"),
            P("tp", "sp"),
            P("tp", None, None),
            P("tp", None, None),
            P("tp"),
        ),
        out_specs=(
            P("sp", "tp", None),
            P("sp", "tp", None),
            P("sp", "tp", None),
            P("sp", "tp"),
            P("tp", "sp"),
            P("tp", "sp"),
        ),
        check_vma=False,
    )
```

```python
import jax
import jax.numpy as jnp
from jax import lax
from jax.experimental import pallas as pl
from jax.experimental.pallas import tpu as pltpu
from jax.sharding import PartitionSpec as P

LEAK = 0.01
DECAY_SCALE = 8.0
GELU_A = 0.7978845608028654
GELU_B = 0.044715

BF = jnp.bfloat16
F32 = jnp.float32
I32 = jnp.int32

HOME_ROWS = 16
GROUP = 4


def iota(shape, dim):
    return lax.broadcasted_iota(I32, shape, dim)


def dot(a, b, ca=1, cb=0, precision=None):
    return lax.dot_general(
        a, b, (((ca,), (cb,)), ((), ())), precision=precision, preferred_element_type=F32
    )


def call(body, outs, args, flops=1, bytes_moved=1, fetched=0, scratch=(), far=()):
    specs = [pl.BlockSpec(memory_space=pltpu.HBM)] * fetched
    specs += [pl.BlockSpec(memory_space=pltpu.VMEM)] * (len(args) - fetched)
    scratch = [pltpu.VMEM(a.shape, a.dtype) for a in args[:fetched]] + list(scratch)
    kept = [pltpu.with_memory_space_constraint(a, pltpu.HBM) for a in args[:fetched]]
    args = kept + list(args[fetched:])
    if fetched:
        scratch.append(pltpu.SemaphoreType.DMA((fetched,)))
    return pl.pallas_call(
        body,
        out_shape=[
            pltpu.HBM(*out) if k in far else jax.ShapeDtypeStruct(*out)
            for k, out in enumerate(outs)
        ],
        in_specs=specs,
        out_specs=[
            pl.BlockSpec(memory_space=pltpu.HBM if k in far else pltpu.VMEM)
            for k in range(len(outs))
        ],
        scratch_shapes=scratch,
        compiler_params=pltpu.CompilerParams(vmem_limit_bytes=24 * 1024 * 1024),
        cost_estimate=pl.CostEstimate(
            flops=flops, bytes_accessed=bytes_moved, transcendentals=0
        ),
    )(*args)


def fetch(sources, targets, sems):
    copies = [
        pltpu.make_async_copy(source, target, sems.at[k])
        for k, (source, target) in enumerate(zip(sources, targets))
    ]
    for copy in copies:
        copy.start()
    return copies


def dispatch_body(experts, *refs):
    sources, (sent, comb), targets, sems = refs[:4], refs[4:6], refs[6:10], refs[10]
    for copy in fetch(sources, targets, sems):
        copy.wait()
    routes, weight, residual, cot = targets
    tokens = residual.shape[0]
    first, second = routes[0:1, :], routes[1:2, :]
    expert = iota((experts, tokens), 0)
    hit0 = (expert == first).astype(F32)
    hit1 = (expert == second).astype(F32)
    earlier = (iota((tokens, tokens), 0) < iota((tokens, tokens), 1)).astype(BF)
    before = dot((hit0 + hit1).astype(BF), earlier)
    slot0 = jnp.sum(before * hit0, axis=0, keepdims=True).astype(I32)
    slot1 = jnp.sum((before + hit0) * hit1, axis=0, keepdims=True).astype(I32)
    back = iota((experts * HOME_ROWS, tokens), 0)
    at_home = (back == first * HOME_ROWS + slot0) | (back == second * HOME_ROWS + slot1)
    comb[...] = at_home.astype(F32).astype(BF)
    count = sent.shape[2] // tokens
    capacity = GROUP * count // 2
    row = iota((experts * GROUP, tokens), 0)
    place0 = first * 2 * capacity + slot0
    place1 = second * 2 * capacity + slot1
    spot = (row & (GROUP - 1)) + (row >> 2) * 2 * capacity
    for k in range(count):
        here = spot + GROUP * k
        in_rows = ((here == place0) | (here == place1)).astype(F32).astype(BF)
        cot0 = here == place0 + capacity
        cot1 = here == place1 + capacity
        factor = jnp.sum(
            jnp.where(cot0, weight[0:1, :], 0.0) + jnp.where(cot1, weight[1:2, :], 0.0),
            axis=1,
            keepdims=True,
        )
        cot_rows = (cot0 | cot1).astype(F32).astype(BF)
        rows = dot(in_rows, residual[...]) + factor * dot(cot_rows, cot[...])
        for e in range(experts):
            sent[e, :, tokens * k : tokens * (k + 1)] = rows[GROUP * e : GROUP * (e + 1)].astype(BF)


def compact_body(experts, capacity, got, out):
    slots = experts * capacity
    lanes = out.shape[2]
    count = got.shape[2] // lanes
    blocks = [
        jnp.concatenate(
            [got[e, :, lanes * k : lanes * (k + 1)].astype(F32) for e in range(experts)], axis=0
        )
        for k in range(count)
    ]
    row = iota((2 * slots, 1), 0)
    half = (row >= slots).astype(I32)
    rest = row - half * slots
    source = jnp.floor((rest.astype(F32) + 0.5) * (1.0 / capacity)).astype(I32)
    inner = half * capacity + (rest - source * capacity)
    target = (inner >> 2) * experts * GROUP + source * GROUP + (inner & (GROUP - 1))
    total = count * experts * GROUP
    pick = (iota((2 * slots, total), 1) == target).astype(F32).astype(BF)
    rows = dot(pick, jnp.concatenate(blocks, axis=0).astype(BF)).astype(BF)
    for j in range(out.shape[0]):
        out[j] = rows


def pair(ref, k, lo, hi):
    return jnp.concatenate([ref[2 * k, lo:hi, :], ref[2 * k + 1, lo:hi, :]], axis=1)


def expert_body(*refs):
    sources, (whole, w_gate, w_up, w_down) = refs[:5], refs[5:9]
    dxp, far_acts, saved, carry = refs[9:13]
    targets, acts, acts_sem, sems = refs[13:18], refs[18], refs[19], refs[20]
    copies = fetch(sources, targets, sems)
    slots = whole.shape[1] // 2
    blocks = whole.shape[0]
    hidden = w_gate.shape[0]
    pre = jnp.zeros((slots, 2 * hidden), F32)
    act_cot = jnp.zeros((slots, hidden), F32)
    for k in range(blocks // 2):
        cols = slice(256 * k, 256 * (k + 1))
        both = jnp.concatenate([w_gate[:, cols], w_up[:, cols]], axis=0)
        pre = pre + dot(pair(whole, k, 0, slots), both, 1, 1)
        act_cot = act_cot + dot(pair(whole, k, slots, 2 * slots), w_down[:, cols], 1, 1)
    pre_gate, pre_up = pre[:, :hidden], pre[:, hidden:]
    sig = jax.nn.sigmoid(pre_gate)
    silu = pre_gate * sig
    slope = sig * (1.0 + pre_gate * (1.0 - sig))
    act = (silu * pre_up).astype(BF)
    gate_cot = (act_cot * pre_up * slope).astype(BF)
    up_cot = (act_cot * silu).astype(BF)
    cots = jnp.concatenate([gate_cot, up_cot], axis=1)
    acts[:, : 2 * hidden] = cots
    acts[:, 2 * hidden :] = act
    write = pltpu.make_async_copy(acts, far_acts, acts_sem)
    write.start()
    for k in range(blocks // 2):
        cols = slice(256 * k, 256 * (k + 1))
        both = jnp.concatenate([w_gate[:, cols], w_up[:, cols]], axis=0)
        part = dot(cots, both).astype(BF)
        dxp[2 * k] = part[:, :128]
        dxp[2 * k + 1] = part[:, 128:]
    for copy in copies:
        copy.wait()
    state_body(*targets, saved, carry)
    write.wait()


def grads_body(whole, acts, g_gate, g_up, g_down):
    slots = whole.shape[1] // 2
    hidden = acts.shape[1] // 3
    both = dot(acts[:, : 2 * hidden], pair(whole, 0, 0, slots), 0, 0).astype(BF)
    g_gate[0] = both[:hidden]
    g_up[0] = both[hidden:]
    g_down[0] = dot(acts[:, 2 * hidden :], pair(whole, 0, slots, 2 * slots), 0, 0).astype(BF)


def expert_grads(whole, acts, width):
    blocks, rows, lanes = whole.shape
    hidden = acts.shape[1] // 3
    out = jax.ShapeDtypeStruct((1, hidden, width), BF)
    spec = pl.BlockSpec((1, hidden, 2 * lanes), lambda i: (0, 0, i))
    return pl.pallas_call(
        grads_body,
        grid=(blocks // 2,),
        out_shape=[out] * 3,
        in_specs=[
            pl.BlockSpec((2, rows, lanes), lambda i: (i, 0, 0)),
            pl.BlockSpec(acts.shape, lambda i: (0, 0)),
        ],
        out_specs=[spec] * 3,
        compiler_params=pltpu.CompilerParams(vmem_limit_bytes=16 * 1024 * 1024),
        cost_estimate=pl.CostEstimate(
            flops=3 * rows * hidden * width, bytes_accessed=6 * hidden * width, transcendentals=0
        ),
    )(whole, acts)


def owner_sum_body(experts, capacity, parts, carry, out):
    total = parts[0].astype(F32)
    for j in range(1, parts.shape[0]):
        total = total + parts[j].astype(F32)
    total = total.astype(BF)
    rows = experts * HOME_ROWS
    place = iota((rows, 1), 0)
    inner = place & (HOME_ROWS - 1)
    source = jnp.where(inner < capacity, (place >> 4) * capacity + inner, -1)
    pick = (iota((rows, experts * capacity), 1) == source).astype(F32).astype(BF)
    extra = (iota((rows, carry.shape[0]), 1) == inner - capacity).astype(F32).astype(BF)
    out[...] = (dot(pick, total) + dot(extra, carry[...])).astype(BF)


def lift_body(home, comb, cot, saved, out, mix, ends, adds):
    grad = dot(comb[...], home[...], 0, 0)
    lifted = (cot[...].astype(F32) + grad).astype(BF)
    for j in range(out.shape[0]):
        out[j] = lifted
    join_body(home, saved, mix, ends, adds)


def shift_in(x, d, fill, lane):
    return jnp.where(lane >= d, pltpu.roll(x, d, 1), fill)


def shift_out(x, d, fill, lane):
    width = x.shape[1]
    return jnp.where(lane < width - d, pltpu.roll(x, width - d, 1), fill)


def scan(decay, drive, lane, moved):
    d = 1
    while d < decay.shape[1]:
        drive = decay * moved(drive, d, 0.0, lane) + drive
        decay = decay * moved(decay, d, 1.0, lane)
        d *= 2
    return decay, drive


def in_three(x):
    high = x.astype(BF)
    rest = x - high.astype(F32)
    mid = rest.astype(BF)
    low = (rest - mid.astype(F32)).astype(BF)
    return high, mid, low


def ends_row(up, down, lane):
    width = up.shape[1]
    ends = jnp.concatenate(
        [jnp.where(lane == width - 1, up, 0.0), jnp.where(lane == 0, down, 0.0)], axis=0
    )
    return dot(jnp.ones((8, width), F32), ends, 1, 1, lax.Precision.HIGHEST)


def to_columns(row, lane):
    channel = iota(lane.shape, 0)
    channels = lane.shape[0]
    up = jnp.sum(jnp.where(lane == channel, row, 0.0), axis=1, keepdims=True)
    down = jnp.sum(jnp.where(lane == channel + channels, row, 0.0), axis=1, keepdims=True)
    return up, down


def fold(me, prods, adds, channels):
    devices, width = prods.shape
    lane = iota((1, width), 1)
    ahead = lane < channels
    total = jnp.zeros((1, width), F32)
    for n in range(devices):
        m = devices - 1 - n
        prod = jnp.where(ahead, prods[n : n + 1, :], prods[m : m + 1, :])
        add = jnp.where(ahead, adds[n : n + 1, :], adds[m : m + 1, :])
        live = jnp.where(ahead, (me > n).astype(I32), (me < m).astype(I32)) > 0
        total = jnp.where(live, prod * total + add, total)
    return total


SAVED = 12


def soft_plus(x):
    small = jnp.exp(-jnp.abs(x))
    z = small / (2.0 + small)
    square = z * z
    series = jnp.full_like(z, 1.0 / 19.0)
    for odd in (17, 15, 13, 11, 9, 7, 5, 3, 1):
        series = series * square + 1.0 / odd
    return jnp.maximum(x, 0.0) + 2.0 * z * series


def state_body(conv, branch, w_recur, w_input, decay_param, saved, carry):
    channels, tokens = conv.shape
    lane = iota((channels, tokens), 1)
    eye = iota((channels, channels), 0) == iota((channels, channels), 1)
    softness = jnp.sum(jnp.where(eye, soft_plus(-decay_param[...]), 0.0), axis=1, keepdims=True)
    values = conv[...].astype(F32)
    sig_r = jax.nn.sigmoid(dot(w_recur[0], conv[...], 0, 0))
    sig_a = jax.nn.sigmoid(dot(w_input[0], conv[...], 0, 0))
    decay = jnp.exp(-DECAY_SCALE * sig_r * softness)
    root = jnp.sqrt(1.0 - decay * decay + LEAK)
    direct = root * sig_a
    drive = direct * values
    up_prod, up_state = scan(decay, drive, lane, shift_in)
    down_prod, down_state = scan(decay, drive, lane, shift_out)
    x = branch[...].astype(F32)
    th = jnp.tanh(GELU_A * (x + GELU_B * x * x * x))
    saved[0] = decay
    saved[1] = up_prod
    saved[2] = up_state
    saved[3] = down_prod
    saved[4] = down_state
    saved[5] = 0.5 * x * (1.0 + th)
    saved[6] = 0.5 * (1.0 + th) + 0.5 * x * (1.0 - th * th) * GELU_A * (
        1.0 + 3.0 * GELU_B * x * x
    )
    saved[7] = decay * (-DECAY_SCALE * softness) * sig_r * (1.0 - sig_r)
    saved[8] = -(decay / root) * sig_a * values
    saved[9] = root * values * sig_a * (1.0 - sig_a)
    saved[10] = direct
    saved[11] = jnp.concatenate([w_recur[0], w_input[0]], axis=1).astype(F32)
    rows = in_three(ends_row(up_prod, down_prod, lane)) + in_three(
        ends_row(up_state, down_state, lane)
    )
    place = iota((8, tokens), 0)
    total = jnp.zeros((8, tokens), F32)
    for k, row in enumerate(rows):
        total = jnp.where(place == k, row.astype(F32), total)
    carry[...] = total.astype(BF)


def joined_states(saved, state_in, state_back):
    return saved[2] + saved[1] * state_in, saved[4] + saved[3] * state_back


def join_body(home, saved, mix, ends, adds):
    channels, tokens = mix.shape
    devices = adds.shape[0]
    rows = home.shape[0]
    lane = iota((channels, tokens), 1)
    offset = iota((devices, rows), 1) - HOME_ROWS * iota((devices, rows), 0)
    base = HOME_ROWS - 6
    prod_rows = ((offset >= base) & (offset < base + 3)).astype(F32).astype(BF)
    add_rows = ((offset >= base + 3) & (offset < base + 6)).astype(F32).astype(BF)
    prods = ends.at[channels:, :]
    prods[...] = dot(prod_rows, home[...])
    adds[...] = dot(add_rows, home[...])
    state_in, state_back = to_columns(fold(lax.axis_index("sp"), prods, adds, channels), lane)
    ends[:channels, :] = jnp.where(lane < channels, state_in, state_back)
    fwd, bwd = joined_states(saved, state_in, state_back)
    mix[...] = (saved[5] * (fwd + bwd)).astype(BF)


def proj_body(lifted, mix, mine, theirs):
    blocks, tokens, _ = lifted.shape
    channels = mix.shape[0]
    half = channels // 2
    part_rows = mine.shape[1]
    left = iota((half, 128), 1) < 64
    even = (lax.axis_index("sp") & 1) == 0
    mixed = mix[...]
    for k in range(blocks // 2):
        proj = dot(mixed, pair(lifted, k, 0, tokens))
        for q in range(2):
            part = proj[:, 128 * q : 128 * (q + 1)]
            top, bottom = part[:half], part[half:]
            spot = 4 * k + 2 * q
            first = jnp.where(left, top, pltpu.roll(bottom, 64, 1))
            second = jnp.where(left, pltpu.roll(top, 64, 1), bottom)
            for n, rows in enumerate((first, second)):
                low, high = rows[:part_rows], rows[part_rows:]
                mine[spot + n] = jnp.where(even, low, high)
                theirs[spot + n] = jnp.where(even, high, low).astype(BF)


def adjoint_body(lifted, w_out, saved, ends, far_kept, carry, kept, sem):
    blocks, tokens, _ = lifted.shape
    channels = w_out.shape[0]
    lane = iota((channels, tokens), 1)
    mix_cot = jnp.zeros((channels, tokens), F32)
    for k in range(blocks // 2):
        both = pair(lifted, k, 0, tokens)
        mix_cot = mix_cot + dot(w_out[:, 256 * k : 256 * (k + 1)], both, 1, 1)
    decay = saved[0]
    cot = mix_cot * saved[5]
    weighted = decay * cot
    _, up = scan(decay, weighted, lane, shift_in)
    _, down = scan(decay, weighted, lane, shift_out)
    kept[:channels] = mix_cot
    kept[channels : 2 * channels] = cot
    kept[2 * channels : 3 * channels] = up
    kept[3 * channels : 4 * channels] = down
    kept[4 * channels :] = ends[...]
    write = pltpu.make_async_copy(kept, far_kept, sem)
    write.start()
    rows = in_three(ends_row(up, down, lane))
    place = iota((8, tokens), 0)
    total = jnp.zeros((8, tokens), F32)
    for k, row in enumerate(rows):
        total = jnp.where(place == k, row.astype(F32), total)
    carry[...] = total
    write.wait()


def pack_body(mine, theirs, carry, far_out, out, sem):
    devices, part_rows, width = mine.shape
    tail = carry[...][:GROUP].astype(BF)
    for s in range(devices):
        rows = mine[s] + theirs[s].astype(F32)
        for k in range(part_rows // GROUP):
            group = rows[GROUP * k : GROUP * (k + 1)].astype(BF)
            out[s, :, width * k : width * (k + 1)] = group
        out[s, :, width * (part_rows // GROUP) :] = tail
    write = pltpu.make_async_copy(out, far_out, sem)
    write.start()
    write.wait()


def finish_body(far_kept, last, saved, g_proj, g_conv, g_branch, kept, adds, sems):
    (copy,) = fetch((far_kept,), (kept,), sems)
    devices = adds.shape[0]
    channels, tokens = g_conv.shape
    ends = kept.at[4 * channels :, :]
    prods = kept.at[5 * channels :, :]
    lane = iota((channels, tokens), 1)
    cut = last.shape[2] - 128
    totals = [jnp.zeros((GROUP, cut), F32)] * 2
    for s in range(devices):
        totals[s & 1] = totals[s & 1] + last[s, :, :cut].astype(F32)
        adds[s : s + 1, :] = jnp.sum(last[s, :, cut:].astype(F32), axis=0, keepdims=True)
    turned = jnp.concatenate(
        [total[:, k : k + 128] for total in totals for k in range(0, cut, 128)], axis=0
    ).T
    g_proj[...] = jnp.concatenate([turned[:64], turned[64:]], axis=1)
    copy.wait()
    adj_in, adj_back = to_columns(fold(lax.axis_index("sp"), prods, adds, channels), lane)
    state_in, state_back = ends[:channels, :1], ends[:channels, tokens - 1 :]
    fwd, bwd = joined_states(saved, state_in, state_back)
    before = jnp.where(lane == 0, state_in, pltpu.roll(fwd, 1, 1))
    after = jnp.where(lane == tokens - 1, state_back, pltpu.roll(bwd, tokens - 1, 1))
    cot = kept[channels : 2 * channels]
    up = kept[2 * channels : 3 * channels] + saved[1] * adj_in
    down = kept[3 * channels : 4 * channels] + saved[3] * adj_back
    past = cot + jnp.where(lane == 0, adj_in, pltpu.roll(up, 1, 1))
    future = cot + jnp.where(lane == tokens - 1, adj_back, pltpu.roll(down, tokens - 1, 1))
    drive_cot = past + future
    decay_cot = future * before + past * after + drive_cot * saved[8]
    recur_cot = decay_cot * saved[7]
    admit_cot = drive_cot * saved[9]
    exact = lax.Precision.HIGHEST
    g_conv[...] = (
        drive_cot * saved[10]
        + dot(saved[11], jnp.concatenate([recur_cot, admit_cot], axis=0), 1, 0, exact)
    )
    g_branch[...] = kept[:channels] * (fwd + bwd) * saved[6]


def local(
    residual,
    out_cot,
    routes,
    route_weight,
    w_gate,
    w_up,
    w_down,
    w_out,
    conv_out,
    gate_branch,
    w_recur,
    w_input,
    decay_param,
):
    experts = lax.axis_size("sp")
    blocks = lax.axis_size("tp")
    tokens, lanes = residual.shape
    capacity = 2 * tokens // experts + 2
    slots = experts * capacity
    hidden, width = w_gate.shape[1:]
    channels = conv_out.shape[0]

    def kernel(body, *static):
        def run(*refs):
            body(*static, *refs)

        return run

    sent, comb = call(
        kernel(dispatch_body, experts),
        [
            ((experts, GROUP, 2 * capacity // GROUP * lanes), BF),
            ((experts * HOME_ROWS, tokens), BF),
        ],
        (routes.T, route_weight.T, residual, out_cot),
        fetched=4,
    )
    got = lax.all_to_all(sent, "sp", split_axis=0, concat_axis=0, tiled=True)
    (spread,) = call(
        kernel(compact_body, experts, capacity),
        [((blocks, 2 * slots, lanes), BF)],
        (got,),
    )
    whole = lax.all_to_all(spread, "tp", 0, 0, tiled=True)
    dxp, acts, saved, carry = call(
        expert_body,
        [
            ((blocks, slots, lanes), BF),
            ((slots, 3 * hidden), BF),
            ((SAVED, channels, tokens), F32),
            ((8, tokens), BF),
        ],
        (
            conv_out,
            gate_branch,
            w_recur,
            w_input,
            decay_param.reshape(1, channels),
            whole,
            w_gate[0],
            w_up[0],
            w_down[0],
        ),
        fetched=5,
        scratch=(pltpu.VMEM((slots, 3 * hidden), BF), pltpu.SemaphoreType.DMA),
        far=(1,),
        flops=10 * slots * hidden * width,
    )
    parts = lax.all_to_all(dxp, "tp", 0, 0, tiled=True)
    (returned,) = call(
        kernel(owner_sum_body, experts, capacity),
        [((experts * HOME_ROWS, lanes), BF)],
        (parts, carry),
    )
    home = lax.all_to_all(
        returned.reshape(experts, HOME_ROWS, lanes), "sp", split_axis=0, concat_axis=0, tiled=True
    ).reshape(experts * HOME_ROWS, lanes)
    own, mix, ends = call(
        lift_body,
        [
            ((blocks, tokens, lanes), BF),
            ((channels, tokens), BF),
            ((channels + experts, tokens), F32),
        ],
        (home, comb, out_cot, saved),
        scratch=(pltpu.VMEM((experts, tokens), F32),),
    )
    lifted = lax.all_to_all(own, "tp", 0, 0, tiled=True)
    part_rows = channels // 4
    last_width = (part_rows // GROUP + 1) * lanes
    mine, theirs = call(
        proj_body,
        [((experts, part_rows, lanes), F32), ((experts, part_rows, lanes), BF)],
        (lifted, mix),
        flops=2 * channels * tokens * width,
    )
    swapped = lax.ppermute(theirs, "sp", [(i, i ^ 1) for i in range(experts)])
    kept, last_carry = call(
        adjoint_body,
        [((5 * channels + experts, tokens), F32), ((8, tokens), F32)],
        (lifted, w_out, saved, ends),
        flops=100 * channels * tokens * width,
        scratch=(pltpu.VMEM((5 * channels + experts, tokens), F32), pltpu.SemaphoreType.DMA),
        far=(0,),
    )
    (piece,) = call(
        pack_body,
        [((experts, GROUP, last_width), BF)],
        (mine, swapped, last_carry),
        scratch=(pltpu.VMEM((experts, GROUP, last_width), BF), pltpu.SemaphoreType.DMA),
        far=(0,),
    )
    piece, acts = lax.optimization_barrier((piece, acts))
    grads = expert_grads(whole, acts, width)
    last = lax.all_to_all(piece, "sp", split_axis=0, concat_axis=0, tiled=True)
    g_proj, g_conv, g_branch = call(
        finish_body,
        [((width // experts, channels), F32), ((channels, tokens), F32), ((channels, tokens), F32)],
        (kept, last, saved),
        fetched=1,
        scratch=(pltpu.VMEM((experts, tokens), F32),),
    )
    return (grads[0], grads[1], grads[2], g_proj, g_conv, g_branch)


def solution(mesh):
    return jax.shard_map(
        local,
        mesh=mesh,
        in_specs=(
            P("sp", "tp"),
            P("sp", "tp"),
            P("sp", None),
            P("sp", None),
            P("sp", "tp", None),
            P("sp", "tp", None),
            P("sp", "tp", None),
            P("tp", None),
            P("tp", "sp"),
            P("tp", "sp"),
            P("tp", None, None),
            P("tp", None, None),
            P("tp"),
        ),
        out_specs=(
            P("sp", "tp", None),
            P("sp", "tp", None),
            P("sp", "tp", None),
            P("sp", "tp"),
            P("tp", "sp"),
            P("tp", "sp"),
        ),
        check_vma=False,
    )
```

```python
import jax
import jax.numpy as jnp
from jax import lax
from jax.experimental import pallas as pl
from jax.experimental.pallas import tpu as pltpu
from jax.sharding import PartitionSpec as P

LEAK = 0.01
DECAY_SCALE = 8.0
GELU_A = 0.7978845608028654
GELU_B = 0.044715

BF = jnp.bfloat16
F32 = jnp.float32
I32 = jnp.int32

HOME_ROWS = 16
GROUP = 4


def iota(shape, dim):
    return lax.broadcasted_iota(I32, shape, dim)


def dot(a, b, ca=1, cb=0, precision=None):
    return lax.dot_general(
        a, b, (((ca,), (cb,)), ((), ())), precision=precision, preferred_element_type=F32
    )


def call(body, outs, args, flops=1, bytes_moved=1, fetched=0, scratch=(), far=()):
    specs = [pl.BlockSpec(memory_space=pltpu.HBM)] * fetched
    specs += [pl.BlockSpec(memory_space=pltpu.VMEM)] * (len(args) - fetched)
    scratch = [pltpu.VMEM(a.shape, a.dtype) for a in args[:fetched]] + list(scratch)
    kept = [pltpu.with_memory_space_constraint(a, pltpu.HBM) for a in args[:fetched]]
    args = kept + list(args[fetched:])
    if fetched:
        scratch.append(pltpu.SemaphoreType.DMA((fetched,)))
    return pl.pallas_call(
        body,
        out_shape=[
            pltpu.HBM(*out) if k in far else jax.ShapeDtypeStruct(*out)
            for k, out in enumerate(outs)
        ],
        in_specs=specs,
        out_specs=[
            pl.BlockSpec(memory_space=pltpu.HBM if k in far else pltpu.VMEM)
            for k in range(len(outs))
        ],
        scratch_shapes=scratch,
        compiler_params=pltpu.CompilerParams(vmem_limit_bytes=24 * 1024 * 1024),
        cost_estimate=pl.CostEstimate(
            flops=flops, bytes_accessed=bytes_moved, transcendentals=0
        ),
    )(*args)


def fetch(sources, targets, sems):
    copies = [
        pltpu.make_async_copy(source, target, sems.at[k])
        for k, (source, target) in enumerate(zip(sources, targets))
    ]
    for copy in copies:
        copy.start()
    return copies


def dispatch_body(experts, *refs):
    sources, (sent, comb), targets, sems = refs[:4], refs[4:6], refs[6:10], refs[10]
    for copy in fetch(sources, targets, sems):
        copy.wait()
    routes, weight, residual, cot = targets
    tokens = residual.shape[0]
    first, second = routes[0:1, :], routes[1:2, :]
    expert = iota((experts, tokens), 0)
    hit0 = (expert == first).astype(F32)
    hit1 = (expert == second).astype(F32)
    earlier = (iota((tokens, tokens), 0) < iota((tokens, tokens), 1)).astype(BF)
    before = dot((hit0 + hit1).astype(BF), earlier)
    slot0 = jnp.sum(before * hit0, axis=0, keepdims=True).astype(I32)
    slot1 = jnp.sum((before + hit0) * hit1, axis=0, keepdims=True).astype(I32)
    back = iota((experts * HOME_ROWS, tokens), 0)
    at_home = (back == first * HOME_ROWS + slot0) | (back == second * HOME_ROWS + slot1)
    comb[...] = at_home.astype(F32).astype(BF)
    count = sent.shape[2] // tokens
    capacity = GROUP * count // 2
    row = iota((experts * GROUP, tokens), 0)
    place0 = first * 2 * capacity + slot0
    place1 = second * 2 * capacity + slot1
    spot = (row & (GROUP - 1)) + (row >> 2) * 2 * capacity
    for k in range(count):
        here = spot + GROUP * k
        in_rows = ((here == place0) | (here == place1)).astype(F32).astype(BF)
        cot0 = here == place0 + capacity
        cot1 = here == place1 + capacity
        factor = jnp.sum(
            jnp.where(cot0, weight[0:1, :], 0.0) + jnp.where(cot1, weight[1:2, :], 0.0),
            axis=1,
            keepdims=True,
        )
        cot_rows = (cot0 | cot1).astype(F32).astype(BF)
        rows = dot(in_rows, residual[...]) + factor * dot(cot_rows, cot[...])
        for e in range(experts):
            sent[e, :, tokens * k : tokens * (k + 1)] = rows[GROUP * e : GROUP * (e + 1)].astype(BF)


def compact_body(experts, capacity, got, out):
    slots = experts * capacity
    lanes = out.shape[2]
    count = got.shape[2] // lanes
    blocks = [
        jnp.concatenate(
            [got[e, :, lanes * k : lanes * (k + 1)].astype(F32) for e in range(experts)], axis=0
        )
        for k in range(count)
    ]
    row = iota((2 * slots, 1), 0)
    half = (row >= slots).astype(I32)
    rest = row - half * slots
    source = jnp.floor((rest.astype(F32) + 0.5) * (1.0 / capacity)).astype(I32)
    inner = half * capacity + (rest - source * capacity)
    target = (inner >> 2) * experts * GROUP + source * GROUP + (inner & (GROUP - 1))
    total = count * experts * GROUP
    pick = (iota((2 * slots, total), 1) == target).astype(F32).astype(BF)
    rows = dot(pick, jnp.concatenate(blocks, axis=0).astype(BF)).astype(BF)
    for j in range(out.shape[0]):
        out[j] = rows


def pair(ref, k, lo, hi):
    return jnp.concatenate([ref[2 * k, lo:hi, :], ref[2 * k + 1, lo:hi, :]], axis=1)


def expert_body(*refs):
    sources, (whole, w_gate, w_up, w_down) = refs[:5], refs[5:9]
    dxp, far_acts, saved, carry = refs[9:13]
    targets, acts, acts_sem, sems = refs[13:18], refs[18], refs[19], refs[20]
    copies = fetch(sources, targets, sems)
    slots = whole.shape[1] // 2
    blocks = whole.shape[0]
    hidden = w_gate.shape[0]
    pre = jnp.zeros((slots, 2 * hidden), F32)
    act_cot = jnp.zeros((slots, hidden), F32)
    for k in range(blocks // 2):
        cols = slice(256 * k, 256 * (k + 1))
        both = jnp.concatenate([w_gate[:, cols], w_up[:, cols]], axis=0)
        pre = pre + dot(pair(whole, k, 0, slots), both, 1, 1)
        act_cot = act_cot + dot(pair(whole, k, slots, 2 * slots), w_down[:, cols], 1, 1)
    pre_gate, pre_up = pre[:, :hidden], pre[:, hidden:]
    sig = jax.nn.sigmoid(pre_gate)
    silu = pre_gate * sig
    slope = sig * (1.0 + pre_gate * (1.0 - sig))
    act = (silu * pre_up).astype(BF)
    gate_cot = (act_cot * pre_up * slope).astype(BF)
    up_cot = (act_cot * silu).astype(BF)
    cots = jnp.concatenate([gate_cot, up_cot], axis=1)
    acts[:, : 2 * hidden] = cots
    acts[:, 2 * hidden :] = act
    write = pltpu.make_async_copy(acts, far_acts, acts_sem)
    write.start()
    for k in range(blocks // 2):
        cols = slice(256 * k, 256 * (k + 1))
        both = jnp.concatenate([w_gate[:, cols], w_up[:, cols]], axis=0)
        part = dot(cots, both).astype(BF)
        dxp[2 * k] = part[:, :128]
        dxp[2 * k + 1] = part[:, 128:]
    for copy in copies:
        copy.wait()
    state_body(*targets, saved, carry)
    write.wait()


def grads_body(whole, acts, g_gate, g_up, g_down):
    slots = whole.shape[1] // 2
    hidden = acts.shape[1] // 3
    both = dot(acts[:, : 2 * hidden], pair(whole, 0, 0, slots), 0, 0).astype(BF)
    g_gate[0] = both[:hidden]
    g_up[0] = both[hidden:]
    g_down[0] = dot(acts[:, 2 * hidden :], pair(whole, 0, slots, 2 * slots), 0, 0).astype(BF)


def expert_grads(whole, acts, width):
    blocks, rows, lanes = whole.shape
    hidden = acts.shape[1] // 3
    out = jax.ShapeDtypeStruct((1, hidden, width), BF)
    spec = pl.BlockSpec((1, hidden, 2 * lanes), lambda i: (0, 0, i))
    return pl.pallas_call(
        grads_body,
        grid=(blocks // 2,),
        out_shape=[out] * 3,
        in_specs=[
            pl.BlockSpec((2, rows, lanes), lambda i: (i, 0, 0)),
            pl.BlockSpec(acts.shape, lambda i: (0, 0)),
        ],
        out_specs=[spec] * 3,
        compiler_params=pltpu.CompilerParams(vmem_limit_bytes=16 * 1024 * 1024),
        cost_estimate=pl.CostEstimate(
            flops=3 * rows * hidden * width, bytes_accessed=6 * hidden * width, transcendentals=0
        ),
    )(whole, acts)


def owner_sum_body(experts, capacity, parts, carry, out):
    total = parts[0].astype(F32)
    for j in range(1, parts.shape[0]):
        total = total + parts[j].astype(F32)
    total = total.astype(BF)
    rows = experts * HOME_ROWS
    place = iota((rows, 1), 0)
    inner = place & (HOME_ROWS - 1)
    source = jnp.where(inner < capacity, (place >> 4) * capacity + inner, -1)
    pick = (iota((rows, experts * capacity), 1) == source).astype(F32).astype(BF)
    extra = (iota((rows, carry.shape[0]), 1) == inner - capacity).astype(F32).astype(BF)
    out[...] = (dot(pick, total) + dot(extra, carry[...])).astype(BF)


def lift_body(home, comb, cot, saved, out, mix, ends, adds):
    grad = dot(comb[...], home[...], 0, 0)
    lifted = (cot[...].astype(F32) + grad).astype(BF)
    for j in range(out.shape[0]):
        out[j] = lifted
    join_body(home, saved, mix, ends, adds)


def shift_in(x, d, fill, lane):
    return jnp.where(lane >= d, pltpu.roll(x, d, 1), fill)


def shift_out(x, d, fill, lane):
    width = x.shape[1]
    return jnp.where(lane < width - d, pltpu.roll(x, width - d, 1), fill)


def scan(decay, drive, lane, moved):
    d = 1
    while d < decay.shape[1]:
        drive = decay * moved(drive, d, 0.0, lane) + drive
        decay = decay * moved(decay, d, 1.0, lane)
        d *= 2
    return decay, drive


def in_three(x):
    high = x.astype(BF)
    rest = x - high.astype(F32)
    mid = rest.astype(BF)
    low = (rest - mid.astype(F32)).astype(BF)
    return high, mid, low


def ends_row(up, down, lane):
    width = up.shape[1]
    ends = jnp.concatenate(
        [jnp.where(lane == width - 1, up, 0.0), jnp.where(lane == 0, down, 0.0)], axis=0
    )
    return dot(jnp.ones((8, width), F32), ends, 1, 1, lax.Precision.HIGHEST)


def to_columns(row, lane):
    channel = iota(lane.shape, 0)
    channels = lane.shape[0]
    up = jnp.sum(jnp.where(lane == channel, row, 0.0), axis=1, keepdims=True)
    down = jnp.sum(jnp.where(lane == channel + channels, row, 0.0), axis=1, keepdims=True)
    return up, down


def fold(me, prods, adds, channels):
    devices, width = prods.shape
    lane = iota((1, width), 1)
    ahead = lane < channels
    total = jnp.zeros((1, width), F32)
    for n in range(devices):
        m = devices - 1 - n
        prod = jnp.where(ahead, prods[n : n + 1, :], prods[m : m + 1, :])
        add = jnp.where(ahead, adds[n : n + 1, :], adds[m : m + 1, :])
        live = jnp.where(ahead, (me > n).astype(I32), (me < m).astype(I32)) > 0
        total = jnp.where(live, prod * total + add, total)
    return total


SAVED = 12
KEPT = 6


def soft_plus(x):
    small = jnp.exp(-jnp.abs(x))
    z = small / (2.0 + small)
    square = z * z
    series = jnp.full_like(z, 1.0 / 19.0)
    for odd in (17, 15, 13, 11, 9, 7, 5, 3, 1):
        series = series * square + 1.0 / odd
    return jnp.maximum(x, 0.0) + 2.0 * z * series


def state_body(conv, branch, w_recur, w_input, decay_param, saved, carry):
    channels, tokens = conv.shape
    lane = iota((channels, tokens), 1)
    eye = iota((channels, channels), 0) == iota((channels, channels), 1)
    softness = jnp.sum(jnp.where(eye, soft_plus(-decay_param[...]), 0.0), axis=1, keepdims=True)
    values = conv[...].astype(F32)
    sig_r = jax.nn.sigmoid(dot(w_recur[0], conv[...], 0, 0))
    sig_a = jax.nn.sigmoid(dot(w_input[0], conv[...], 0, 0))
    decay = jnp.exp(-DECAY_SCALE * sig_r * softness)
    root = jnp.sqrt(1.0 - decay * decay + LEAK)
    direct = root * sig_a
    drive = direct * values
    up_prod, up_state = scan(decay, drive, lane, shift_in)
    down_prod, down_state = scan(decay, drive, lane, shift_out)
    x = branch[...].astype(F32)
    th = jnp.tanh(GELU_A * (x + GELU_B * x * x * x))
    saved[0] = decay
    saved[1] = up_prod
    saved[2] = up_state
    saved[3] = down_prod
    saved[4] = down_state
    saved[5] = 0.5 * x * (1.0 + th)
    saved[6] = 0.5 * (1.0 + th) + 0.5 * x * (1.0 - th * th) * GELU_A * (
        1.0 + 3.0 * GELU_B * x * x
    )
    saved[7] = decay * (-DECAY_SCALE * softness) * sig_r * (1.0 - sig_r)
    saved[8] = -(decay / root) * sig_a * values
    saved[9] = root * values * sig_a * (1.0 - sig_a)
    saved[10] = direct
    saved[11] = jnp.concatenate([w_recur[0], w_input[0]], axis=1).astype(F32)
    rows = in_three(ends_row(up_prod, down_prod, lane)) + in_three(
        ends_row(up_state, down_state, lane)
    )
    place = iota((8, tokens), 0)
    total = jnp.zeros((8, tokens), F32)
    for k, row in enumerate(rows):
        total = jnp.where(place == k, row.astype(F32), total)
    carry[...] = total.astype(BF)


def joined_states(saved, state_in, state_back):
    return saved[2] + saved[1] * state_in, saved[4] + saved[3] * state_back


def join_body(home, saved, mix, ends, adds):
    channels, tokens = mix.shape
    devices = adds.shape[0]
    rows = home.shape[0]
    lane = iota((channels, tokens), 1)
    offset = iota((devices, rows), 1) - HOME_ROWS * iota((devices, rows), 0)
    base = HOME_ROWS - 6
    prod_rows = ((offset >= base) & (offset < base + 3)).astype(F32).astype(BF)
    add_rows = ((offset >= base + 3) & (offset < base + 6)).astype(F32).astype(BF)
    prods = ends.at[channels:, :]
    prods[...] = dot(prod_rows, home[...])
    adds[...] = dot(add_rows, home[...])
    state_in, state_back = to_columns(fold(lax.axis_index("sp"), prods, adds, channels), lane)
    ends[:channels, :] = jnp.where(lane < channels, state_in, state_back)
    fwd, bwd = joined_states(saved, state_in, state_back)
    mix[...] = (saved[5] * (fwd + bwd)).astype(BF)


def proj_body(lifted, mix, mine, theirs):
    blocks, tokens, _ = lifted.shape
    channels = mix.shape[0]
    half = channels // 2
    part_rows = mine.shape[1]
    left = iota((half, 128), 1) < 64
    even = (lax.axis_index("sp") & 1) == 0
    mixed = mix[...]
    for k in range(blocks // 2):
        proj = dot(mixed, pair(lifted, k, 0, tokens))
        for q in range(2):
            part = proj[:, 128 * q : 128 * (q + 1)]
            top, bottom = part[:half], part[half:]
            spot = 4 * k + 2 * q
            first = jnp.where(left, top, pltpu.roll(bottom, 64, 1))
            second = jnp.where(left, pltpu.roll(top, 64, 1), bottom)
            for n, rows in enumerate((first, second)):
                low, high = rows[:part_rows], rows[part_rows:]
                mine[spot + n] = jnp.where(even, low, high)
                theirs[spot + n] = jnp.where(even, high, low).astype(BF)


def adjoint_body(lifted, w_out, saved, ends, kept):
    blocks, tokens, _ = lifted.shape
    channels = w_out.shape[0]
    lane = iota((channels, tokens), 1)
    mix_cot = jnp.zeros((channels, tokens), F32)
    for k in range(blocks // 2):
        both = pair(lifted, k, 0, tokens)
        mix_cot = mix_cot + dot(w_out[:, 256 * k : 256 * (k + 1)], both, 1, 1)
    decay = saved[0]
    cot = mix_cot * saved[5]
    weighted = decay * cot
    _, up = scan(decay, weighted, lane, shift_in)
    _, down = scan(decay, weighted, lane, shift_out)
    kept[:channels] = mix_cot
    kept[channels : 2 * channels] = cot
    kept[2 * channels : 3 * channels] = up
    kept[3 * channels : 4 * channels] = down
    kept[4 * channels : 4 * channels + ends.shape[0]] = ends[...]
    rows = in_three(ends_row(up, down, lane))
    place = iota((8, tokens), 0)
    total = jnp.zeros((8, tokens), F32)
    for k, row in enumerate(rows):
        total = jnp.where(place == k, row.astype(F32), total)
    kept[kept.shape[0] - 8 :] = total


def pack_body(mine, theirs, kept, far_out, out, sem):
    devices, part_rows, width = mine.shape
    spot = kept.shape[0] - 8
    tail = kept[spot : spot + 8][:GROUP].astype(BF)
    for s in range(devices):
        rows = mine[s] + theirs[s].astype(F32)
        for k in range(part_rows // GROUP):
            group = rows[GROUP * k : GROUP * (k + 1)].astype(BF)
            out[s, :, width * k : width * (k + 1)] = group
        out[s, :, width * (part_rows // GROUP) :] = tail
    write = pltpu.make_async_copy(out, far_out, sem)
    write.start()
    write.wait()


def finish_body(last, saved, kept, g_proj, g_conv, g_branch, adds):
    devices = adds.shape[0]
    channels, tokens = g_conv.shape
    ends = kept.at[4 * channels :, :]
    prods = kept.at[5 * channels : 5 * channels + devices, :]
    lane = iota((channels, tokens), 1)
    cut = last.shape[2] - 128
    totals = [jnp.zeros((GROUP, cut), F32)] * 2
    for s in range(devices):
        totals[s & 1] = totals[s & 1] + last[s, :, :cut].astype(F32)
        adds[s : s + 1, :] = jnp.sum(last[s, :, cut:].astype(F32), axis=0, keepdims=True)
    turned = jnp.concatenate(
        [total[:, k : k + 128] for total in totals for k in range(0, cut, 128)], axis=0
    ).T
    g_proj[...] = jnp.concatenate([turned[:64], turned[64:]], axis=1)
    adj_in, adj_back = to_columns(fold(lax.axis_index("sp"), prods, adds, channels), lane)
    state_in, state_back = ends[:channels, :1], ends[:channels, tokens - 1 :]
    fwd, bwd = joined_states(saved, state_in, state_back)
    before = jnp.where(lane == 0, state_in, pltpu.roll(fwd, 1, 1))
    after = jnp.where(lane == tokens - 1, state_back, pltpu.roll(bwd, tokens - 1, 1))
    cot = kept[channels : 2 * channels]
    up = kept[2 * channels : 3 * channels] + saved[1] * adj_in
    down = kept[3 * channels : 4 * channels] + saved[3] * adj_back
    past = cot + jnp.where(lane == 0, adj_in, pltpu.roll(up, 1, 1))
    future = cot + jnp.where(lane == tokens - 1, adj_back, pltpu.roll(down, tokens - 1, 1))
    drive_cot = past + future
    decay_cot = future * before + past * after + drive_cot * saved[8]
    recur_cot = decay_cot * saved[7]
    admit_cot = drive_cot * saved[9]
    exact = lax.Precision.HIGHEST
    g_conv[...] = (
        drive_cot * saved[10]
        + dot(saved[11], jnp.concatenate([recur_cot, admit_cot], axis=0), 1, 0, exact)
    )
    g_branch[...] = kept[:channels] * (fwd + bwd) * saved[6]


def local(
    residual,
    out_cot,
    routes,
    route_weight,
    w_gate,
    w_up,
    w_down,
    w_out,
    conv_out,
    gate_branch,
    w_recur,
    w_input,
    decay_param,
):
    experts = lax.axis_size("sp")
    blocks = lax.axis_size("tp")
    tokens, lanes = residual.shape
    capacity = 2 * tokens // experts + 2
    slots = experts * capacity
    hidden, width = w_gate.shape[1:]
    channels = conv_out.shape[0]

    def kernel(body, *static):
        def run(*refs):
            body(*static, *refs)

        return run

    sent, comb = call(
        kernel(dispatch_body, experts),
        [
            ((experts, GROUP, 2 * capacity // GROUP * lanes), BF),
            ((experts * HOME_ROWS, tokens), BF),
        ],
        (routes.T, route_weight.T, residual, out_cot),
        fetched=4,
    )
    got = lax.all_to_all(sent, "sp", split_axis=0, concat_axis=0, tiled=True)
    (spread,) = call(
        kernel(compact_body, experts, capacity),
        [((blocks, 2 * slots, lanes), BF)],
        (got,),
    )
    whole = lax.all_to_all(spread, "tp", 0, 0, tiled=True)
    dxp, acts, saved, carry = call(
        expert_body,
        [
            ((blocks, slots, lanes), BF),
            ((slots, 3 * hidden), BF),
            ((SAVED, channels, tokens), F32),
            ((8, tokens), BF),
        ],
        (
            conv_out,
            gate_branch,
            w_recur,
            w_input,
            decay_param.reshape(1, channels),
            whole,
            w_gate[0],
            w_up[0],
            w_down[0],
        ),
        fetched=5,
        scratch=(pltpu.VMEM((slots, 3 * hidden), BF), pltpu.SemaphoreType.DMA),
        far=(1,),
        flops=10 * slots * hidden * width,
    )
    parts = lax.all_to_all(dxp, "tp", 0, 0, tiled=True)
    (returned,) = call(
        kernel(owner_sum_body, experts, capacity),
        [((experts * HOME_ROWS, lanes), BF)],
        (parts, carry),
    )
    home = lax.all_to_all(
        returned.reshape(experts, HOME_ROWS, lanes), "sp", split_axis=0, concat_axis=0, tiled=True
    ).reshape(experts * HOME_ROWS, lanes)
    own, mix, ends = call(
        lift_body,
        [
            ((blocks, tokens, lanes), BF),
            ((channels, tokens), BF),
            ((channels + experts, tokens), F32),
        ],
        (home, comb, out_cot, saved),
        scratch=(pltpu.VMEM((experts, tokens), F32),),
    )
    lifted = lax.all_to_all(own, "tp", 0, 0, tiled=True)
    part_rows = channels // 4
    last_width = (part_rows // GROUP + 1) * lanes
    mine, theirs = call(
        proj_body,
        [((experts, part_rows, lanes), F32), ((experts, part_rows, lanes), BF)],
        (lifted, mix),
        flops=2 * channels * tokens * width,
    )
    swapped = lax.ppermute(theirs, "sp", [(i, i ^ 1) for i in range(experts)])
    (kept,) = call(
        adjoint_body,
        [((KEPT * channels, tokens), F32)],
        (lifted, w_out, saved, ends),
        flops=100 * channels * tokens * width,
    )
    (piece,) = call(
        pack_body,
        [((experts, GROUP, last_width), BF)],
        (mine, swapped, kept),
        scratch=(pltpu.VMEM((experts, GROUP, last_width), BF), pltpu.SemaphoreType.DMA),
        far=(0,),
    )
    piece, acts = lax.optimization_barrier((piece, acts))
    grads = expert_grads(whole, acts, width)
    last = lax.all_to_all(piece, "sp", split_axis=0, concat_axis=0, tiled=True)
    g_proj, g_conv, g_branch = call(
        finish_body,
        [((width // experts, channels), F32), ((channels, tokens), F32), ((channels, tokens), F32)],
        (last, saved, kept),
        scratch=(pltpu.VMEM((experts, tokens), F32),),
    )
    return (grads[0], grads[1], grads[2], g_proj, g_conv, g_branch)


def solution(mesh):
    return jax.shard_map(
        local,
        mesh=mesh,
        in_specs=(
            P("sp", "tp"),
            P("sp", "tp"),
            P("sp", None),
            P("sp", None),
            P("sp", "tp", None),
            P("sp", "tp", None),
            P("sp", "tp", None),
            P("tp", None),
            P("tp", "sp"),
            P("tp", "sp"),
            P("tp", None, None),
            P("tp", None, None),
            P("tp"),
        ),
        out_specs=(
            P("sp", "tp", None),
            P("sp", "tp", None),
            P("sp", "tp", None),
            P("sp", "tp"),
            P("tp", "sp"),
            P("tp", "sp"),
        ),
        check_vma=False,
    )
```

```python
import jax
import jax.numpy as jnp
from jax import lax
from jax.experimental import pallas as pl
from jax.experimental.pallas import tpu as pltpu
from jax.sharding import PartitionSpec as P

LEAK = 0.01
DECAY_SCALE = 8.0
GELU_A = 0.7978845608028654
GELU_B = 0.044715

BF = jnp.bfloat16
F32 = jnp.float32
I32 = jnp.int32

HOME_ROWS = 16
GROUP = 4


def iota(shape, dim):
    return lax.broadcasted_iota(I32, shape, dim)


def dot(a, b, ca=1, cb=0, precision=None):
    return lax.dot_general(
        a, b, (((ca,), (cb,)), ((), ())), precision=precision, preferred_element_type=F32
    )


def call(body, outs, args, flops=1, bytes_moved=1, fetched=0, scratch=(), far=()):
    specs = [pl.BlockSpec(memory_space=pltpu.HBM)] * fetched
    specs += [pl.BlockSpec(memory_space=pltpu.VMEM)] * (len(args) - fetched)
    scratch = [pltpu.VMEM(a.shape, a.dtype) for a in args[:fetched]] + list(scratch)
    kept = [pltpu.with_memory_space_constraint(a, pltpu.HBM) for a in args[:fetched]]
    args = kept + list(args[fetched:])
    if fetched:
        scratch.append(pltpu.SemaphoreType.DMA((fetched,)))
    return pl.pallas_call(
        body,
        out_shape=[
            pltpu.HBM(*out) if k in far else jax.ShapeDtypeStruct(*out)
            for k, out in enumerate(outs)
        ],
        in_specs=specs,
        out_specs=[
            pl.BlockSpec(memory_space=pltpu.HBM if k in far else pltpu.VMEM)
            for k in range(len(outs))
        ],
        scratch_shapes=scratch,
        compiler_params=pltpu.CompilerParams(vmem_limit_bytes=24 * 1024 * 1024),
        cost_estimate=pl.CostEstimate(
            flops=flops, bytes_accessed=bytes_moved, transcendentals=0
        ),
    )(*args)


def fetch(sources, targets, sems):
    copies = [
        pltpu.make_async_copy(source, target, sems.at[k])
        for k, (source, target) in enumerate(zip(sources, targets))
    ]
    for copy in copies:
        copy.start()
    return copies


def dispatch_body(experts, *refs):
    sources, (sent, comb), targets, sems = refs[:4], refs[4:6], refs[6:10], refs[10]
    for copy in fetch(sources, targets, sems):
        copy.wait()
    routes, weight, residual, cot = targets
    tokens = residual.shape[0]
    first, second = routes[0:1, :], routes[1:2, :]
    expert = iota((experts, tokens), 0)
    hit0 = (expert == first).astype(F32)
    hit1 = (expert == second).astype(F32)
    earlier = (iota((tokens, tokens), 0) < iota((tokens, tokens), 1)).astype(BF)
    before = dot((hit0 + hit1).astype(BF), earlier)
    slot0 = jnp.sum(before * hit0, axis=0, keepdims=True).astype(I32)
    slot1 = jnp.sum((before + hit0) * hit1, axis=0, keepdims=True).astype(I32)
    back = iota((experts * HOME_ROWS, tokens), 0)
    at_home = (back == first * HOME_ROWS + slot0) | (back == second * HOME_ROWS + slot1)
    comb[...] = at_home.astype(F32).astype(BF)
    count = sent.shape[2] // tokens
    capacity = GROUP * count // 2
    row = iota((experts * GROUP, tokens), 0)
    place0 = first * 2 * capacity + slot0
    place1 = second * 2 * capacity + slot1
    spot = (row & (GROUP - 1)) + (row >> 2) * 2 * capacity
    for k in range(count):
        here = spot + GROUP * k
        in_rows = ((here == place0) | (here == place1)).astype(F32).astype(BF)
        cot0 = here == place0 + capacity
        cot1 = here == place1 + capacity
        factor = jnp.sum(
            jnp.where(cot0, weight[0:1, :], 0.0) + jnp.where(cot1, weight[1:2, :], 0.0),
            axis=1,
            keepdims=True,
        )
        cot_rows = (cot0 | cot1).astype(F32).astype(BF)
        rows = dot(in_rows, residual[...]) + factor * dot(cot_rows, cot[...])
        for e in range(experts):
            sent[e, :, tokens * k : tokens * (k + 1)] = rows[GROUP * e : GROUP * (e + 1)].astype(BF)


def compact_body(experts, capacity, got, out):
    slots = experts * capacity
    lanes = out.shape[2]
    count = got.shape[2] // lanes
    blocks = [
        jnp.concatenate(
            [got[e, :, lanes * k : lanes * (k + 1)].astype(F32) for e in range(experts)], axis=0
        )
        for k in range(count)
    ]
    row = iota((2 * slots, 1), 0)
    half = (row >= slots).astype(I32)
    rest = row - half * slots
    source = jnp.floor((rest.astype(F32) + 0.5) * (1.0 / capacity)).astype(I32)
    inner = half * capacity + (rest - source * capacity)
    target = (inner >> 2) * experts * GROUP + source * GROUP + (inner & (GROUP - 1))
    total = count * experts * GROUP
    pick = (iota((2 * slots, total), 1) == target).astype(F32).astype(BF)
    rows = dot(pick, jnp.concatenate(blocks, axis=0).astype(BF)).astype(BF)
    for j in range(out.shape[0]):
        out[j] = rows


def pair(ref, k, lo, hi):
    return jnp.concatenate([ref[2 * k, lo:hi, :], ref[2 * k + 1, lo:hi, :]], axis=1)


def expert_body(*refs):
    sources, (whole, w_gate, w_up, w_down) = refs[:5], refs[5:9]
    dxp, far_acts, saved, carry = refs[9:13]
    targets, acts, acts_sem, sems = refs[13:18], refs[18], refs[19], refs[20]
    copies = fetch(sources, targets, sems)
    slots = whole.shape[1] // 2
    blocks = whole.shape[0]
    hidden = w_gate.shape[0]
    pre = jnp.zeros((slots, 2 * hidden), F32)
    act_cot = jnp.zeros((slots, hidden), F32)
    for k in range(blocks // 2):
        cols = slice(256 * k, 256 * (k + 1))
        both = jnp.concatenate([w_gate[:, cols], w_up[:, cols]], axis=0)
        pre = pre + dot(pair(whole, k, 0, slots), both, 1, 1)
        act_cot = act_cot + dot(pair(whole, k, slots, 2 * slots), w_down[:, cols], 1, 1)
    pre_gate, pre_up = pre[:, :hidden], pre[:, hidden:]
    sig = jax.nn.sigmoid(pre_gate)
    silu = pre_gate * sig
    slope = sig * (1.0 + pre_gate * (1.0 - sig))
    act = (silu * pre_up).astype(BF)
    gate_cot = (act_cot * pre_up * slope).astype(BF)
    up_cot = (act_cot * silu).astype(BF)
    cots = jnp.concatenate([gate_cot, up_cot], axis=1)
    acts[:, : 2 * hidden] = cots
    acts[:, 2 * hidden :] = act
    write = pltpu.make_async_copy(acts, far_acts, acts_sem)
    write.start()
    for k in range(blocks // 2):
        cols = slice(256 * k, 256 * (k + 1))
        both = jnp.concatenate([w_gate[:, cols], w_up[:, cols]], axis=0)
        part = dot(cots, both).astype(BF)
        dxp[2 * k] = part[:, :128]
        dxp[2 * k + 1] = part[:, 128:]
    for copy in copies:
        copy.wait()
    state_body(*targets, saved, carry)
    write.wait()


def grads_body(whole, acts, g_gate, g_up, g_down):
    slots = whole.shape[1] // 2
    hidden = acts.shape[1] // 3
    both = dot(acts[:, : 2 * hidden], pair(whole, 0, 0, slots), 0, 0).astype(BF)
    g_gate[0] = both[:hidden]
    g_up[0] = both[hidden:]
    g_down[0] = dot(acts[:, 2 * hidden :], pair(whole, 0, slots, 2 * slots), 0, 0).astype(BF)


def expert_grads(whole, acts, width):
    blocks, rows, lanes = whole.shape
    hidden = acts.shape[1] // 3
    out = jax.ShapeDtypeStruct((1, hidden, width), BF)
    spec = pl.BlockSpec((1, hidden, 2 * lanes), lambda i: (0, 0, i))
    return pl.pallas_call(
        grads_body,
        grid=(blocks // 2,),
        out_shape=[out] * 3,
        in_specs=[
            pl.BlockSpec((2, rows, lanes), lambda i: (i, 0, 0)),
            pl.BlockSpec(acts.shape, lambda i: (0, 0)),
        ],
        out_specs=[spec] * 3,
        compiler_params=pltpu.CompilerParams(vmem_limit_bytes=16 * 1024 * 1024),
        cost_estimate=pl.CostEstimate(
            flops=3 * rows * hidden * width, bytes_accessed=6 * hidden * width, transcendentals=0
        ),
    )(whole, acts)


def owner_sum_body(experts, capacity, parts, carry, out):
    total = parts[0].astype(F32)
    for j in range(1, parts.shape[0]):
        total = total + parts[j].astype(F32)
    total = total.astype(BF)
    rows = experts * HOME_ROWS
    place = iota((rows, 1), 0)
    inner = place & (HOME_ROWS - 1)
    source = jnp.where(inner < capacity, (place >> 4) * capacity + inner, -1)
    pick = (iota((rows, experts * capacity), 1) == source).astype(F32).astype(BF)
    extra = (iota((rows, carry.shape[0]), 1) == inner - capacity).astype(F32).astype(BF)
    out[...] = (dot(pick, total) + dot(extra, carry[...])).astype(BF)


def lift_body(home, comb, cot, saved, out, mix, ends, adds):
    grad = dot(comb[...], home[...], 0, 0)
    lifted = (cot[...].astype(F32) + grad).astype(BF)
    for j in range(out.shape[0]):
        out[j] = lifted
    join_body(home, saved, mix, ends, adds)


def shift_in(x, d, fill, lane):
    return jnp.where(lane >= d, pltpu.roll(x, d, 1), fill)


def shift_out(x, d, fill, lane):
    width = x.shape[1]
    return jnp.where(lane < width - d, pltpu.roll(x, width - d, 1), fill)


def scan(decay, drive, lane, moved):
    d = 1
    while d < decay.shape[1]:
        drive = decay * moved(drive, d, 0.0, lane) + drive
        decay = decay * moved(decay, d, 1.0, lane)
        d *= 2
    return decay, drive


def in_three(x):
    high = x.astype(BF)
    rest = x - high.astype(F32)
    mid = rest.astype(BF)
    low = (rest - mid.astype(F32)).astype(BF)
    return high, mid, low


def ends_rows(up, down, lane):
    width = up.shape[1]
    ends = jnp.concatenate(
        [jnp.where(lane == width - 1, up, 0.0), jnp.where(lane == 0, down, 0.0)], axis=0
    )
    ones = jnp.ones((8, width), BF)
    return [dot(ones, piece, 1, 1) for piece in in_three(ends)]


def stacked(rows, width):
    place = iota((8, width), 0)
    total = jnp.zeros((8, width), F32)
    for k, row in enumerate(rows):
        total = jnp.where(place == k, row, total)
    return total


def to_columns(row, lane):
    channel = iota(lane.shape, 0)
    channels = lane.shape[0]
    up = jnp.sum(jnp.where(lane == channel, row, 0.0), axis=1, keepdims=True)
    down = jnp.sum(jnp.where(lane == channel + channels, row, 0.0), axis=1, keepdims=True)
    return up, down


def fold(me, prods, adds, channels):
    devices, width = prods.shape
    row, lane = iota((devices, width), 0), iota((devices, width), 1)
    ahead = lane < channels
    live = jnp.where(ahead, (row < me).astype(I32), (row > me).astype(I32)) > 0
    prod = jnp.where(live, prods[...], 1.0)
    add = jnp.where(live, adds[...], 0.0)
    d = 1
    while d < devices:
        next_prod = pltpu.roll(prod, devices - d, 0)
        next_add = pltpu.roll(add, devices - d, 0)
        add = jnp.where(ahead, next_prod * add + next_add, prod * next_add + add)
        prod = prod * next_prod
        d *= 2
    return add[:1]


SAVED = 12
KEPT = 6


def soft_plus(x):
    small = jnp.exp(-jnp.abs(x))
    z = small / (2.0 + small)
    square = z * z
    series = jnp.full_like(z, 1.0 / 19.0)
    for odd in (17, 15, 13, 11, 9, 7, 5, 3, 1):
        series = series * square + 1.0 / odd
    return jnp.maximum(x, 0.0) + 2.0 * z * series


def state_body(conv, branch, w_recur, w_input, decay_param, saved, carry):
    channels, tokens = conv.shape
    lane = iota((channels, tokens), 1)
    eye = iota((channels, channels), 0) == iota((channels, channels), 1)
    softness = jnp.sum(jnp.where(eye, soft_plus(-decay_param[...]), 0.0), axis=1, keepdims=True)
    values = conv[...].astype(F32)
    sig_r = jax.nn.sigmoid(dot(w_recur[0], conv[...], 0, 0))
    sig_a = jax.nn.sigmoid(dot(w_input[0], conv[...], 0, 0))
    decay = jnp.exp(-DECAY_SCALE * sig_r * softness)
    root = jnp.sqrt(1.0 - decay * decay + LEAK)
    direct = root * sig_a
    drive = direct * values
    up_prod, up_state = scan(decay, drive, lane, shift_in)
    down_prod, down_state = scan(decay, drive, lane, shift_out)
    x = branch[...].astype(F32)
    th = jnp.tanh(GELU_A * (x + GELU_B * x * x * x))
    saved[0] = decay
    saved[1] = up_prod
    saved[2] = up_state
    saved[3] = down_prod
    saved[4] = down_state
    saved[5] = 0.5 * x * (1.0 + th)
    saved[6] = 0.5 * (1.0 + th) + 0.5 * x * (1.0 - th * th) * GELU_A * (
        1.0 + 3.0 * GELU_B * x * x
    )
    saved[7] = decay * (-DECAY_SCALE * softness) * sig_r * (1.0 - sig_r)
    saved[8] = -(decay / root) * sig_a * values
    saved[9] = root * values * sig_a * (1.0 - sig_a)
    saved[10] = direct
    saved[11] = jnp.concatenate([w_recur[0], w_input[0]], axis=1).astype(F32)
    rows = ends_rows(up_prod, down_prod, lane) + ends_rows(up_state, down_state, lane)
    carry[...] = stacked(rows, tokens).astype(BF)


def joined_states(saved, state_in, state_back):
    return saved[2] + saved[1] * state_in, saved[4] + saved[3] * state_back


def join_body(home, saved, mix, ends, adds):
    channels, tokens = mix.shape
    devices = adds.shape[0]
    rows = home.shape[0]
    lane = iota((channels, tokens), 1)
    offset = iota((devices, rows), 1) - HOME_ROWS * iota((devices, rows), 0)
    base = HOME_ROWS - 6
    prod_rows = ((offset >= base) & (offset < base + 3)).astype(F32).astype(BF)
    add_rows = ((offset >= base + 3) & (offset < base + 6)).astype(F32).astype(BF)
    prods = ends.at[channels:, :]
    prods[...] = dot(prod_rows, home[...])
    adds[...] = dot(add_rows, home[...])
    state_in, state_back = to_columns(fold(lax.axis_index("sp"), prods, adds, channels), lane)
    ends[:channels, :] = jnp.where(lane < channels, state_in, state_back)
    fwd, bwd = joined_states(saved, state_in, state_back)
    mix[...] = (saved[5] * (fwd + bwd)).astype(BF)


def proj_body(lifted, mix, mine, theirs):
    blocks, tokens, _ = lifted.shape
    channels = mix.shape[0]
    half = channels // 2
    part_rows = mine.shape[1]
    left = iota((half, 128), 1) < 64
    even = (lax.axis_index("sp") & 1) == 0
    mixed = mix[...]
    for k in range(blocks // 2):
        proj = dot(mixed, pair(lifted, k, 0, tokens))
        for q in range(2):
            part = proj[:, 128 * q : 128 * (q + 1)]
            top, bottom = part[:half], part[half:]
            spot = 4 * k + 2 * q
            first = jnp.where(left, top, pltpu.roll(bottom, 64, 1))
            second = jnp.where(left, pltpu.roll(top, 64, 1), bottom)
            for n, rows in enumerate((first, second)):
                low, high = rows[:part_rows], rows[part_rows:]
                mine[spot + n] = jnp.where(even, low, high)
                theirs[spot + n] = jnp.where(even, high, low).astype(BF)


def adjoint_body(lifted, w_out, saved, ends, kept):
    blocks, tokens, _ = lifted.shape
    channels = w_out.shape[0]
    lane = iota((channels, tokens), 1)
    mix_cot = jnp.zeros((channels, tokens), F32)
    for k in range(blocks // 2):
        both = pair(lifted, k, 0, tokens)
        mix_cot = mix_cot + dot(w_out[:, 256 * k : 256 * (k + 1)], both, 1, 1)
    decay = saved[0]
    cot = mix_cot * saved[5]
    weighted = decay * cot
    _, up = scan(decay, weighted, lane, shift_in)
    _, down = scan(decay, weighted, lane, shift_out)
    kept[:channels] = mix_cot
    kept[channels : 2 * channels] = cot
    kept[2 * channels : 3 * channels] = up
    kept[3 * channels : 4 * channels] = down
    kept[4 * channels : 4 * channels + ends.shape[0]] = ends[...]
    kept[kept.shape[0] - 8 :] = stacked(ends_rows(up, down, lane), tokens)


def pack_body(mine, theirs, kept, far_out, out, sems):
    devices, part_rows, width = mine.shape
    spot = kept.shape[0] - 8
    tail = kept[spot : spot + 8][:GROUP].astype(BF)
    step, writes = devices // 4, []
    for s in range(devices):
        rows = mine[s] + theirs[s].astype(F32)
        for k in range(part_rows // GROUP):
            group = rows[GROUP * k : GROUP * (k + 1)].astype(BF)
            out[s, :, width * k : width * (k + 1)] = group
        out[s, :, width * (part_rows // GROUP) :] = tail
        if (s + 1) % step == 0:
            n = s // step
            span = pl.ds(n * step, step)
            writes.append(pltpu.make_async_copy(out.at[span], far_out.at[span], sems.at[n]))
            writes[n].start()
    for write in writes:
        write.wait()


def finish_body(last, saved, kept, g_proj, g_conv, g_branch, adds):
    devices = adds.shape[0]
    channels, tokens = g_conv.shape
    ends = kept.at[4 * channels :, :]
    prods = kept.at[5 * channels : 5 * channels + devices, :]
    lane = iota((channels, tokens), 1)
    cut = last.shape[2] - 128
    totals = [jnp.zeros((GROUP, cut), F32)] * 2
    for s in range(devices):
        totals[s & 1] = totals[s & 1] + last[s, :, :cut].astype(F32)
        adds[s : s + 1, :] = jnp.sum(last[s, :, cut:].astype(F32), axis=0, keepdims=True)
    turned = jnp.concatenate(
        [total[:, k : k + 128] for total in totals for k in range(0, cut, 128)], axis=0
    ).T
    g_proj[...] = jnp.concatenate([turned[:64], turned[64:]], axis=1)
    adj_in, adj_back = to_columns(fold(lax.axis_index("sp"), prods, adds, channels), lane)
    state_in, state_back = ends[:channels, :1], ends[:channels, tokens - 1 :]
    fwd, bwd = joined_states(saved, state_in, state_back)
    before = jnp.where(lane == 0, state_in, pltpu.roll(fwd, 1, 1))
    after = jnp.where(lane == tokens - 1, state_back, pltpu.roll(bwd, tokens - 1, 1))
    cot = kept[channels : 2 * channels]
    up = kept[2 * channels : 3 * channels] + saved[1] * adj_in
    down = kept[3 * channels : 4 * channels] + saved[3] * adj_back
    past = cot + jnp.where(lane == 0, adj_in, pltpu.roll(up, 1, 1))
    future = cot + jnp.where(lane == tokens - 1, adj_back, pltpu.roll(down, tokens - 1, 1))
    drive_cot = past + future
    decay_cot = future * before + past * after + drive_cot * saved[8]
    recur_cot = decay_cot * saved[7]
    admit_cot = drive_cot * saved[9]
    exact = lax.Precision.HIGHEST
    g_conv[...] = (
        drive_cot * saved[10]
        + dot(saved[11], jnp.concatenate([recur_cot, admit_cot], axis=0), 1, 0, exact)
    )
    g_branch[...] = kept[:channels] * (fwd + bwd) * saved[6]


def local(
    residual,
    out_cot,
    routes,
    route_weight,
    w_gate,
    w_up,
    w_down,
    w_out,
    conv_out,
    gate_branch,
    w_recur,
    w_input,
    decay_param,
):
    experts = lax.axis_size("sp")
    blocks = lax.axis_size("tp")
    tokens, lanes = residual.shape
    capacity = 2 * tokens // experts + 2
    slots = experts * capacity
    hidden, width = w_gate.shape[1:]
    channels = conv_out.shape[0]

    def kernel(body, *static):
        def run(*refs):
            body(*static, *refs)

        return run

    sent, comb = call(
        kernel(dispatch_body, experts),
        [
            ((experts, GROUP, 2 * capacity // GROUP * lanes), BF),
            ((experts * HOME_ROWS, tokens), BF),
        ],
        (routes.T, route_weight.T, residual, out_cot),
        fetched=4,
    )
    got = lax.all_to_all(sent, "sp", split_axis=0, concat_axis=0, tiled=True)
    (spread,) = call(
        kernel(compact_body, experts, capacity),
        [((blocks, 2 * slots, lanes), BF)],
        (got,),
    )
    whole = lax.all_to_all(spread, "tp", 0, 0, tiled=True)
    dxp, acts, saved, carry = call(
        expert_body,
        [
            ((blocks, slots, lanes), BF),
            ((slots, 3 * hidden), BF),
            ((SAVED, channels, tokens), F32),
            ((8, tokens), BF),
        ],
        (
            conv_out,
            gate_branch,
            w_recur,
            w_input,
            decay_param.reshape(1, channels),
            whole,
            w_gate[0],
            w_up[0],
            w_down[0],
        ),
        fetched=5,
        scratch=(pltpu.VMEM((slots, 3 * hidden), BF), pltpu.SemaphoreType.DMA),
        far=(1,),
        flops=10 * slots * hidden * width,
    )
    parts = lax.all_to_all(dxp, "tp", 0, 0, tiled=True)
    (returned,) = call(
        kernel(owner_sum_body, experts, capacity),
        [((experts * HOME_ROWS, lanes), BF)],
        (parts, carry),
    )
    home = lax.all_to_all(
        returned.reshape(experts, HOME_ROWS, lanes), "sp", split_axis=0, concat_axis=0, tiled=True
    ).reshape(experts * HOME_ROWS, lanes)
    own, mix, ends = call(
        lift_body,
        [
            ((blocks, tokens, lanes), BF),
            ((channels, tokens), BF),
            ((channels + experts, tokens), F32),
        ],
        (home, comb, out_cot, saved),
        scratch=(pltpu.VMEM((experts, tokens), F32),),
    )
    lifted = lax.all_to_all(own, "tp", 0, 0, tiled=True)
    part_rows = channels // 4
    last_width = (part_rows // GROUP + 1) * lanes
    mine, theirs = call(
        proj_body,
        [((experts, part_rows, lanes), F32), ((experts, part_rows, lanes), BF)],
        (lifted, mix),
        flops=2 * channels * tokens * width,
    )
    swapped = lax.ppermute(theirs, "sp", [(i, i ^ 1) for i in range(experts)])
    (kept,) = call(
        adjoint_body,
        [((KEPT * channels, tokens), F32)],
        (lifted, w_out, saved, ends),
        flops=100 * channels * tokens * width,
    )
    (piece,) = call(
        pack_body,
        [((experts, GROUP, last_width), BF)],
        (mine, swapped, kept),
        scratch=(pltpu.VMEM((experts, GROUP, last_width), BF), pltpu.SemaphoreType.DMA((4,))),
        far=(0,),
    )
    piece, acts = lax.optimization_barrier((piece, acts))
    grads = expert_grads(whole, acts, width)
    last = lax.all_to_all(piece, "sp", split_axis=0, concat_axis=0, tiled=True)
    g_proj, g_conv, g_branch = call(
        finish_body,
        [((width // experts, channels), F32), ((channels, tokens), F32), ((channels, tokens), F32)],
        (last, saved, kept),
        scratch=(pltpu.VMEM((experts, tokens), F32),),
    )
    return (grads[0], grads[1], grads[2], g_proj, g_conv, g_branch)


def solution(mesh):
    return jax.shard_map(
        local,
        mesh=mesh,
        in_specs=(
            P("sp", "tp"),
            P("sp", "tp"),
            P("sp", None),
            P("sp", None),
            P("sp", "tp", None),
            P("sp", "tp", None),
            P("sp", "tp", None),
            P("tp", None),
            P("tp", "sp"),
            P("tp", "sp"),
            P("tp", None, None),
            P("tp", None, None),
            P("tp"),
        ),
        out_specs=(
            P("sp", "tp", None),
            P("sp", "tp", None),
            P("sp", "tp", None),
            P("sp", "tp"),
            P("tp", "sp"),
            P("tp", "sp"),
        ),
        check_vma=False,
    )
```

```python
import jax
import jax.numpy as jnp
from jax import lax
from jax.experimental import pallas as pl
from jax.experimental.pallas import tpu as pltpu
from jax.sharding import PartitionSpec as P

LEAK = 0.01
DECAY_SCALE = 8.0
GELU_A = 0.7978845608028654
GELU_B = 0.044715

BF = jnp.bfloat16
F32 = jnp.float32
I32 = jnp.int32

HOME_ROWS = 16
GROUP = 4


def iota(shape, dim):
    return lax.broadcasted_iota(I32, shape, dim)


def dot(a, b, ca=1, cb=0, precision=None):
    return lax.dot_general(
        a, b, (((ca,), (cb,)), ((), ())), precision=precision, preferred_element_type=F32
    )


def call(body, outs, args, flops=1, bytes_moved=1, fetched=0, scratch=(), far=()):
    specs = [pl.BlockSpec(memory_space=pltpu.HBM)] * fetched
    specs += [pl.BlockSpec(memory_space=pltpu.VMEM)] * (len(args) - fetched)
    scratch = [pltpu.VMEM(a.shape, a.dtype) for a in args[:fetched]] + list(scratch)
    kept = [pltpu.with_memory_space_constraint(a, pltpu.HBM) for a in args[:fetched]]
    args = kept + list(args[fetched:])
    if fetched:
        scratch.append(pltpu.SemaphoreType.DMA((fetched,)))
    return pl.pallas_call(
        body,
        out_shape=[
            pltpu.HBM(*out) if k in far else jax.ShapeDtypeStruct(*out)
            for k, out in enumerate(outs)
        ],
        in_specs=specs,
        out_specs=[
            pl.BlockSpec(memory_space=pltpu.HBM if k in far else pltpu.VMEM)
            for k in range(len(outs))
        ],
        scratch_shapes=scratch,
        compiler_params=pltpu.CompilerParams(vmem_limit_bytes=24 * 1024 * 1024),
        cost_estimate=pl.CostEstimate(
            flops=flops, bytes_accessed=bytes_moved, transcendentals=0
        ),
    )(*args)


def fetch(sources, targets, sems):
    copies = [
        pltpu.make_async_copy(source, target, sems.at[k])
        for k, (source, target) in enumerate(zip(sources, targets))
    ]
    for copy in copies:
        copy.start()
    return copies


def dispatch_body(experts, *refs):
    sources, (sent, comb), targets, sems = refs[:4], refs[4:6], refs[6:10], refs[10]
    for copy in fetch(sources, targets, sems):
        copy.wait()
    routes, weight, residual, cot = targets
    tokens = residual.shape[0]
    first, second = routes[0:1, :], routes[1:2, :]
    expert = iota((experts, tokens), 0)
    hit0 = (expert == first).astype(F32)
    hit1 = (expert == second).astype(F32)
    earlier = (iota((tokens, tokens), 0) < iota((tokens, tokens), 1)).astype(BF)
    before = dot((hit0 + hit1).astype(BF), earlier)
    slot0 = jnp.sum(before * hit0, axis=0, keepdims=True).astype(I32)
    slot1 = jnp.sum((before + hit0) * hit1, axis=0, keepdims=True).astype(I32)
    back = iota((experts * HOME_ROWS, tokens), 0)
    at_home = (back == first * HOME_ROWS + slot0) | (back == second * HOME_ROWS + slot1)
    comb[...] = at_home.astype(F32).astype(BF)
    count = sent.shape[2] // tokens
    capacity = GROUP * count // 2
    row = iota((experts * GROUP, tokens), 0)
    place0 = first * 2 * capacity + slot0
    place1 = second * 2 * capacity + slot1
    spot = (row & (GROUP - 1)) + (row >> 2) * 2 * capacity
    for k in range(count):
        here = spot + GROUP * k
        in_rows = ((here == place0) | (here == place1)).astype(F32).astype(BF)
        cot0 = here == place0 + capacity
        cot1 = here == place1 + capacity
        factor = jnp.sum(
            jnp.where(cot0, weight[0:1, :], 0.0) + jnp.where(cot1, weight[1:2, :], 0.0),
            axis=1,
            keepdims=True,
        )
        cot_rows = (cot0 | cot1).astype(F32).astype(BF)
        rows = dot(in_rows, residual[...]) + factor * dot(cot_rows, cot[...])
        for e in range(experts):
            sent[e, :, tokens * k : tokens * (k + 1)] = rows[GROUP * e : GROUP * (e + 1)].astype(BF)


def compact_body(experts, capacity, got, out):
    slots = experts * capacity
    lanes = out.shape[2]
    count = got.shape[2] // lanes
    blocks = [
        jnp.concatenate(
            [got[e, :, lanes * k : lanes * (k + 1)].astype(F32) for e in range(experts)], axis=0
        )
        for k in range(count)
    ]
    row = iota((2 * slots, 1), 0)
    half = (row >= slots).astype(I32)
    rest = row - half * slots
    source = jnp.floor((rest.astype(F32) + 0.5) * (1.0 / capacity)).astype(I32)
    inner = half * capacity + (rest - source * capacity)
    target = (inner >> 2) * experts * GROUP + source * GROUP + (inner & (GROUP - 1))
    total = count * experts * GROUP
    pick = (iota((2 * slots, total), 1) == target).astype(F32).astype(BF)
    rows = dot(pick, jnp.concatenate(blocks, axis=0).astype(BF)).astype(BF)
    for j in range(out.shape[0]):
        out[j] = rows


def pair(ref, k, lo, hi):
    return jnp.concatenate([ref[2 * k, lo:hi, :], ref[2 * k + 1, lo:hi, :]], axis=1)


def expert_body(
    conv,
    branch,
    w_recur,
    w_input,
    decay_param,
    whole,
    w_gate,
    w_up,
    w_down,
    dxp,
    far_acts,
    saved,
    carry,
    acts,
    acts_sem,
):
    slots = whole.shape[1] // 2
    blocks = whole.shape[0]
    hidden = w_gate.shape[0]
    pre = jnp.zeros((slots, 2 * hidden), F32)
    act_cot = jnp.zeros((slots, hidden), F32)
    for k in range(blocks // 2):
        cols = slice(256 * k, 256 * (k + 1))
        both = jnp.concatenate([w_gate[:, cols], w_up[:, cols]], axis=0)
        pre = pre + dot(pair(whole, k, 0, slots), both, 1, 1)
        act_cot = act_cot + dot(pair(whole, k, slots, 2 * slots), w_down[:, cols], 1, 1)
    state_body(conv, branch, w_recur, w_input, decay_param, saved, carry)
    pre_gate, pre_up = pre[:, :hidden], pre[:, hidden:]
    sig = jax.nn.sigmoid(pre_gate)
    silu = pre_gate * sig
    slope = sig * (1.0 + pre_gate * (1.0 - sig))
    act = (silu * pre_up).astype(BF)
    gate_cot = (act_cot * pre_up * slope).astype(BF)
    up_cot = (act_cot * silu).astype(BF)
    cots = jnp.concatenate([gate_cot, up_cot], axis=1)
    acts[:, : 2 * hidden] = cots
    acts[:, 2 * hidden :] = act
    write = pltpu.make_async_copy(acts, far_acts, acts_sem)
    write.start()
    for k in range(blocks // 2):
        cols = slice(256 * k, 256 * (k + 1))
        both = jnp.concatenate([w_gate[:, cols], w_up[:, cols]], axis=0)
        part = dot(cots, both).astype(BF)
        dxp[2 * k] = part[:, :128]
        dxp[2 * k + 1] = part[:, 128:]
    write.wait()


def grads_body(whole, acts, g_gate, g_up, g_down):
    slots = whole.shape[1] // 2
    hidden = acts.shape[1] // 3
    both = dot(acts[:, : 2 * hidden], pair(whole, 0, 0, slots), 0, 0).astype(BF)
    g_gate[0] = both[:hidden]
    g_up[0] = both[hidden:]
    g_down[0] = dot(acts[:, 2 * hidden :], pair(whole, 0, slots, 2 * slots), 0, 0).astype(BF)


def expert_grads(whole, acts, width):
    blocks, rows, lanes = whole.shape
    hidden = acts.shape[1] // 3
    out = jax.ShapeDtypeStruct((1, hidden, width), BF)
    spec = pl.BlockSpec((1, hidden, 2 * lanes), lambda i: (0, 0, i))
    return pl.pallas_call(
        grads_body,
        grid=(blocks // 2,),
        out_shape=[out] * 3,
        in_specs=[
            pl.BlockSpec((2, rows, lanes), lambda i: (i, 0, 0)),
            pl.BlockSpec(acts.shape, lambda i: (0, 0)),
        ],
        out_specs=[spec] * 3,
        compiler_params=pltpu.CompilerParams(vmem_limit_bytes=16 * 1024 * 1024),
        cost_estimate=pl.CostEstimate(
            flops=3 * rows * hidden * width, bytes_accessed=6 * hidden * width, transcendentals=0
        ),
    )(whole, acts)


def owner_sum_body(experts, capacity, parts, carry, out):
    total = parts[0].astype(F32)
    for j in range(1, parts.shape[0]):
        total = total + parts[j].astype(F32)
    total = total.astype(BF)
    rows = experts * HOME_ROWS
    place = iota((rows, 1), 0)
    inner = place & (HOME_ROWS - 1)
    source = jnp.where(inner < capacity, (place >> 4) * capacity + inner, -1)
    pick = (iota((rows, experts * capacity), 1) == source).astype(F32).astype(BF)
    extra = (iota((rows, carry.shape[0]), 1) == inner - capacity).astype(F32).astype(BF)
    out[...] = (dot(pick, total) + dot(extra, carry[...])).astype(BF)


def lift_body(home, comb, cot, saved, out, mix, ends, adds):
    grad = dot(comb[...], home[...], 0, 0)
    lifted = (cot[...].astype(F32) + grad).astype(BF)
    for j in range(out.shape[0]):
        out[j] = lifted
    join_body(home, saved, mix, ends, adds)


def shift_in(x, d, fill, lane):
    return jnp.where(lane >= d, pltpu.roll(x, d, 1), fill)


def shift_out(x, d, fill, lane):
    width = x.shape[1]
    return jnp.where(lane < width - d, pltpu.roll(x, width - d, 1), fill)


def scan(decay, drive, lane, moved):
    d = 1
    while d < decay.shape[1]:
        drive = decay * moved(drive, d, 0.0, lane) + drive
        decay = decay * moved(decay, d, 1.0, lane)
        d *= 2
    return decay, drive


def in_three(x):
    high = x.astype(BF)
    rest = x - high.astype(F32)
    mid = rest.astype(BF)
    low = (rest - mid.astype(F32)).astype(BF)
    return high, mid, low


def ends_rows(up, down, lane):
    width = up.shape[1]
    ends = jnp.concatenate(
        [jnp.where(lane == width - 1, up, 0.0), jnp.where(lane == 0, down, 0.0)], axis=0
    )
    ones = jnp.ones((8, width), BF)
    return [dot(ones, piece, 1, 1) for piece in in_three(ends)]


def stacked(rows, width):
    place = iota((8, width), 0)
    total = jnp.zeros((8, width), F32)
    for k, row in enumerate(rows):
        total = jnp.where(place == k, row, total)
    return total


def to_columns(row, lane):
    channel = iota(lane.shape, 0)
    channels = lane.shape[0]
    up = jnp.sum(jnp.where(lane == channel, row, 0.0), axis=1, keepdims=True)
    down = jnp.sum(jnp.where(lane == channel + channels, row, 0.0), axis=1, keepdims=True)
    return up, down


def fold(me, prods, adds, channels):
    devices, width = prods.shape
    row, lane = iota((devices, width), 0), iota((devices, width), 1)
    ahead = lane < channels
    live = jnp.where(ahead, (row < me).astype(I32), (row > me).astype(I32)) > 0
    prod = jnp.where(live, prods[...], 1.0)
    add = jnp.where(live, adds[...], 0.0)
    d = 1
    while d < devices:
        next_prod = pltpu.roll(prod, devices - d, 0)
        next_add = pltpu.roll(add, devices - d, 0)
        add = jnp.where(ahead, next_prod * add + next_add, prod * next_add + add)
        prod = prod * next_prod
        d *= 2
    return add[:1]


SAVED = 12
KEPT = 6


def soft_plus(x):
    small = jnp.exp(-jnp.abs(x))
    z = small / (2.0 + small)
    square = z * z
    series = jnp.full_like(z, 1.0 / 19.0)
    for odd in (17, 15, 13, 11, 9, 7, 5, 3, 1):
        series = series * square + 1.0 / odd
    return jnp.maximum(x, 0.0) + 2.0 * z * series


def state_body(conv, branch, w_recur, w_input, decay_param, saved, carry):
    channels, tokens = conv.shape
    lane = iota((channels, tokens), 1)
    eye = iota((channels, channels), 0) == iota((channels, channels), 1)
    softness = jnp.sum(jnp.where(eye, soft_plus(-decay_param[...]), 0.0), axis=1, keepdims=True)
    values = conv[...].astype(F32)
    sig_r = jax.nn.sigmoid(dot(w_recur[0], conv[...], 0, 0))
    sig_a = jax.nn.sigmoid(dot(w_input[0], conv[...], 0, 0))
    decay = jnp.exp(-DECAY_SCALE * sig_r * softness)
    root = jnp.sqrt(1.0 - decay * decay + LEAK)
    direct = root * sig_a
    drive = direct * values
    up_prod, up_state = scan(decay, drive, lane, shift_in)
    down_prod, down_state = scan(decay, drive, lane, shift_out)
    x = branch[...].astype(F32)
    th = jnp.tanh(GELU_A * (x + GELU_B * x * x * x))
    saved[0] = decay
    saved[1] = up_prod
    saved[2] = up_state
    saved[3] = down_prod
    saved[4] = down_state
    saved[5] = 0.5 * x * (1.0 + th)
    saved[6] = 0.5 * (1.0 + th) + 0.5 * x * (1.0 - th * th) * GELU_A * (
        1.0 + 3.0 * GELU_B * x * x
    )
    saved[7] = decay * (-DECAY_SCALE * softness) * sig_r * (1.0 - sig_r)
    saved[8] = -(decay / root) * sig_a * values
    saved[9] = root * values * sig_a * (1.0 - sig_a)
    saved[10] = direct
    saved[11] = jnp.concatenate([w_recur[0], w_input[0]], axis=1).astype(F32)
    rows = ends_rows(up_prod, down_prod, lane) + ends_rows(up_state, down_state, lane)
    carry[...] = stacked(rows, tokens).astype(BF)


def joined_states(saved, state_in, state_back):
    return saved[2] + saved[1] * state_in, saved[4] + saved[3] * state_back


def join_body(home, saved, mix, ends, adds):
    channels, tokens = mix.shape
    devices = adds.shape[0]
    rows = home.shape[0]
    lane = iota((channels, tokens), 1)
    offset = iota((devices, rows), 1) - HOME_ROWS * iota((devices, rows), 0)
    base = HOME_ROWS - 6
    prod_rows = ((offset >= base) & (offset < base + 3)).astype(F32).astype(BF)
    add_rows = ((offset >= base + 3) & (offset < base + 6)).astype(F32).astype(BF)
    prods = ends.at[channels:, :]
    prods[...] = dot(prod_rows, home[...])
    adds[...] = dot(add_rows, home[...])
    state_in, state_back = to_columns(fold(lax.axis_index("sp"), prods, adds, channels), lane)
    ends[:channels, :] = jnp.where(lane < channels, state_in, state_back)
    fwd, bwd = joined_states(saved, state_in, state_back)
    mix[...] = (saved[5] * (fwd + bwd)).astype(BF)


def proj_body(lifted, mix, mine, theirs):
    blocks, tokens, _ = lifted.shape
    channels = mix.shape[0]
    half = channels // 2
    part_rows = mine.shape[1]
    left = iota((half, 128), 1) < 64
    even = (lax.axis_index("sp") & 1) == 0
    mixed = mix[...]
    for k in range(blocks // 2):
        proj = dot(mixed, pair(lifted, k, 0, tokens))
        for q in range(2):
            part = proj[:, 128 * q : 128 * (q + 1)]
            top, bottom = part[:half], part[half:]
            spot = 4 * k + 2 * q
            first = jnp.where(left, top, pltpu.roll(bottom, 64, 1))
            second = jnp.where(left, pltpu.roll(top, 64, 1), bottom)
            for n, rows in enumerate((first, second)):
                low, high = rows[:part_rows], rows[part_rows:]
                mine[spot + n] = jnp.where(even, low, high)
                theirs[spot + n] = jnp.where(even, high, low).astype(BF)


def adjoint_body(lifted, w_out, saved, ends, kept):
    blocks, tokens, _ = lifted.shape
    channels = w_out.shape[0]
    lane = iota((channels, tokens), 1)
    mix_cot = jnp.zeros((channels, tokens), F32)
    for k in range(blocks // 2):
        both = pair(lifted, k, 0, tokens)
        mix_cot = mix_cot + dot(w_out[:, 256 * k : 256 * (k + 1)], both, 1, 1)
    decay = saved[0]
    cot = mix_cot * saved[5]
    weighted = decay * cot
    _, up = scan(decay, weighted, lane, shift_in)
    _, down = scan(decay, weighted, lane, shift_out)
    kept[:channels] = mix_cot
    kept[channels : 2 * channels] = cot
    kept[2 * channels : 3 * channels] = up
    kept[3 * channels : 4 * channels] = down
    kept[4 * channels : 4 * channels + ends.shape[0]] = ends[...]
    kept[kept.shape[0] - 8 :] = stacked(ends_rows(up, down, lane), tokens)


def pack_body(mine, theirs, kept, far_out, out, sems):
    devices, part_rows, width = mine.shape
    spot = kept.shape[0] - 8
    tail = kept[spot : spot + 8][:GROUP].astype(BF)
    step, writes = devices // 4, []
    for s in range(devices):
        rows = mine[s] + theirs[s].astype(F32)
        for k in range(part_rows // GROUP):
            group = rows[GROUP * k : GROUP * (k + 1)].astype(BF)
            out[s, :, width * k : width * (k + 1)] = group
        out[s, :, width * (part_rows // GROUP) :] = tail
        if (s + 1) % step == 0:
            n = s // step
            span = pl.ds(n * step, step)
            writes.append(pltpu.make_async_copy(out.at[span], far_out.at[span], sems.at[n]))
            writes[n].start()
    for write in writes:
        write.wait()


def finish_body(last, saved, kept, g_proj, g_conv, g_branch, adds):
    devices = adds.shape[0]
    channels, tokens = g_conv.shape
    ends = kept.at[4 * channels :, :]
    prods = kept.at[5 * channels : 5 * channels + devices, :]
    lane = iota((channels, tokens), 1)
    cut = last.shape[2] - 128
    totals = [jnp.zeros((GROUP, cut), F32)] * 2
    for s in range(devices):
        totals[s & 1] = totals[s & 1] + last[s, :, :cut].astype(F32)
        adds[s : s + 1, :] = jnp.sum(last[s, :, cut:].astype(F32), axis=0, keepdims=True)
    turned = jnp.concatenate(
        [total[:, k : k + 128] for total in totals for k in range(0, cut, 128)], axis=0
    ).T
    g_proj[...] = jnp.concatenate([turned[:64], turned[64:]], axis=1)
    adj_in, adj_back = to_columns(fold(lax.axis_index("sp"), prods, adds, channels), lane)
    state_in, state_back = ends[:channels, :1], ends[:channels, tokens - 1 :]
    fwd, bwd = joined_states(saved, state_in, state_back)
    before = jnp.where(lane == 0, state_in, pltpu.roll(fwd, 1, 1))
    after = jnp.where(lane == tokens - 1, state_back, pltpu.roll(bwd, tokens - 1, 1))
    cot = kept[channels : 2 * channels]
    up = kept[2 * channels : 3 * channels] + saved[1] * adj_in
    down = kept[3 * channels : 4 * channels] + saved[3] * adj_back
    past = cot + jnp.where(lane == 0, adj_in, pltpu.roll(up, 1, 1))
    future = cot + jnp.where(lane == tokens - 1, adj_back, pltpu.roll(down, tokens - 1, 1))
    drive_cot = past + future
    decay_cot = future * before + past * after + drive_cot * saved[8]
    recur_cot = decay_cot * saved[7]
    admit_cot = drive_cot * saved[9]
    exact = lax.Precision.HIGHEST
    g_conv[...] = (
        drive_cot * saved[10]
        + dot(saved[11], jnp.concatenate([recur_cot, admit_cot], axis=0), 1, 0, exact)
    )
    g_branch[...] = kept[:channels] * (fwd + bwd) * saved[6]


def local(
    residual,
    out_cot,
    routes,
    route_weight,
    w_gate,
    w_up,
    w_down,
    w_out,
    conv_out,
    gate_branch,
    w_recur,
    w_input,
    decay_param,
):
    experts = lax.axis_size("sp")
    blocks = lax.axis_size("tp")
    tokens, lanes = residual.shape
    capacity = 2 * tokens // experts + 2
    slots = experts * capacity
    hidden, width = w_gate.shape[1:]
    channels = conv_out.shape[0]

    def kernel(body, *static):
        def run(*refs):
            body(*static, *refs)

        return run

    sent, comb = call(
        kernel(dispatch_body, experts),
        [
            ((experts, GROUP, 2 * capacity // GROUP * lanes), BF),
            ((experts * HOME_ROWS, tokens), BF),
        ],
        (routes.T, route_weight.T, residual, out_cot),
        fetched=4,
    )
    got = lax.all_to_all(sent, "sp", split_axis=0, concat_axis=0, tiled=True)
    (spread,) = call(
        kernel(compact_body, experts, capacity),
        [((blocks, 2 * slots, lanes), BF)],
        (got,),
    )
    whole = lax.all_to_all(spread, "tp", 0, 0, tiled=True)
    dxp, acts, saved, carry = call(
        expert_body,
        [
            ((blocks, slots, lanes), BF),
            ((slots, 3 * hidden), BF),
            ((SAVED, channels, tokens), F32),
            ((8, tokens), BF),
        ],
        (
            conv_out,
            gate_branch,
            w_recur,
            w_input,
            decay_param.reshape(1, channels),
            whole,
            w_gate[0],
            w_up[0],
            w_down[0],
        ),
        scratch=(pltpu.VMEM((slots, 3 * hidden), BF), pltpu.SemaphoreType.DMA),
        far=(1,),
        flops=10 * slots * hidden * width,
    )
    parts = lax.all_to_all(dxp, "tp", 0, 0, tiled=True)
    (returned,) = call(
        kernel(owner_sum_body, experts, capacity),
        [((experts * HOME_ROWS, lanes), BF)],
        (parts, carry),
    )
    home = lax.all_to_all(
        returned.reshape(experts, HOME_ROWS, lanes), "sp", split_axis=0, concat_axis=0, tiled=True
    ).reshape(experts * HOME_ROWS, lanes)
    own, mix, ends = call(
        lift_body,
        [
            ((blocks, tokens, lanes), BF),
            ((channels, tokens), BF),
            ((channels + experts, tokens), F32),
        ],
        (home, comb, out_cot, saved),
        scratch=(pltpu.VMEM((experts, tokens), F32),),
    )
    lifted = lax.all_to_all(own, "tp", 0, 0, tiled=True)
    part_rows = channels // 4
    last_width = (part_rows // GROUP + 1) * lanes
    mine, theirs = call(
        proj_body,
        [((experts, part_rows, lanes), F32), ((experts, part_rows, lanes), BF)],
        (lifted, mix),
        flops=2 * channels * tokens * width,
    )
    swapped = lax.ppermute(theirs, "sp", [(i, i ^ 1) for i in range(experts)])
    (kept,) = call(
        adjoint_body,
        [((KEPT * channels, tokens), F32)],
        (lifted, w_out, saved, ends),
        flops=100 * channels * tokens * width,
    )
    (piece,) = call(
        pack_body,
        [((experts, GROUP, last_width), BF)],
        (mine, swapped, kept),
        scratch=(pltpu.VMEM((experts, GROUP, last_width), BF), pltpu.SemaphoreType.DMA((4,))),
        far=(0,),
    )
    piece, acts = lax.optimization_barrier((piece, acts))
    grads = expert_grads(whole, acts, width)
    last = lax.all_to_all(piece, "sp", split_axis=0, concat_axis=0, tiled=True)
    g_proj, g_conv, g_branch = call(
        finish_body,
        [((width // experts, channels), F32), ((channels, tokens), F32), ((channels, tokens), F32)],
        (last, saved, kept),
        scratch=(pltpu.VMEM((experts, tokens), F32),),
    )
    return (grads[0], grads[1], grads[2], g_proj, g_conv, g_branch)


def solution(mesh):
    return jax.shard_map(
        local,
        mesh=mesh,
        in_specs=(
            P("sp", "tp"),
            P("sp", "tp"),
            P("sp", None),
            P("sp", None),
            P("sp", "tp", None),
            P("sp", "tp", None),
            P("sp", "tp", None),
            P("tp", None),
            P("tp", "sp"),
            P("tp", "sp"),
            P("tp", None, None),
            P("tp", None, None),
            P("tp"),
        ),
        out_specs=(
            P("sp", "tp", None),
            P("sp", "tp", None),
            P("sp", "tp", None),
            P("sp", "tp"),
            P("tp", "sp"),
            P("tp", "sp"),
        ),
        check_vma=False,
    )
```

```python
import jax
import jax.numpy as jnp
from jax import lax
from jax.experimental import pallas as pl
from jax.experimental.pallas import tpu as pltpu
from jax.sharding import PartitionSpec as P

LEAK = 0.01
DECAY_SCALE = 8.0
GELU_A = 0.7978845608028654
GELU_B = 0.044715

BF = jnp.bfloat16
F32 = jnp.float32
I32 = jnp.int32

HOME_ROWS = 16
GROUP = 4


def iota(shape, dim):
    return lax.broadcasted_iota(I32, shape, dim)


def dot(a, b, ca=1, cb=0, precision=None):
    return lax.dot_general(
        a, b, (((ca,), (cb,)), ((), ())), precision=precision, preferred_element_type=F32
    )


def call(body, outs, args, flops=1, bytes_moved=1, fetched=0, scratch=(), far=()):
    specs = [pl.BlockSpec(memory_space=pltpu.HBM)] * fetched
    specs += [pl.BlockSpec(memory_space=pltpu.VMEM)] * (len(args) - fetched)
    scratch = [pltpu.VMEM(a.shape, a.dtype) for a in args[:fetched]] + list(scratch)
    kept = [pltpu.with_memory_space_constraint(a, pltpu.HBM) for a in args[:fetched]]
    args = kept + list(args[fetched:])
    if fetched:
        scratch.append(pltpu.SemaphoreType.DMA((fetched,)))
    return pl.pallas_call(
        body,
        out_shape=[
            pltpu.HBM(*out) if k in far else jax.ShapeDtypeStruct(*out)
            for k, out in enumerate(outs)
        ],
        in_specs=specs,
        out_specs=[
            pl.BlockSpec(memory_space=pltpu.HBM if k in far else pltpu.VMEM)
            for k in range(len(outs))
        ],
        scratch_shapes=scratch,
        compiler_params=pltpu.CompilerParams(vmem_limit_bytes=24 * 1024 * 1024),
        cost_estimate=pl.CostEstimate(
            flops=flops, bytes_accessed=bytes_moved, transcendentals=0
        ),
    )(*args)


def fetch(sources, targets, sems):
    copies = [
        pltpu.make_async_copy(source, target, sems.at[k])
        for k, (source, target) in enumerate(zip(sources, targets))
    ]
    for copy in copies:
        copy.start()
    return copies


def dispatch_body(experts, *refs):
    sources, (sent, comb), targets, sems = refs[:4], refs[4:6], refs[6:10], refs[10]
    for copy in fetch(sources, targets, sems):
        copy.wait()
    routes, weight, residual, cot = targets
    tokens = residual.shape[0]
    first, second = routes[0:1, :], routes[1:2, :]
    expert = iota((experts, tokens), 0)
    hit0 = (expert == first).astype(F32)
    hit1 = (expert == second).astype(F32)
    earlier = (iota((tokens, tokens), 0) < iota((tokens, tokens), 1)).astype(BF)
    before = dot((hit0 + hit1).astype(BF), earlier)
    slot0 = jnp.sum(before * hit0, axis=0, keepdims=True).astype(I32)
    slot1 = jnp.sum((before + hit0) * hit1, axis=0, keepdims=True).astype(I32)
    back = iota((experts * HOME_ROWS, tokens), 0)
    at_home = (back == first * HOME_ROWS + slot0) | (back == second * HOME_ROWS + slot1)
    comb[...] = at_home.astype(F32).astype(BF)
    count = sent.shape[2] // tokens
    capacity = GROUP * count // 2
    row = iota((experts * GROUP, tokens), 0)
    place0 = first * 2 * capacity + slot0
    place1 = second * 2 * capacity + slot1
    spot = (row & (GROUP - 1)) + (row >> 2) * 2 * capacity
    for k in range(count):
        here = spot + GROUP * k
        in_rows = ((here == place0) | (here == place1)).astype(F32).astype(BF)
        cot0 = here == place0 + capacity
        cot1 = here == place1 + capacity
        factor = jnp.sum(
            jnp.where(cot0, weight[0:1, :], 0.0) + jnp.where(cot1, weight[1:2, :], 0.0),
            axis=1,
            keepdims=True,
        )
        cot_rows = (cot0 | cot1).astype(F32).astype(BF)
        rows = dot(in_rows, residual[...]) + factor * dot(cot_rows, cot[...])
        for e in range(experts):
            sent[e, :, tokens * k : tokens * (k + 1)] = rows[GROUP * e : GROUP * (e + 1)].astype(BF)


def compact_body(experts, capacity, got, out):
    slots = experts * capacity
    lanes = out.shape[2]
    count = got.shape[2] // lanes
    blocks = [
        jnp.concatenate(
            [got[e, :, lanes * k : lanes * (k + 1)].astype(F32) for e in range(experts)], axis=0
        )
        for k in range(count)
    ]
    row = iota((2 * slots, 1), 0)
    half = (row >= slots).astype(I32)
    rest = row - half * slots
    source = jnp.floor((rest.astype(F32) + 0.5) * (1.0 / capacity)).astype(I32)
    inner = half * capacity + (rest - source * capacity)
    target = (inner >> 2) * experts * GROUP + source * GROUP + (inner & (GROUP - 1))
    total = count * experts * GROUP
    pick = (iota((2 * slots, total), 1) == target).astype(F32).astype(BF)
    rows = dot(pick, jnp.concatenate(blocks, axis=0).astype(BF)).astype(BF)
    for j in range(out.shape[0]):
        out[j] = rows


def pair(ref, k, lo, hi):
    return jnp.concatenate([ref[2 * k, lo:hi, :], ref[2 * k + 1, lo:hi, :]], axis=1)


def expert_body(
    conv,
    branch,
    w_recur,
    w_input,
    decay_param,
    whole,
    w_gate,
    w_up,
    w_down,
    dxp,
    acts,
    saved,
    carry,
):
    slots = whole.shape[1] // 2
    blocks = whole.shape[0]
    hidden = w_gate.shape[0]
    pre = jnp.zeros((slots, 2 * hidden), F32)
    act_cot = jnp.zeros((slots, hidden), F32)
    for k in range(blocks // 2):
        cols = slice(256 * k, 256 * (k + 1))
        both = jnp.concatenate([w_gate[:, cols], w_up[:, cols]], axis=0)
        pre = pre + dot(pair(whole, k, 0, slots), both, 1, 1)
        act_cot = act_cot + dot(pair(whole, k, slots, 2 * slots), w_down[:, cols], 1, 1)
    state_body(conv, branch, w_recur, w_input, decay_param, saved, carry)
    pre_gate, pre_up = pre[:, :hidden], pre[:, hidden:]
    sig = jax.nn.sigmoid(pre_gate)
    silu = pre_gate * sig
    slope = sig * (1.0 + pre_gate * (1.0 - sig))
    act = (silu * pre_up).astype(BF)
    gate_cot = (act_cot * pre_up * slope).astype(BF)
    up_cot = (act_cot * silu).astype(BF)
    cots = jnp.concatenate([gate_cot, up_cot], axis=1)
    acts[:, : 2 * hidden] = cots
    acts[:, 2 * hidden :] = act
    for k in range(blocks // 2):
        cols = slice(256 * k, 256 * (k + 1))
        both = jnp.concatenate([w_gate[:, cols], w_up[:, cols]], axis=0)
        part = dot(cots, both).astype(BF)
        dxp[2 * k] = part[:, :128]
        dxp[2 * k + 1] = part[:, 128:]


def grads_body(whole, acts, g_gate, g_up, g_down):
    slots = whole.shape[1] // 2
    hidden = acts.shape[1] // 3
    both = dot(acts[:, : 2 * hidden], pair(whole, 0, 0, slots), 0, 0).astype(BF)
    g_gate[0] = both[:hidden]
    g_up[0] = both[hidden:]
    g_down[0] = dot(acts[:, 2 * hidden :], pair(whole, 0, slots, 2 * slots), 0, 0).astype(BF)


def expert_grads(whole, acts, width):
    blocks, rows, lanes = whole.shape
    hidden = acts.shape[1] // 3
    out = jax.ShapeDtypeStruct((1, hidden, width), BF)
    spec = pl.BlockSpec((1, hidden, 2 * lanes), lambda i: (0, 0, i))
    return pl.pallas_call(
        grads_body,
        grid=(blocks // 2,),
        out_shape=[out] * 3,
        in_specs=[
            pl.BlockSpec((2, rows, lanes), lambda i: (i, 0, 0)),
            pl.BlockSpec(acts.shape, lambda i: (0, 0)),
        ],
        out_specs=[spec] * 3,
        compiler_params=pltpu.CompilerParams(vmem_limit_bytes=16 * 1024 * 1024),
        cost_estimate=pl.CostEstimate(
            flops=3 * rows * hidden * width, bytes_accessed=6 * hidden * width, transcendentals=0
        ),
    )(whole, acts)


def owner_sum_body(experts, capacity, parts, carry, acts, out):
    total = parts[0].astype(F32)
    for j in range(1, parts.shape[0]):
        total = total + parts[j].astype(F32)
    total = total.astype(BF)
    rows = experts * HOME_ROWS
    place = iota((rows, 1), 0)
    inner = place & (HOME_ROWS - 1)
    source = jnp.where(inner < capacity, (place >> 4) * capacity + inner, -1)
    pick = (iota((rows, experts * capacity), 1) == source).astype(F32).astype(BF)
    extra = (iota((rows, carry.shape[0]), 1) == inner - capacity).astype(F32).astype(BF)
    out[...] = (dot(pick, total) + dot(extra, carry[...])).astype(BF)


def lift_body(home, comb, cot, saved, out, mix, ends, adds):
    grad = dot(comb[...], home[...], 0, 0)
    lifted = (cot[...].astype(F32) + grad).astype(BF)
    for j in range(out.shape[0]):
        out[j] = lifted
    join_body(home, saved, mix, ends, adds)


def shift_in(x, d, fill, lane):
    return jnp.where(lane >= d, pltpu.roll(x, d, 1), fill)


def shift_out(x, d, fill, lane):
    width = x.shape[1]
    return jnp.where(lane < width - d, pltpu.roll(x, width - d, 1), fill)


def scan(decay, drive, lane, moved):
    d = 1
    while d < decay.shape[1]:
        drive = decay * moved(drive, d, 0.0, lane) + drive
        decay = decay * moved(decay, d, 1.0, lane)
        d *= 2
    return decay, drive


def in_three(x):
    high = x.astype(BF)
    rest = x - high.astype(F32)
    mid = rest.astype(BF)
    low = (rest - mid.astype(F32)).astype(BF)
    return high, mid, low


def ends_rows(up, down, lane):
    width = up.shape[1]
    ends = jnp.concatenate(
        [jnp.where(lane == width - 1, up, 0.0), jnp.where(lane == 0, down, 0.0)], axis=0
    )
    ones = jnp.ones((8, width), BF)
    return [dot(ones, piece, 1, 1) for piece in in_three(ends)]


def stacked(rows, width):
    place = iota((8, width), 0)
    total = jnp.zeros((8, width), F32)
    for k, row in enumerate(rows):
        total = jnp.where(place == k, row, total)
    return total


def to_columns(row, lane):
    channel = iota(lane.shape, 0)
    channels = lane.shape[0]
    up = jnp.sum(jnp.where(lane == channel, row, 0.0), axis=1, keepdims=True)
    down = jnp.sum(jnp.where(lane == channel + channels, row, 0.0), axis=1, keepdims=True)
    return up, down


def fold(me, prods, adds, channels):
    devices, width = prods.shape
    row, lane = iota((devices, width), 0), iota((devices, width), 1)
    ahead = lane < channels
    live = jnp.where(ahead, (row < me).astype(I32), (row > me).astype(I32)) > 0
    prod = jnp.where(live, prods[...], 1.0)
    add = jnp.where(live, adds[...], 0.0)
    d = 1
    while d < devices:
        next_prod = pltpu.roll(prod, devices - d, 0)
        next_add = pltpu.roll(add, devices - d, 0)
        add = jnp.where(ahead, next_prod * add + next_add, prod * next_add + add)
        prod = prod * next_prod
        d *= 2
    return add[:1]


SAVED = 12
KEPT = 6


def soft_plus(x):
    small = jnp.exp(-jnp.abs(x))
    z = small / (2.0 + small)
    square = z * z
    series = jnp.full_like(z, 1.0 / 19.0)
    for odd in (17, 15, 13, 11, 9, 7, 5, 3, 1):
        series = series * square + 1.0 / odd
    return jnp.maximum(x, 0.0) + 2.0 * z * series


def state_body(conv, branch, w_recur, w_input, decay_param, saved, carry):
    channels, tokens = conv.shape
    lane = iota((channels, tokens), 1)
    eye = iota((channels, channels), 0) == iota((channels, channels), 1)
    softness = jnp.sum(jnp.where(eye, soft_plus(-decay_param[...]), 0.0), axis=1, keepdims=True)
    values = conv[...].astype(F32)
    sig_r = jax.nn.sigmoid(dot(w_recur[0], conv[...], 0, 0))
    sig_a = jax.nn.sigmoid(dot(w_input[0], conv[...], 0, 0))
    decay = jnp.exp(-DECAY_SCALE * sig_r * softness)
    root = jnp.sqrt(1.0 - decay * decay + LEAK)
    direct = root * sig_a
    drive = direct * values
    up_prod, up_state = scan(decay, drive, lane, shift_in)
    down_prod, down_state = scan(decay, drive, lane, shift_out)
    x = branch[...].astype(F32)
    th = jnp.tanh(GELU_A * (x + GELU_B * x * x * x))
    saved[0] = decay
    saved[1] = up_prod
    saved[2] = up_state
    saved[3] = down_prod
    saved[4] = down_state
    saved[5] = 0.5 * x * (1.0 + th)
    saved[6] = 0.5 * (1.0 + th) + 0.5 * x * (1.0 - th * th) * GELU_A * (
        1.0 + 3.0 * GELU_B * x * x
    )
    saved[7] = decay * (-DECAY_SCALE * softness) * sig_r * (1.0 - sig_r)
    saved[8] = -(decay / root) * sig_a * values
    saved[9] = root * values * sig_a * (1.0 - sig_a)
    saved[10] = direct
    saved[11] = jnp.concatenate([w_recur[0], w_input[0]], axis=1).astype(F32)
    rows = ends_rows(up_prod, down_prod, lane) + ends_rows(up_state, down_state, lane)
    carry[...] = stacked(rows, tokens).astype(BF)


def joined_states(saved, state_in, state_back):
    return saved[2] + saved[1] * state_in, saved[4] + saved[3] * state_back


def join_body(home, saved, mix, ends, adds):
    channels, tokens = mix.shape
    devices = adds.shape[0]
    rows = home.shape[0]
    lane = iota((channels, tokens), 1)
    offset = iota((devices, rows), 1) - HOME_ROWS * iota((devices, rows), 0)
    base = HOME_ROWS - 6
    prod_rows = ((offset >= base) & (offset < base + 3)).astype(F32).astype(BF)
    add_rows = ((offset >= base + 3) & (offset < base + 6)).astype(F32).astype(BF)
    prods = ends.at[channels:, :]
    prods[...] = dot(prod_rows, home[...])
    adds[...] = dot(add_rows, home[...])
    state_in, state_back = to_columns(fold(lax.axis_index("sp"), prods, adds, channels), lane)
    ends[:channels, :] = jnp.where(lane < channels, state_in, state_back)
    fwd, bwd = joined_states(saved, state_in, state_back)
    mix[...] = (saved[5] * (fwd + bwd)).astype(BF)


def proj_body(lifted, mix, mine, theirs):
    blocks, tokens, _ = lifted.shape
    channels = mix.shape[0]
    half = channels // 2
    part_rows = mine.shape[1]
    left = iota((half, 128), 1) < 64
    even = (lax.axis_index("sp") & 1) == 0
    mixed = mix[...]
    for k in range(blocks // 2):
        proj = dot(mixed, pair(lifted, k, 0, tokens))
        for q in range(2):
            part = proj[:, 128 * q : 128 * (q + 1)]
            top, bottom = part[:half], part[half:]
            spot = 4 * k + 2 * q
            first = jnp.where(left, top, pltpu.roll(bottom, 64, 1))
            second = jnp.where(left, pltpu.roll(top, 64, 1), bottom)
            for n, rows in enumerate((first, second)):
                low, high = rows[:part_rows], rows[part_rows:]
                mine[spot + n] = jnp.where(even, low, high)
                theirs[spot + n] = jnp.where(even, high, low).astype(BF)


def adjoint_body(lifted, w_out, saved, ends, kept):
    blocks, tokens, _ = lifted.shape
    channels = w_out.shape[0]
    lane = iota((channels, tokens), 1)
    mix_cot = jnp.zeros((channels, tokens), F32)
    for k in range(blocks // 2):
        both = pair(lifted, k, 0, tokens)
        mix_cot = mix_cot + dot(w_out[:, 256 * k : 256 * (k + 1)], both, 1, 1)
    decay = saved[0]
    cot = mix_cot * saved[5]
    weighted = decay * cot
    _, up = scan(decay, weighted, lane, shift_in)
    _, down = scan(decay, weighted, lane, shift_out)
    kept[:channels] = mix_cot
    kept[channels : 2 * channels] = cot
    kept[2 * channels : 3 * channels] = up
    kept[3 * channels : 4 * channels] = down
    kept[4 * channels : 4 * channels + ends.shape[0]] = ends[...]
    kept[kept.shape[0] - 8 :] = stacked(ends_rows(up, down, lane), tokens)


def pack_body(mine, theirs, kept, far_out, out, sems):
    devices, part_rows, width = mine.shape
    spot = kept.shape[0] - 8
    tail = kept[spot : spot + 8][:GROUP].astype(BF)
    step, writes = devices // 4, []
    for s in range(devices):
        rows = mine[s] + theirs[s].astype(F32)
        for k in range(part_rows // GROUP):
            group = rows[GROUP * k : GROUP * (k + 1)].astype(BF)
            out[s, :, width * k : width * (k + 1)] = group
        out[s, :, width * (part_rows // GROUP) :] = tail
        if (s + 1) % step == 0:
            n = s // step
            span = pl.ds(n * step, step)
            writes.append(pltpu.make_async_copy(out.at[span], far_out.at[span], sems.at[n]))
            writes[n].start()
    for write in writes:
        write.wait()


def finish_body(last, saved, kept, g_proj, g_conv, g_branch, adds):
    devices = adds.shape[0]
    channels, tokens = g_conv.shape
    ends = kept.at[4 * channels :, :]
    prods = kept.at[5 * channels : 5 * channels + devices, :]
    lane = iota((channels, tokens), 1)
    cut = last.shape[2] - 128
    totals = [jnp.zeros((GROUP, cut), F32)] * 2
    for s in range(devices):
        totals[s & 1] = totals[s & 1] + last[s, :, :cut].astype(F32)
        adds[s : s + 1, :] = jnp.sum(last[s, :, cut:].astype(F32), axis=0, keepdims=True)
    turned = jnp.concatenate(
        [total[:, k : k + 128] for total in totals for k in range(0, cut, 128)], axis=0
    ).T
    g_proj[...] = jnp.concatenate([turned[:64], turned[64:]], axis=1)
    adj_in, adj_back = to_columns(fold(lax.axis_index("sp"), prods, adds, channels), lane)
    state_in, state_back = ends[:channels, :1], ends[:channels, tokens - 1 :]
    fwd, bwd = joined_states(saved, state_in, state_back)
    before = jnp.where(lane == 0, state_in, pltpu.roll(fwd, 1, 1))
    after = jnp.where(lane == tokens - 1, state_back, pltpu.roll(bwd, tokens - 1, 1))
    cot = kept[channels : 2 * channels]
    up = kept[2 * channels : 3 * channels] + saved[1] * adj_in
    down = kept[3 * channels : 4 * channels] + saved[3] * adj_back
    past = cot + jnp.where(lane == 0, adj_in, pltpu.roll(up, 1, 1))
    future = cot + jnp.where(lane == tokens - 1, adj_back, pltpu.roll(down, tokens - 1, 1))
    drive_cot = past + future
    decay_cot = future * before + past * after + drive_cot * saved[8]
    recur_cot = decay_cot * saved[7]
    admit_cot = drive_cot * saved[9]
    exact = lax.Precision.HIGHEST
    g_conv[...] = (
        drive_cot * saved[10]
        + dot(saved[11], jnp.concatenate([recur_cot, admit_cot], axis=0), 1, 0, exact)
    )
    g_branch[...] = kept[:channels] * (fwd + bwd) * saved[6]


def local(
    residual,
    out_cot,
    routes,
    route_weight,
    w_gate,
    w_up,
    w_down,
    w_out,
    conv_out,
    gate_branch,
    w_recur,
    w_input,
    decay_param,
):
    experts = lax.axis_size("sp")
    blocks = lax.axis_size("tp")
    tokens, lanes = residual.shape
    capacity = 2 * tokens // experts + 2
    slots = experts * capacity
    hidden, width = w_gate.shape[1:]
    channels = conv_out.shape[0]

    def kernel(body, *static):
        def run(*refs):
            body(*static, *refs)

        return run

    sent, comb = call(
        kernel(dispatch_body, experts),
        [
            ((experts, GROUP, 2 * capacity // GROUP * lanes), BF),
            ((experts * HOME_ROWS, tokens), BF),
        ],
        (routes.T, route_weight.T, residual, out_cot),
        fetched=4,
    )
    got = lax.all_to_all(sent, "sp", split_axis=0, concat_axis=0, tiled=True)
    (spread,) = call(
        kernel(compact_body, experts, capacity),
        [((blocks, 2 * slots, lanes), BF)],
        (got,),
    )
    whole = lax.all_to_all(spread, "tp", 0, 0, tiled=True)
    dxp, acts, saved, carry = call(
        expert_body,
        [
            ((blocks, slots, lanes), BF),
            ((slots, 3 * hidden), BF),
            ((SAVED, channels, tokens), F32),
            ((8, tokens), BF),
        ],
        (
            conv_out,
            gate_branch,
            w_recur,
            w_input,
            decay_param.reshape(1, channels),
            whole,
            w_gate[0],
            w_up[0],
            w_down[0],
        ),
        flops=10 * slots * hidden * width,
    )
    parts = lax.all_to_all(dxp, "tp", 0, 0, tiled=True)
    (returned,) = call(
        kernel(owner_sum_body, experts, capacity),
        [((experts * HOME_ROWS, lanes), BF)],
        (parts, carry, acts),
    )
    home = lax.all_to_all(
        returned.reshape(experts, HOME_ROWS, lanes), "sp", split_axis=0, concat_axis=0, tiled=True
    ).reshape(experts * HOME_ROWS, lanes)
    own, mix, ends = call(
        lift_body,
        [
            ((blocks, tokens, lanes), BF),
            ((channels, tokens), BF),
            ((channels + experts, tokens), F32),
        ],
        (home, comb, out_cot, saved),
        scratch=(pltpu.VMEM((experts, tokens), F32),),
    )
    lifted = lax.all_to_all(own, "tp", 0, 0, tiled=True)
    part_rows = channels // 4
    last_width = (part_rows // GROUP + 1) * lanes
    mine, theirs = call(
        proj_body,
        [((experts, part_rows, lanes), F32), ((experts, part_rows, lanes), BF)],
        (lifted, mix),
        flops=2 * channels * tokens * width,
    )
    swapped = lax.ppermute(theirs, "sp", [(i, i ^ 1) for i in range(experts)])
    (kept,) = call(
        adjoint_body,
        [((KEPT * channels, tokens), F32)],
        (lifted, w_out, saved, ends),
        flops=100 * channels * tokens * width,
    )
    (piece,) = call(
        pack_body,
        [((experts, GROUP, last_width), BF)],
        (mine, swapped, kept),
        scratch=(pltpu.VMEM((experts, GROUP, last_width), BF), pltpu.SemaphoreType.DMA((4,))),
        far=(0,),
    )
    piece, acts = lax.optimization_barrier((piece, acts))
    grads = expert_grads(whole, acts, width)
    last = lax.all_to_all(piece, "sp", split_axis=0, concat_axis=0, tiled=True)
    g_proj, g_conv, g_branch = call(
        finish_body,
        [((width // experts, channels), F32), ((channels, tokens), F32), ((channels, tokens), F32)],
        (last, saved, kept),
        scratch=(pltpu.VMEM((experts, tokens), F32),),
    )
    return (grads[0], grads[1], grads[2], g_proj, g_conv, g_branch)


def solution(mesh):
    return jax.shard_map(
        local,
        mesh=mesh,
        in_specs=(
            P("sp", "tp"),
            P("sp", "tp"),
            P("sp", None),
            P("sp", None),
            P("sp", "tp", None),
            P("sp", "tp", None),
            P("sp", "tp", None),
            P("tp", None),
            P("tp", "sp"),
            P("tp", "sp"),
            P("tp", None, None),
            P("tp", None, None),
            P("tp"),
        ),
        out_specs=(
            P("sp", "tp", None),
            P("sp", "tp", None),
            P("sp", "tp", None),
            P("sp", "tp"),
            P("tp", "sp"),
            P("tp", "sp"),
        ),
        check_vma=False,
    )
```
